256 devices in a mesh: sp: 32 (over z, y), tp: 8 (over x, core).
Axes of the slice: x: 4, y: 4, z: 8, core: 2. Of those that a mesh axis runs over, the one named last changes fastest.
Arguments:
- mix_input: bfloat16 [8192, 1024], P('sp', 'tp'), may hold values from -6 to 6
- stream: bfloat16 [8192, 2048], P(('sp', 'tp')), may hold values from -48 to 48
- doc_ids: int32 [8192], P('sp'), may hold values from 0 to 3, never falling along the last dimension, each value on 1 to 4096 neighbouring positions
- log_dt: float32 [64], P('tp'), may hold values from -12 to -2
- decay_rate: float32 [64, 64], P('tp'), may hold values from 0.5 to 1
- frequency: float32 [64, 64], P('tp'), may hold values from 0 to 64
- input_real: float32 [2, 64, 64, 16], P(None, 'tp'), may hold values from -400 to 400
- input_imag: float32 [2, 64, 64, 16], P(None, 'tp'), may hold values from -400 to 400
- output_real: float32 [2, 64, 16, 64], P(None, 'tp'), may hold values from -0.75 to 0.75
- output_imag: float32 [2, 64, 16, 64], P(None, 'tp'), may hold values from -0.75 to 0.75
- skip_gain: float32 [1024], P('tp'), may hold values from -4 to 4
- log_keep: float32 [64, 8192], P('tp', 'sp'), may hold values from -2 to 0
- proj_weight: bfloat16 [1024, 2048], P('tp'), may hold values from -0.1875 to 0.1875
- norm_gain: float32 [2048], replicated, may hold values from 0.1 to 1.9
- gate_weight: bfloat16 [2048, 5632], P('sp', 'tp'), may hold values from -0.125 to 0.125
- up_weight: bfloat16 [2048, 5632], P('sp', 'tp'), may hold values from -0.125 to 0.125
- down_weight: bfloat16 [5632, 2048], P('tp', 'sp'), may hold values from -0.078125 to 0.078125
Outputs:
- layer_out: bfloat16 [8192, 2048], P(('sp', 'tp'))
The draws below stay inside these ranges and needn't reach their ends.
Inputs may be any that keep to these rules, and one draw needn't show every extreme that they name: `doc_ids`: document numbers never fall along the positions; a document covers at most half of the positions.
All inputs are finite; a program needn't handle non-finite values.
Results may differ from the reference program's by a relative error of at most 0.009.
Values may be sent and summed in bfloat16 or wider, within the bound.
A program may use at most 128 MiB of HBM per device.

```python
import math
import jax
import jax.numpy as jnp
import numpy as np
from jax import lax

D = 2048
WIDTH = 1024
GROUP = 16
STATE = 64
FF = 5632
TOK_DEV = 256
DOCS = 4
GROUPS = 64
TOKENS = 8192
N_TP = 8


def group_steps(key):
    base = jax.random.fold_in(key, 11)
    first_key, second_key, third_key = jax.random.split(base, 3)
    picked = jax.random.uniform(first_key, (GROUPS,), jnp.float32)
    slower = picked < 0.5
    slow_value = math.log(0.5 / TOKENS) + jax.random.uniform(second_key, (GROUPS,), jnp.float32, -0.3, 0.3)
    fast_value = jax.random.uniform(third_key, (GROUPS,), jnp.float32, math.log(0.04), math.log(0.05))
    return jnp.where(slower, slow_value, fast_value)


def draw_log_dt(key, part):
    return group_steps(key).astype(jnp.float32)


def input_matrix(key, salt):
    log_step = group_steps(key)
    scale = jnp.sqrt(2.0 / (jnp.exp(log_step) * GROUP))
    noise = jax.random.truncated_normal(jax.random.fold_in(key, salt), -4.0, 4.0, (2, GROUPS, STATE, GROUP), jnp.float32)
    return (noise * scale[None, :, None, None]).astype(jnp.float32)


def draw_input_real(key, part):
    return input_matrix(key, 21)


def draw_input_imag(key, part):
    return input_matrix(key, 22)


def draw_log_keep(key, part):
    base = jax.random.fold_in(key, 31)
    first_key, second_key, third_key, fourth_random_key = jax.random.split(base, 4)
    blocks = TOKENS // TOK_DEV
    level = jnp.exp(jax.random.uniform(first_key, (GROUPS, blocks), jnp.float32, math.log(0.1), 0.0)) / TOKENS
    per_slot_feedforward = jnp.repeat(level, TOK_DEV, axis=1) * jax.random.uniform(second_key, (GROUPS, TOKENS), jnp.float32, 0.0, 2.0)
    slot_indices = jax.random.randint(third_key, (GROUPS, 2), 0, TOKENS)
    stack_level_count = jax.random.uniform(fourth_random_key, (GROUPS, 2), jnp.float32, 0.22, 0.69)
    sequence_offsets = jnp.arange(TOKENS, dtype=jnp.int32)
    segment_sets = jnp.sum((sequence_offsets[None, None, :] == slot_indices[:, :, None]).astype(jnp.float32) * stack_level_count[:, :, None], axis=1)
    return (-(per_slot_feedforward + segment_sets)).astype(jnp.float32)


def draw_stream(key, part):
    base = jax.random.fold_in(key, 41)
    first_key, second_key, third_key = jax.random.split(base, 3)
    row_scale = jnp.exp(jax.random.uniform(first_key, (TOKENS, 1), jnp.float32, math.log(0.3), math.log(3.0)))
    col_scale = jnp.exp(jax.random.uniform(second_key, (1, D), jnp.float32, math.log(0.3), math.log(3.0)))
    values = jax.random.truncated_normal(third_key, -4.0, 4.0, (TOKENS, D), jnp.float32)
    return (values * row_scale * col_scale).astype(jnp.bfloat16)


def block_levels(own_key, extent, shards, least, largest):
    level = 1.0
    for axis_at, parts in shards:
        draws = jax.random.uniform(jax.random.fold_in(jax.random.fold_in(own_key, 6), axis_at), (parts,), jnp.float32, least / len(shards), largest / len(shards))
        level = level * jnp.repeat(jnp.exp(draws), extent[axis_at] // parts).reshape((-1,) + (1,) * (len(extent) - 1 - axis_at))
    return level


def split_up(amount, total, reach, slope):
    loads = [(1 << 20) // math.isqrt(rank ** slope) + 1 for rank in range(2, amount + 1)]
    surplus, holding = total - reach - (amount - 1), [1] * (amount - 1)
    while surplus > 0:
        candidates = [i for i in range(amount - 1) if holding[i] < reach]
        mass, left = sum([loads[i] for i in candidates]), surplus
        for i in candidates:
            extra = min(reach - holding[i], max(1, left * loads[i] // mass), surplus)
            holding[i] = holding[i] + extra
            surplus = surplus - extra
    return np.array([reach] + holding)


def uneven(rng, count, total, most, lean):
    if count == 2:
        one = jax.random.randint(rng, (), max(1, total - most), min(most, total - 1) + 1)
        return jnp.stack([one, total - one])
    sizes = jnp.asarray(split_up(count, total, most, lean), jnp.int32)
    couples = (count - 1) // 2
    giver, receiver = sizes[1:1 + 2 * couples:2], sizes[2:2 + 2 * couples:2]
    room = jnp.minimum(giver - 1, most - receiver)
    moved = jax.random.randint(jax.random.fold_in(rng, 1), (couples,), 0, 1 << 20) % (room + 1)
    sizes = sizes.at[1:1 + 2 * couples:2].set(giver - moved).at[2:2 + 2 * couples:2].set(receiver + moved)
    return sizes[jax.random.permutation(jax.random.fold_in(rng, 2), count)]


def scatter_about(stream_key, shape, scale, bound, cuts=(), kind=jnp.bfloat16):
    array = scale * jax.random.normal(stream_key, shape, jnp.float32)
    if cuts:
        array = array * block_levels(stream_key, shape, cuts, -0.22, 0.18)
    return jnp.clip(array, -bound, bound).astype(kind)


def setup_inputs(seed: int = 0) -> dict:
    streams_of = jax.random.split(jax.random.key(seed), 18)
    return {
        "mix_input": scatter_about(streams_of[0], (TOKENS, WIDTH), 1.0, 6.0, ((0, 32), (1, 8))),
        "stream": draw_stream(jax.random.fold_in(streams_of[17], 71), 0),
        "doc_ids": jnp.searchsorted(jnp.cumsum(uneven(streams_of[2], DOCS, TOKENS, TOKENS // 2, 0)), jnp.arange(TOKENS), side="right").astype(jnp.int32),
        "log_dt": draw_log_dt(jax.random.fold_in(streams_of[17], 71), 0),
        "decay_rate": jnp.clip(jnp.exp(math.log(1.0) - 0.6931472 * jax.random.uniform(streams_of[4], (GROUPS, STATE), jnp.float32) ** block_levels(streams_of[4], (GROUPS, STATE), ((0, 8),), -0.2, 0.2)), 0.5, 1.0),
        "frequency": jnp.clip(64.0 * jax.random.uniform(streams_of[5], (GROUPS, STATE), jnp.float32) ** block_levels(streams_of[5], (GROUPS, STATE), ((0, 8),), -0.2, 0.2), 0.0, 64.0),
        "input_real": draw_input_real(jax.random.fold_in(streams_of[17], 71), 0),
        "input_imag": draw_input_imag(jax.random.fold_in(streams_of[17], 71), 0),
        "output_real": scatter_about(streams_of[8], (2, GROUPS, GROUP, STATE), STATE ** -0.5, 0.75, ((1, 8),), jnp.float32),
        "output_imag": scatter_about(streams_of[9], (2, GROUPS, GROUP, STATE), STATE ** -0.5, 0.75, ((1, 8),), jnp.float32),
        "skip_gain": scatter_about(streams_of[10], (WIDTH,), 1.0, 4.0, ((0, 8),), jnp.float32),
        "log_keep": draw_log_keep(jax.random.fold_in(streams_of[17], 71), 0),
        "proj_weight": scatter_about(streams_of[12], (WIDTH, D), WIDTH ** -0.5, 0.1875, ((0, 8),)),
        "norm_gain": jnp.clip(1.0 + 0.18 * jax.random.normal(streams_of[13], (D,), jnp.float32), 0.1, 1.9),
        "gate_weight": scatter_about(streams_of[14], (D, FF), D ** -0.5, 0.125, ((0, 32), (1, 8))),
        "up_weight": scatter_about(streams_of[15], (D, FF), D ** -0.5, 0.125, ((0, 32), (1, 8))),
        "down_weight": scatter_about(streams_of[16], (FF, D), FF ** -0.5, 0.078125, ((0, 8), (1, 32))),
    }


HIGHEST = lax.Precision.HIGHEST

def discretize(log_dt, decay_rate, frequency):
    step_size = jnp.exp(log_dt)[:, None]
    magnitude = jnp.exp(-step_size * decay_rate)
    angle_step = step_size * frequency
    state_real = magnitude * jnp.cos(angle_step)
    state_imag = magnitude * jnp.sin(angle_step)
    denominator = decay_rate * decay_rate + frequency * frequency
    shifted = state_real - 1.0
    zoh_real = (-shifted * decay_rate + state_imag * frequency) / denominator
    holdfixed_angle_part = (-state_imag * decay_rate - shifted * frequency) / denominator
    return (state_real, state_imag, zoh_real, holdfixed_angle_part)

def input_maps(zoh_real, holdfixed_angle_part, input_real, input_imag):
    scale_real = zoh_real[None, :, :, None]
    scale_imag = holdfixed_angle_part[None, :, :, None]
    return (scale_real * input_real - scale_imag * input_imag, scale_real * input_imag + scale_imag * input_real)

def pair_combine(earlier, later):
    mult_one_real, mult_one_imag, first_state_real, state_one_imag = earlier
    mult_two_real, second_multiplier_imag, state_two_real, state_two_imag = later
    return (mult_two_real * mult_one_real - second_multiplier_imag * mult_one_imag, mult_two_real * mult_one_imag + second_multiplier_imag * mult_one_real, mult_two_real * first_state_real - second_multiplier_imag * state_one_imag + state_two_real, mult_two_real * state_one_imag + second_multiplier_imag * first_state_real + state_two_imag)

def rounded_sum(activations, weights, pieces):
    block_width = activations.shape[1] // pieces
    summed = jnp.zeros((activations.shape[0], weights.shape[1]), jnp.float32)
    for number in range(pieces):
        lower = number * block_width
        partial_value = jnp.dot(activations[:, lower:lower + block_width], weights[lower:lower + block_width], preferred_element_type=jnp.float32).astype(jnp.bfloat16)
        summed = summed + lax.optimization_barrier(partial_value).astype(jnp.float32)
    return summed

def reference(mix_input, stream, doc_ids, log_dt, decay_rate, frequency, input_real, input_imag, output_real, output_imag, skip_gain, log_keep, proj_weight, norm_gain, gate_weight, up_weight, down_weight):
    state_real, state_imag, zoh_real, holdfixed_angle_part = discretize(log_dt, decay_rate, frequency)
    map_real, map_imag = input_maps(zoh_real, holdfixed_angle_part, input_real, input_imag)
    channels = mix_input.astype(jnp.float32)
    grouped = channels.reshape(TOKENS, GROUPS, GROUP).transpose(1, 0, 2)
    same_doc = (doc_ids[1:] == doc_ids[:-1]).astype(jnp.float32)
    nothing = jnp.zeros((1,), jnp.float32)
    link_prev = jnp.concatenate([nothing, same_doc])
    link_next = jnp.concatenate([same_doc, nothing])
    keep_rates = jnp.exp(log_keep)

    def group_pass(packed):
        cluster_source, group_real, group_imag, group_map_real, group_map_imag, read_real, read_imag, keep_row = packed
        result = jnp.zeros((TOKENS, GROUP), jnp.float32)
        for direction, doc_links, reverse in ((0, link_prev, False), (1, link_next, True)):
            factor = (keep_row * doc_links)[:, None]
            mult_real = factor * group_real[None, :]
            mult_imag = factor * group_imag[None, :]
            drive_real = jnp.dot(cluster_source, group_map_real[direction].T, precision=HIGHEST)
            drive_imag = jnp.dot(cluster_source, group_map_imag[direction].T, precision=HIGHEST)
            scanned = lax.associative_scan(pair_combine, (mult_real, mult_imag, drive_real, drive_imag), reverse=reverse, axis=0)
            result = result + jnp.dot(scanned[2], read_real[direction].T, precision=HIGHEST)
            result = result - jnp.dot(scanned[3], read_imag[direction].T, precision=HIGHEST)
        return result
    outputs = lax.map(group_pass, (grouped, state_real, state_imag, map_real.transpose(1, 0, 2, 3), map_imag.transpose(1, 0, 2, 3), output_real.transpose(1, 0, 2, 3), output_imag.transpose(1, 0, 2, 3), keep_rates))
    mixed_pre = outputs.transpose(1, 0, 2).reshape(TOKENS, WIDTH) + skip_gain * channels
    mixed = jax.nn.gelu(mixed_pre).astype(jnp.bfloat16)
    branch = rounded_sum(mixed, proj_weight, N_TP)
    resid = stream.astype(jnp.float32) + branch
    scale = lax.rsqrt(lax.optimization_barrier(jnp.mean(resid * resid, axis=-1, keepdims=True)) + 1e-06)
    normed = (resid * scale * norm_gain).astype(jnp.bfloat16)
    block_width = FF // N_TP
    ffn = jnp.zeros((TOKENS, D), jnp.float32)
    for number in range(N_TP):
        lower = number * block_width
        gate = jnp.dot(normed, gate_weight[:, lower:lower + block_width], preferred_element_type=jnp.float32)
        upward = jnp.dot(normed, up_weight[:, lower:lower + block_width], preferred_element_type=jnp.float32)
        hidden = (jax.nn.silu(gate) * upward).astype(jnp.bfloat16)
        partial_value = jnp.dot(hidden, down_weight[lower:lower + block_width], preferred_element_type=jnp.float32).astype(jnp.bfloat16)
        ffn = ffn + lax.optimization_barrier(partial_value).astype(jnp.float32)
    return (resid + 0.5 * ffn).astype(jnp.bfloat16)
```

```python
import functools

import jax
import jax.numpy as jnp
from jax import lax
from jax.experimental import pallas as pl
from jax.experimental.pallas import tpu as pltpu
from jax.sharding import Mesh
from jax.sharding import PartitionSpec as P

HIGHEST = lax.Precision.HIGHEST
MESH = pl.DeviceIdType.MESH
F32, BF16 = jnp.float32, jnp.bfloat16

NZ, NY, NX, NC = 8, 4, 4, 2
SP, TP = NZ * NY, NX * NC
T, CH, G, S, GW = 256, 128, 8, 64, 16
W = G * S
CHUNKS = 8
STEPS = T // CHUNKS
D = 2048
FF = 704
MAIN = 640
ROWS = D // SP
TOK = T // TP
GUA, GUB = MAIN + 128, MAIN
DA, DB = 512, 256
KPAD = DA + DB
NT = (((1,), (1,)), ((), ()))


def dot(a, b, precision=None):
    return jnp.dot(a, b, preferred_element_type=F32, precision=precision)


def dot_nt(a, b, precision=None):
    return lax.dot_general(a, b, NT, preferred_element_type=F32, precision=precision)


def halves(value):
    high = value.astype(BF16)
    return high, (value - high.astype(F32)).astype(BF16)


def iota(shape, dim):
    return lax.broadcasted_iota(jnp.int32, shape, dim)


def one_hot(mask, dtype):
    return jnp.where(mask, 1.0, 0.0).astype(F32).astype(dtype)


def cmul(ar, ai, br, bi):
    return ar * br - ai * bi, ar * bi + ai * br


class Relay:
    def __init__(self, ra, rb, send, recv, base, z, y):
        self.ra, self.rb, self.send, self.recv, self.base = ra, rb, send, recv, base
        self.z, self.y = z, y
        self.started = []

    def zi(self, offset):
        return lax.rem(self.z + (offset + NZ), NZ)

    def yi(self, offset):
        return lax.rem(self.y + (offset + NY), NY)

    def copy(self, number, ref, axis, to):
        to = self.zi(to) if axis == "z" else self.yi(to)
        return pltpu.make_async_remote_copy(
            src_ref=ref,
            dst_ref=ref,
            send_sem=self.send.at[self.base + number],
            recv_sem=self.recv.at[self.base + number],
            device_id={axis: to},
            device_id_type=MESH,
        )

    def start(self, number, ref, axis, to):
        copy = self.copy(number, ref, axis, to)
        copy.start()
        self.started.append(copy)

    def wait(self, number, ref, axis):
        self.copy(number, ref, axis, 1).wait_recv()

    def a_z_ref(self, way, distance):
        ref = self.ra.at[self.zi(-way * distance), self.y]
        return ref

    def a_z_part(self, way, distance, last):
        piece = self.ra.at[self.zi(-way * distance), self.y]
        if last:
            piece = piece.at[pl.ds(0 if way > 0 else ROWS // 2, ROWS // 2)]
        return piece

    def a_send_z(self, d):
        for n, way in enumerate((1, -1)):
            self.start(n * 4 + d - 1, self.a_z_part(way, d - 1, d == 4), "z", way)

    def a_recv_z(self, d):
        for n, way in enumerate((1, -1)):
            self.wait(n * 4 + d - 1, self.a_z_part(way, d, d == 4), "z")

    def a_y(self, offset, dy):
        return self.ra.at[self.zi(offset), self.yi(dy)]

    def a_send_y(self, o):
        q = 8 + 3 * (o % NZ)
        self.start(q, self.a_y(o, 0), "y", 1)
        self.start(q + 1, self.a_y(o, 0), "y", -1)

    def a_pass_y(self, o):
        q = 8 + 3 * (o % NZ)
        self.wait(q, self.a_y(o, -1), "y")
        if o % 2 == 0:
            self.start(q + 2, self.a_y(o, -1), "y", 1)
        self.wait(q + 1, self.a_y(o, 1), "y")
        if o % 2 == 1:
            self.start(q + 2, self.a_y(o, 1), "y", -1)

    def a_last_y(self, o):
        self.wait(8 + 3 * (o % NZ) + 2, self.a_y(o, 2), "y")

    def b_y_part(self, way, distance, last):
        piece = self.rb.at[self.z, self.yi(-way * distance)]
        if last:
            piece = piece.at[pl.ds(0 if way > 0 else ROWS // 2, ROWS // 2)]
        return piece

    def b_send_y(self, d):
        for n, way in enumerate((1, -1)):
            self.start(32 + n * 2 + d - 1, self.b_y_part(way, d - 1, d == 2), "y", way)

    def b_recv_y(self, d):
        for n, way in enumerate((1, -1)):
            self.wait(32 + n * 2 + d - 1, self.b_y_part(way, d, d == 2), "y")

    def b_z_part(self, way, distance, last):
        piece = self.rb.at[self.zi(-way * distance)]
        if last:
            piece = piece.at[pl.ds(0 if way > 0 else NY // 2, NY // 2)]
        return piece

    def b_send_z(self, d):
        for n, way in enumerate((1, -1)):
            self.start(36 + n * 4 + d - 1, self.b_z_part(way, d - 1, d == 4), "z", way)

    def b_recv_z(self, d):
        for n, way in enumerate((1, -1)):
            self.wait(36 + n * 4 + d - 1, self.b_z_part(way, d, d == 4), "z")

    def drain(self):
        for copy in self.started:
            copy.wait_send()


RELAYS = 44
OFFSETS = (0, -1, 1, -2, 2, -3, 3, 4)


def row_of(block):
    return jnp.concatenate([block[g : g + 1, :] for g in range(G)], axis=1)


def rows_of(row):
    return jnp.concatenate([row[:, 128 * k : 128 * (k + 1)] for k in range(W // 128)], axis=0)


def flat_of(rows):
    return jnp.concatenate([rows[k : k + 1, :] for k in range(W // 128)], axis=1)


def kernel(
    mix, stream, docs, doc_scalar, log_dt, decay, freq, in_real, in_imag, out_real, out_imag,
    skip, log_keep, proj, gain, gate_w, up_w, down_w,
    result,
    gua, gub, dna, dnb, drive, factor, states, message, arrived, part, branch, resid, normed,
    hidden, ffn_send, ffn_recv,
    send, recv, carry_send, carry_recv, rs_send, rs_recv, ag_send, ag_recv, fs_send, fs_recv,
):
    z, y, x, c = (lax.axis_index(a) for a in ("z", "y", "x", "c"))
    sp, tp = z * NY + y, x * NC + c

    def sp_peer(k):
        other = lax.rem(sp + k, SP)
        return other, {"z": other // NY, "y": lax.rem(other, NY)}

    def tp_peer(k):
        other = lax.rem(tp + k, TP)
        return other, {"x": other // NC, "c": lax.rem(other, NC)}

    barrier = pltpu.get_barrier_semaphore()

    @pl.loop(1, SP)
    def _(k):
        pl.semaphore_signal(barrier, inc=1, device_id=sp_peer(k)[1], device_id_type=MESH)

    @pl.loop(1, TP)
    def _(k):
        pl.semaphore_signal(barrier, inc=1, device_id=tp_peer(k)[1], device_id_type=MESH)

    gua[z, y, :, 0:MAIN] = up_w[:, 0:MAIN]
    gua[z, y, :, MAIN:GUA] = jnp.concatenate([gate_w[:, MAIN:FF], up_w[:, MAIN:FF]], axis=1)
    gub[z, y] = gate_w[:, 0:MAIN]
    dna[z, y] = down_w[:, 0:DA]
    dnb[z, y] = jnp.concatenate([down_w[:, DA:FF], jnp.zeros((ROWS, KPAD - FF), BF16)], axis=1)

    group = iota((G, S), 0)
    steps = jnp.zeros((G, S), F32)
    for g in range(G):
        steps = jnp.where(group == g, log_dt[g], steps)
    steps = jnp.exp(steps)
    rate, turn_rate = decay[...], freq[...]
    magnitude = jnp.exp(-steps * rate)
    angle = steps * turn_rate
    a_real, a_imag = magnitude * jnp.cos(angle), magnitude * jnp.sin(angle)
    below = rate * rate + turn_rate * turn_rate
    shifted = a_real - 1.0
    z_real = (-shifted * rate + a_imag * turn_rate) / below
    z_imag = (-a_imag * rate - shifted * turn_rate) / below
    ar, ai, zr, zi = (row_of(v) for v in (a_real, a_imag, z_real, z_imag))

    r, t = iota((T, T), 0), iota((T, T), 1)
    order = t == lax.rem(r, CHUNKS) * STEPS + r // CHUNKS
    order_f = one_hot(order, F32)
    u = dot(order_f.astype(BF16), mix[...])
    ub = u.astype(BF16)

    tile = one_hot(lax.rem(iota((S, W), 1), S) == iota((S, W), 0), BF16)
    own = lax.rem(iota((2 * CH, W), 0), CH) // GW == iota((2 * CH, W), 1) // S
    for n, ref in enumerate((in_real, in_imag)):
        high, low = (
            jnp.where(own, dot(half, tile), 0.0).astype(BF16) for half in halves(ref[...])
        )
        for d in range(2):
            at = slice(CH * d, CH * (d + 1))
            drive[:, W * (2 * n + d) : W * (2 * n + d + 1)] = dot(ub, high[at]) + dot(ub, low[at])

    doc = docs[...].astype(F32) + jnp.zeros((G, T), F32)
    place = iota((G, T), 1)
    before, after = pltpu.roll(doc, 1, 1), pltpu.roll(doc, T - 1, 1)
    keep = jnp.exp(log_keep[...])
    keep_f = jnp.where((place == 0) | (doc == before), keep, 0.0)
    keep_b = jnp.where((place == T - 1) | (doc == after), keep, 0.0)
    both = dot_nt(order_f, jnp.concatenate([keep_f, keep_b], axis=0), HIGHEST)
    spread = one_hot(iota((2 * G, 2 * W), 0) == iota((2 * G, 2 * W), 1) // S, F32)
    factor[...] = dot(both, spread, HIGHEST)

    zero = jnp.zeros((CHUNKS, W), F32)
    ar8, ai8 = zero + ar, zero + ai

    def advance(j, state, direction):
        at = pl.ds(pl.multiple_of(j * CHUNKS, CHUNKS), CHUNKS)
        f = factor[at, W * direction : W * (direction + 1)]
        dr = drive[at, W * direction : W * (direction + 1)]
        di = drive[at, W * (2 + direction) : W * (3 + direction)]
        hr, hi = state
        nr, ni = cmul(f * ar8, f * ai8, hr, hi)
        return f, nr + dr, ni + di

    def first(j, state):
        fr, fi, fp, br, bi, bp = state
        f, fr, fi = advance(j, (fr, fi), 0)
        b, br, bi = advance(STEPS - 1 - j, (br, bi), 1)
        return fr, fi, fp * f, br, bi, bp * b

    fr, fi, fp, br, bi, bp = lax.fori_loop(
        0, STEPS, first, (zero, zero, zero + 1.0, zero, zero, zero + 1.0)
    )
    pr, pi = ar, ai
    for _ in range(5):
        pr, pi = cmul(pr, pi, pr, pi)

    def chunk_entries(enter, hr, hi, passed, backward):
        er, ei = enter
        entries = [None] * CHUNKS
        chunks = range(CHUNKS - 1, -1, -1) if backward else range(CHUNKS)
        for k in chunks:
            entries[k] = (er, ei)
            f = passed[k : k + 1]
            nr, ni = cmul(f * pr, f * pi, er, ei)
            er, ei = nr + hr[k : k + 1], ni + hi[k : k + 1]
        return entries, (er, ei)

    none = (jnp.zeros((1, W), F32), jnp.zeros((1, W), F32))
    end_f = chunk_entries(none, fr, fi, fp, False)[1]
    end_b = chunk_entries(none, br, bi, bp, True)[1]
    passed = fp[0:1]
    for k in range(1, CHUNKS):
        passed = passed * fp[k : k + 1]
    qr, qi = pr, pi
    for _ in range(3):
        qr, qi = cmul(qr, qi, qr, qi)
    edge_first = doc_scalar[0].astype(F32)
    edge_last = doc_scalar[T - 1].astype(F32)
    passed_rows = rows_of(passed)
    edges = jnp.concatenate(
        [jnp.full((1, 128), edge_first, F32), jnp.full((1, 128), edge_last, F32),
         jnp.zeros((2, 128), F32)], axis=0)
    for n, (er, ei) in enumerate((end_f, end_b)):
        message[n, 0:4] = rows_of(er)
        message[n, 4:8] = rows_of(ei)
        message[n, 8:12] = passed_rows
        message[n, 12:16] = edges
    arrived[sp] = jnp.zeros((16, 128), F32)

    gu = Relay(gua, gub, send, recv, 0, z, y)
    dn = Relay(dna, dnb, send, recv, RELAYS, z, y)

    pl.semaphore_wait(barrier, SP - 1 + TP - 1)
    gu.a_send_z(1)
    gu.b_send_y(1)
    gu.a_send_y(0)

    def carry_copy(k):
        other, device = sp_peer(k)
        side = jnp.where(other > sp, 0, 1)
        return pltpu.make_async_remote_copy(
            src_ref=message.at[side], dst_ref=arrived.at[sp],
            send_sem=carry_send.at[other], recv_sem=carry_recv.at[sp],
            device_id=device, device_id_type=MESH)

    @pl.loop(1, SP)
    def _(k):
        carry_copy(k).start()

    gu.a_recv_z(1)
    gu.a_send_z(2)
    gu.b_recv_y(1)
    gu.b_send_y(2)
    gu.a_send_y(-1)
    gu.a_send_y(1)
    gu.a_recv_z(2)
    gu.a_send_z(3)
    gu.b_recv_y(2)
    gu.b_send_z(1)
    gu.a_pass_y(0)
    gu.a_send_y(-2)
    gu.a_send_y(2)

    @pl.loop(1, SP)
    def _(k):
        other, device = sp_peer(k)
        pltpu.make_async_remote_copy(
            src_ref=message.at[0], dst_ref=arrived.at[other],
            send_sem=carry_send.at[other], recv_sem=carry_recv.at[other],
            device_id=device, device_id_type=MESH).wait_recv()

    q4r, q4i = rows_of(qr), rows_of(qi)
    four = jnp.zeros((4, 128), F32)

    def fold(j, state, near, far, use):
        cr, ci, last = state
        m = arrived[j]
        link = jnp.where(m[near : near + 1] == last, 1.0, 0.0) * m[8:12]
        nr, ni = cmul(link * q4r, link * q4i, cr, ci)
        cr = jnp.where(use, nr + m[0:4], cr)
        ci = jnp.where(use, ni + m[4:8], ci)
        return cr, ci, jnp.where(use, m[far : far + 1], last)

    def folds(k, state):
        forward = fold(k, state[0], 12, 13, k < sp)
        j = SP - 1 - k
        return forward, fold(j, state[1], 13, 12, j > sp)

    start = (four, four, jnp.zeros((1, 128), F32) - 1.0)
    into_f, into_b = lax.fori_loop(0, SP, folds, (start, start))
    enter_f = jnp.where(into_f[2] == edge_first, 1.0, 0.0)
    enter_b = jnp.where(into_b[2] == edge_last, 1.0, 0.0)
    enter_f = (flat_of(into_f[0] * enter_f), flat_of(into_f[1] * enter_f))
    enter_b = (flat_of(into_b[0] * enter_b), flat_of(into_b[1] * enter_b))
    entries_f = chunk_entries(enter_f, fr, fi, fp, False)[0]
    entries_b = chunk_entries(enter_b, br, bi, bp, True)[0]
    stacked = [
        jnp.concatenate([e[part_no] for e in entries], axis=0)
        for entries in (entries_f, entries_b) for part_no in (0, 1)
    ]

    def second(j, state):
        fr, fi, br, bi = state
        _, fr, fi = advance(j, (fr, fi), 0)
        k = STEPS - 1 - j
        _, br, bi = advance(k, (br, bi), 1)
        at = pl.ds(pl.multiple_of(j * CHUNKS, CHUNKS), CHUNKS)
        states[at, 0:W] = fr
        states[at, 2 * W : 3 * W] = fi
        at = pl.ds(pl.multiple_of(k * CHUNKS, CHUNKS), CHUNKS)
        states[at, W : 2 * W] = br
        states[at, 3 * W : 4 * W] = bi
        return fr, fi, br, bi

    lax.fori_loop(0, STEPS, second, tuple(stacked))

    tile = tile.astype(F32)
    cr = jnp.where(own, dot(out_real[...], tile, HIGHEST), 0.0)
    ci = jnp.where(own, dot(out_imag[...], tile, HIGHEST), 0.0)
    cr, ci = cmul(zr, zi, cr, ci)
    pre = skip[...] * u
    for n in range(4):
        read = (cr if n < 2 else -ci)[CH * (n % 2) : CH * (n % 2 + 1)]
        read_high, read_low = halves(read)
        high, low = halves(states[:, W * n : W * (n + 1)])
        pre = pre + dot_nt(high, read_high) + dot_nt(high, read_low) + dot_nt(low, read_high)
    mixed = jax.nn.gelu(pre).astype(BF16)
    back = one_hot(
        t == lax.rem(r, STEPS) * CHUNKS + r // STEPS, BF16)
    mixed = dot(back, mixed).astype(BF16)
    part[...] = dot(mixed, proj[...]).astype(BF16).reshape(TP, TOK, D)

    def rs_copy(k):
        other, device = tp_peer(k)
        return pltpu.make_async_remote_copy(
            src_ref=part.at[other], dst_ref=branch.at[tp],
            send_sem=rs_send.at[other], recv_sem=rs_recv.at[tp],
            device_id=device, device_id_type=MESH)

    @pl.loop(1, TP)
    def _(k):
        rs_copy(k).start()

    gu.a_recv_z(3)
    gu.a_send_z(4)
    gu.a_send_y(-3)
    gu.a_send_y(3)
    gu.a_pass_y(-1)
    gu.a_pass_y(1)
    dn.a_send_z(1)
    dn.b_send_y(1)
    gu.a_recv_z(4)
    gu.a_send_y(4)
    gu.b_recv_z(1)
    gu.b_send_z(2)
    gu.a_pass_y(-2)
    gu.a_pass_y(2)
    dn.a_send_y(0)
    dn.a_recv_z(1)
    dn.a_send_z(2)
    dn.b_recv_y(1)
    dn.b_send_y(2)

    branch[tp] = part[tp]

    @pl.loop(1, TP)
    def _(k):
        other, device = tp_peer(k)
        pltpu.make_async_remote_copy(
            src_ref=part.at[other], dst_ref=branch.at[other],
            send_sem=rs_send.at[other], recv_sem=rs_recv.at[other],
            device_id=device, device_id_type=MESH).wait_recv()

    kept = stream[...].astype(F32)
    for k in range(TP):
        kept = kept + branch[k].astype(F32)
    resid[...] = kept
    scale = lax.rsqrt(jnp.mean(kept * kept, axis=-1, keepdims=True) + 1e-6)
    normed[tp] = (kept * scale * gain[...]).astype(BF16)

    def ag_copy(k, number):
        other, device = tp_peer(k)
        return pltpu.make_async_remote_copy(
            src_ref=normed.at[number], dst_ref=normed.at[number],
            send_sem=ag_send.at[other], recv_sem=ag_recv.at[number],
            device_id=device, device_id_type=MESH)

    @pl.loop(1, TP)
    def _(k):
        ag_copy(k, tp).start()

    gu.b_recv_z(2)
    gu.b_send_z(3)
    gu.a_pass_y(-3)
    gu.a_pass_y(3)
    dn.a_send_y(-1)
    dn.a_send_y(1)
    dn.a_recv_z(2)
    dn.a_send_z(3)
    dn.b_recv_y(2)
    dn.b_send_z(1)
    dn.a_pass_y(0)
    dn.a_send_y(-2)
    dn.a_send_y(2)
    gu.a_pass_y(4)
    gu.b_recv_z(3)
    gu.b_send_z(4)
    dn.a_recv_z(3)
    dn.a_send_z(4)
    dn.a_send_y(-3)
    dn.a_send_y(3)
    dn.a_pass_y(-1)
    dn.a_pass_y(1)
    dn.a_recv_z(4)
    dn.a_send_y(4)
    for o in OFFSETS:
        gu.a_last_y(o)
    gu.b_recv_z(4)
    dn.b_recv_z(1)
    dn.b_send_z(2)

    @pl.loop(1, TP)
    def _(k):
        other, _ = tp_peer(k)
        ag_copy(k, other).wait_recv()

    rows = normed[...].reshape(T, D)
    second_part = dot(rows, gua[...].reshape(D, GUA))
    first_part = dot(rows, gub[...].reshape(D, GUB))
    hidden[:, 0:MAIN] = (jax.nn.silu(first_part) * second_part[:, 0:MAIN]).astype(BF16)
    tail_gate = second_part[:, MAIN : MAIN + FF - MAIN]
    tail_up = second_part[:, MAIN + FF - MAIN : GUA]
    tail = (jax.nn.silu(tail_gate) * tail_up).astype(BF16)
    hidden[:, MAIN:KPAD] = jnp.concatenate([tail, jnp.zeros((T, KPAD - FF), BF16)], axis=1)

    dn.a_pass_y(-2)
    dn.a_pass_y(2)
    dn.b_recv_z(2)
    dn.b_send_z(3)

    def fs_copy(zi, k, source):
        other, device = tp_peer(k)
        return pltpu.make_async_remote_copy(
            src_ref=ffn_send.at[zi, other], dst_ref=ffn_recv.at[zi, source],
            send_sem=fs_send.at[zi, other], recv_sem=fs_recv.at[zi, source],
            device_id=device, device_id_type=MESH)

    def product(o):
        zi = gu.zi(o)
        out = dot_nt(hidden[:, 0:DA], dna[zi].reshape(NY * ROWS, DA))
        out = out + dot_nt(hidden[:, DA:KPAD], dnb[zi].reshape(NY * ROWS, DB))
        ffn_send[zi] = out.astype(BF16).reshape(TP, TOK, NY * ROWS)

        @pl.loop(1, TP)
        def _(k):
            fs_copy(zi, k, tp).start()

    dn.a_last_y(0)
    product(0)
    dn.a_pass_y(-3)
    dn.a_pass_y(3)
    dn.a_pass_y(4)
    for o in (-1, 1):
        dn.a_last_y(o)
        product(o)
    dn.b_recv_z(3)
    dn.b_send_z(4)
    for o in (-2, 2, -3, 3):
        dn.a_last_y(o)
        product(o)
    dn.b_recv_z(4)
    dn.a_last_y(4)
    product(4)

    for zi in range(NZ):
        @pl.loop(1, TP)
        def _(k):
            other, _ = tp_peer(k)
            fs_copy(zi, k, other).wait_recv()

        at = slice(NY * ROWS * zi, NY * ROWS * (zi + 1))
        ffn_recv[zi, tp] = ffn_send[zi, tp]
        ffn = ffn_recv[zi, 0].astype(F32)
        for k in range(1, TP):
            ffn = ffn + ffn_recv[zi, k].astype(F32)
        result[:, at] = (resid[:, at] + 0.5 * ffn).astype(BF16)

    gu.drain()
    dn.drain()

    @pl.loop(1, SP)
    def _(k):
        carry_copy(k).wait_send()

    @pl.loop(1, TP)
    def _(k):
        rs_copy(k).wait_send()
        ag_copy(k, tp).wait_send()

        @pl.loop(0, NZ)
        def _(zi):
            fs_copy(zi, k, tp).wait_send()


def by_channel(maps):
    return jnp.swapaxes(maps, 2, 3).reshape(2 * CH, S)


def local(
    mix_input, stream, doc_ids, log_dt, decay_rate, frequency, input_real, input_imag,
    output_real, output_imag, skip_gain, log_keep, proj_weight, norm_gain, gate_weight,
    up_weight, down_weight,
):
    vmem = pl.BlockSpec(memory_space=pltpu.VMEM)
    smem = pl.BlockSpec(memory_space=pltpu.SMEM)
    specs = [vmem] * 3 + [smem] * 2 + [vmem] * 13
    dma = pltpu.SemaphoreType.DMA
    scratch = [
        pltpu.VMEM((NZ, NY, ROWS, GUA), BF16),
        pltpu.VMEM((NZ, NY, ROWS, GUB), BF16),
        pltpu.VMEM((NZ, NY, ROWS, DA), BF16),
        pltpu.VMEM((NZ, NY, ROWS, DB), BF16),
        pltpu.VMEM((T, 4 * W), F32),
        pltpu.VMEM((T, 2 * W), F32),
        pltpu.VMEM((T, 4 * W), F32),
        pltpu.VMEM((2, 16, 128), F32),
        pltpu.VMEM((SP, 16, 128), F32),
        pltpu.VMEM((TP, TOK, D), BF16),
        pltpu.VMEM((TP, TOK, D), BF16),
        pltpu.VMEM((TOK, D), F32),
        pltpu.VMEM((TP, TOK, D), BF16),
        pltpu.VMEM((T, KPAD), BF16),
        pltpu.VMEM((NZ, TP, TOK, NY * ROWS), BF16),
        pltpu.VMEM((NZ, TP, TOK, NY * ROWS), BF16),
        dma((2 * RELAYS,)), dma((2 * RELAYS,)),
        dma((SP,)), dma((SP,)),
        dma((TP,)), dma((TP,)),
        dma((TP,)), dma((TP,)),
        dma((NZ, TP)), dma((NZ, TP)),
    ]
    return pl.pallas_call(
        kernel,
        out_shape=jax.ShapeDtypeStruct((TOK, D), BF16),
        in_specs=specs,
        out_specs=vmem,
        scratch_shapes=scratch,
        compiler_params=pltpu.CompilerParams(
            collective_id=0, has_side_effects=True, vmem_limit_bytes=60 << 20
        ),
        name="layer",
    )(
        mix_input, stream, doc_ids.reshape(1, T), doc_ids, log_dt, decay_rate, frequency,
        by_channel(input_real), by_channel(input_imag),
        output_real.reshape(2 * CH, S), output_imag.reshape(2 * CH, S),
        skip_gain.reshape(1, CH), log_keep, proj_weight, norm_gain.reshape(1, D),
        gate_weight, up_weight, down_weight.T,
    )


def solution(mesh):
    torus = Mesh(mesh.devices.reshape(NZ, NY, NX, NC), ("z", "y", "x", "c"))
    sp, tp = ("z", "y"), ("x", "c")
    every = ("z", "y", "x", "c")
    in_specs = (
        P(sp, tp), P(every, None), P(sp), P(tp), P(tp, None), P(tp, None),
        P(None, tp, None, None), P(None, tp, None, None),
        P(None, tp, None, None), P(None, tp, None, None),
        P(tp), P(tp, sp), P(tp, None), P(), P(sp, tp), P(sp, tp), P(tp, sp),
    )
    return jax.shard_map(
        local, mesh=torus, in_specs=in_specs, out_specs=P(every, None), check_vma=False
    )
```

```python
import functools

import jax
import jax.numpy as jnp
from jax import lax
from jax.experimental import pallas as pl
from jax.experimental.pallas import tpu as pltpu
from jax.sharding import Mesh
from jax.sharding import PartitionSpec as P

HIGHEST = lax.Precision.HIGHEST
MESH = pl.DeviceIdType.MESH
F32, BF16 = jnp.float32, jnp.bfloat16

NZ, NY, NX, NC = 8, 4, 4, 2
SP, TP = NZ * NY, NX * NC
T, CH, G, S, GW = 256, 128, 8, 64, 16
W = G * S
CHUNKS = 8
STEPS = T // CHUNKS
D = 2048
FF = 704
MAIN = 640
ROWS = D // SP
TOK = T // TP
GUA, GUB = MAIN + 128, MAIN
DA, DB = 512, 256
KPAD = DA + DB
NT = (((1,), (1,)), ((), ()))


def dot(a, b, precision=None):
    return jnp.dot(a, b, preferred_element_type=F32, precision=precision)


def dot_nt(a, b, precision=None):
    return lax.dot_general(a, b, NT, preferred_element_type=F32, precision=precision)


def halves(value):
    high = value.astype(BF16)
    return high, (value - high.astype(F32)).astype(BF16)


def iota(shape, dim):
    return lax.broadcasted_iota(jnp.int32, shape, dim)


def one_hot(mask, dtype):
    return jnp.where(mask, 1.0, 0.0).astype(F32).astype(dtype)


def cmul(ar, ai, br, bi):
    return ar * br - ai * bi, ar * bi + ai * br


class Relay:
    def __init__(self, ra, rb, send, recv, z, y):
        self.ra, self.rb, self.send, self.recv = ra, rb, send, recv
        self.z, self.y = z, y

    def zi(self, offset):
        return lax.rem(self.z + (offset + NZ), NZ)

    def yi(self, offset):
        return lax.rem(self.y + (offset + NY), NY)

    def start(self, number, ref, axis, to):
        pltpu.make_async_remote_copy(
            src_ref=ref,
            dst_ref=ref,
            send_sem=self.send.at[0 if number < 20 else 1],
            recv_sem=self.recv.at[number],
            device_id={axis: self.zi(to) if axis == "z" else self.yi(to)},
            device_id_type=MESH,
        ).start()

    def wait(self, number, ref):
        pltpu.make_async_copy(ref, ref, self.recv.at[number]).wait()

    def a(self, dz, dy):
        return self.ra.at[self.zi(dz) * NY + self.yi(dy)]

    def send_az(self, d):
        for way in (1, -1):
            ref = self.a(-way * (d - 1), 0)
            if d == 4:
                ref = ref.at[pl.ds(0 if way > 0 else ROWS // 2, ROWS // 2)]
            self.start(d - 1, ref, "z", way)

    def send_ay(self, o):
        for way in (1, -1):
            self.start(4 + o % NZ, self.a(o, 0), "y", way)

    def az(self, d):
        self.wait(d - 1, self.ra.at[0] if d == 4 else self.ra.at[pl.ds(0, 2)])
        if d < 4:
            self.send_az(d + 1)
        for o in (4,) if d == 4 else (-d, d):
            self.send_ay(o)

    def ay(self, o):
        self.wait(4 + o % NZ, self.ra.at[pl.ds(0, 2)])
        way = 1 if o % 2 == 0 else -1
        self.start(12 + o % NZ, self.a(o, -way), "y", way)

    def al(self, o):
        self.wait(12 + o % NZ, self.ra.at[0])

    def send_by(self, d):
        for way in (1, -1):
            ref = self.rb.at[self.z * NY + self.yi(-way * (d - 1))]
            if d == 2:
                ref = ref.at[pl.ds(0 if way > 0 else ROWS // 2, ROWS // 2)]
            self.start(19 + d, ref, "y", way)

    def by(self, d):
        self.wait(19 + d, self.rb.at[pl.ds(0, 2)] if d == 1 else self.rb.at[0])
        if d == 1:
            self.send_by(2)
        else:
            self.send_bz(1)

    def send_bz(self, d):
        for way in (1, -1):
            first, count = self.zi(-way * (d - 1)) * NY, NY
            if d == 4:
                first, count = first + (0 if way > 0 else NY // 2), NY // 2
            self.start(21 + d, self.rb.at[pl.ds(first, count)], "z", way)

    def bz(self, d):
        self.wait(21 + d, self.rb.at[pl.ds(0, NY if d == 4 else 2 * NY)])
        if d < 4:
            self.send_bz(d + 1)

    def drain(self):
        for n, ref in enumerate((self.ra, self.rb)):
            part = ref.at[pl.ds(0, SP - 1)]
            pltpu.make_async_copy(part, part, self.send.at[n]).wait()


RECVS = 26
OFFSETS = (0, -1, 1, -2, 2, -3, 3, 4)
ORDER = (
    "gby 1", "gaz 1", "line", "gay 0", "gby 2", "gaz 2", "gay -1", "gay 1", "scan", "out",
    "gay -2", "share", "gbz 1", "gay 2", "down", "gaz 3", "dby 1", "pass", "day 0", "gay -3",
    "gbz 2", "daz 1", "gay 3", "dby 2", "last", "gaz 4", "proj", "day -1", "norm", "day 1",
    "gbz 3", "gay 4", "daz 2", "dbz 1", "day -2", "day 2", "gal 0", "gal -1", "gal 1", "gal -2",
    "gal 2", "gal -3", "gal 3", "gal 4", "gbz 4", "widen", "daz 3", "dal 0", "product 0",
    "dal -1", "product -1", "dal 1", "product 1", "dbz 2", "dal -2", "product -2", "dal 2",
    "product 2", "daz 4", "day -3", "day 3", "day 4", "dbz 3", "dal -3", "product -3", "dal 3",
    "product 3", "dbz 4", "dal 4", "product 4", "finish 0", "finish -1", "finish 1", "finish -2",
    "finish 2", "finish -3", "finish 3", "finish 4",
)


def row_of(block):
    return jnp.concatenate([block[g : g + 1, :] for g in range(G)], axis=1)


def rows_of(row):
    return jnp.concatenate([row[:, 128 * k : 128 * (k + 1)] for k in range(W // 128)], axis=0)


def flat_of(rows):
    return jnp.concatenate([rows[k : k + 1, :] for k in range(W // 128)], axis=1)


def kernel(
    mix, stream, docs, doc_scalar, log_dt, decay, freq, in_real, in_imag, out_real, out_imag,
    skip, log_keep, proj, gain, gate_w, up_w, down_w,
    result,
    gua, gub, dna, dnb, drive, factor, states, maps, line, message, column, shared, mixes,
    branch, resid, normed, hidden, ffn_send, ffn_recv,
    gu_send, gu_recv, dn_send, dn_recv, carry_sem, shared_sem, mix_sem, fs_send, fs_recv,
):
    z, y, x, c = (lax.axis_index(a) for a in ("z", "y", "x", "c"))
    sp, tp = z * NY + y, x * NC + c

    def tp_peer(k):
        other = lax.rem(tp + k, TP)
        return other, {"x": other // NC, "c": lax.rem(other, NC)}

    def at_z(k):
        return {"z": lax.rem(z + k, NZ)}

    def at_y(k):
        return {"y": lax.rem(y + k, NY)}

    def at_x(k):
        return {"x": lax.rem(x + k, NX)}

    sibling = {"c": 1 - c}

    barrier = pltpu.get_barrier_semaphore()

    def greet(device):
        pl.semaphore_signal(barrier, inc=1, device_id=device, device_id_type=MESH)

    for k in (1, 7, 2, 6, 3, 5, 4):
        greet(at_z(k))
    for k in (1, 3, 2):
        greet(at_y(k))
    for k in range(1, TP):
        greet(tp_peer(k)[1])

    def push(source, target, sems, n, device):
        pltpu.make_async_remote_copy(
            src_ref=source, dst_ref=target, send_sem=sems.at[0, n], recv_sem=sems.at[1, n],
            device_id=device, device_id_type=MESH).start()

    def take(ref, sem):
        pltpu.make_async_copy(ref, ref, sem).wait()

    gua[sp, :, 0:MAIN] = up_w[:, 0:MAIN]
    gua[sp, :, MAIN:GUA] = jnp.concatenate([gate_w[:, MAIN:FF], up_w[:, MAIN:FF]], axis=1)
    gub[sp] = gate_w[:, 0:MAIN]
    dna[sp] = down_w[:, 0:DA]
    dnb[sp] = jnp.concatenate([down_w[:, DA:FF], jnp.zeros((ROWS, KPAD - FF), BF16)], axis=1)

    shared[tp, 0:CH] = proj[...]
    shared[tp, CH : CH + TOK] = stream[...]

    group = iota((G, S), 0)
    steps = jnp.zeros((G, S), F32)
    for g in range(G):
        steps = jnp.where(group == g, log_dt[g], steps)
    steps = jnp.exp(steps)
    rate, turn_rate = decay[...], freq[...]
    magnitude = jnp.exp(-steps * rate)
    angle = steps * turn_rate
    a_real, a_imag = magnitude * jnp.cos(angle), magnitude * jnp.sin(angle)
    below = rate * rate + turn_rate * turn_rate
    shifted = a_real - 1.0
    z_real = (-shifted * rate + a_imag * turn_rate) / below
    z_imag = (-a_imag * rate - shifted * turn_rate) / below
    ar, ai, zr, zi = (row_of(v) for v in (a_real, a_imag, z_real, z_imag))

    r, t = iota((T, T), 0), iota((T, T), 1)
    order = t == lax.rem(r, CHUNKS) * STEPS + r // CHUNKS
    order_f = one_hot(order, F32)
    u = dot(order_f.astype(BF16), mix[...])
    ub = u.astype(BF16)

    tile = one_hot(lax.rem(iota((S, W), 1), S) == iota((S, W), 0), BF16)
    own = lax.rem(iota((2 * CH, W), 0), CH) // GW == iota((2 * CH, W), 1) // S
    for n, ref in enumerate((in_real, in_imag)):
        high, low = (
            jnp.where(own, dot(half, tile), 0.0).astype(BF16) for half in halves(ref[...])
        )
        for d in range(2):
            at = slice(CH * d, CH * (d + 1))
            drive[:, W * (2 * n + d) : W * (2 * n + d + 1)] = dot(ub, high[at]) + dot(ub, low[at])

    doc = docs[...].astype(F32) + jnp.zeros((G, T), F32)
    place = iota((G, T), 1)
    before, after = pltpu.roll(doc, 1, 1), pltpu.roll(doc, T - 1, 1)
    keep = jnp.exp(log_keep[...])
    keep_f = jnp.where((place == 0) | (doc == before), keep, 0.0)
    keep_b = jnp.where((place == T - 1) | (doc == after), keep, 0.0)
    both = dot_nt(order_f, jnp.concatenate([keep_f, keep_b], axis=0), HIGHEST)
    spread = one_hot(iota((2 * G, 2 * W), 0) == iota((2 * G, 2 * W), 1) // S, F32)
    factor[...] = dot(both, spread, HIGHEST)

    zero = jnp.zeros((CHUNKS, W), F32)
    ar8, ai8 = zero + ar, zero + ai

    def advance(j, state, direction):
        at = pl.ds(pl.multiple_of(j * CHUNKS, CHUNKS), CHUNKS)
        f = factor[at, W * direction : W * (direction + 1)]
        dr = drive[at, W * direction : W * (direction + 1)]
        di = drive[at, W * (2 + direction) : W * (3 + direction)]
        hr, hi = state
        nr, ni = cmul(f * ar8, f * ai8, hr, hi)
        return f, nr + dr, ni + di

    def first(j, state):
        fr, fi, fp, br, bi, bp = state
        f, fr, fi = advance(j, (fr, fi), 0)
        b, br, bi = advance(STEPS - 1 - j, (br, bi), 1)
        return fr, fi, fp * f, br, bi, bp * b

    fr, fi, fp, br, bi, bp = lax.fori_loop(
        0, STEPS, first, (zero, zero, zero + 1.0, zero, zero, zero + 1.0)
    )
    pr, pi = ar, ai
    for _ in range(5):
        pr, pi = cmul(pr, pi, pr, pi)

    def chunk_entries(enter, hr, hi, passed, backward):
        er, ei = enter
        entries = [None] * CHUNKS
        chunks = range(CHUNKS - 1, -1, -1) if backward else range(CHUNKS)
        for k in chunks:
            entries[k] = (er, ei)
            f = passed[k : k + 1]
            nr, ni = cmul(f * pr, f * pi, er, ei)
            er, ei = nr + hr[k : k + 1], ni + hi[k : k + 1]
        return entries, (er, ei)

    none = (jnp.zeros((1, W), F32), jnp.zeros((1, W), F32))
    end_f = chunk_entries(none, fr, fi, fp, False)[1]
    end_b = chunk_entries(none, br, bi, bp, True)[1]
    passed = fp[0:1]
    for k in range(1, CHUNKS):
        passed = passed * fp[k : k + 1]
    qr, qi = pr, pi
    for _ in range(3):
        qr, qi = cmul(qr, qi, qr, qi)
    edge_first = doc_scalar[0].astype(F32)
    edge_last = doc_scalar[T - 1].astype(F32)
    passed_rows = rows_of(passed)
    edges = jnp.concatenate(
        [jnp.full((1, 128), edge_first, F32), jnp.full((1, 128), edge_last, F32),
         jnp.zeros((2, 128), F32)], axis=0)
    for n, (er, ei) in enumerate((end_f, end_b)):
        line[y, 8 * n : 8 * n + 4] = rows_of(er)
        line[y, 8 * n + 4 : 8 * n + 8] = rows_of(ei)
    line[y, 16:20] = passed_rows
    line[y, 20:24] = edges

    gu = Relay(gua, gub, gu_send, gu_recv, z, y)
    dn = Relay(dna, dnb, dn_send, dn_recv, z, y)

    pl.semaphore_wait(barrier, NZ - 1 + NY - 1 + TP - 1)
    gu.send_by(1)
    gu.send_az(1)
    for k in (2, 1, 3):
        push(line.at[y], line.at[y], carry_sem, 0, at_y(k))
    for k in (1, 3):
        push(shared.at[tp], shared.at[tp], shared_sem, 0, at_x(k))
    gu.send_ay(0)
    push(shared.at[tp], shared.at[tp], shared_sem, 2, sibling)

    tile = tile.astype(F32)
    cr = jnp.where(own, dot(out_real[...], tile, HIGHEST), 0.0)
    ci = jnp.where(own, dot(out_imag[...], tile, HIGHEST), 0.0)
    cr, ci = cmul(zr, zi, cr, ci)
    for n in range(4):
        read = (cr if n < 2 else -ci)[CH * (n % 2) : CH * (n % 2 + 1)]
        maps[0, n], maps[1, n] = halves(read)

    q4r, q4i = rows_of(qr), rows_of(qi)
    s4r, s4i = cmul(q4r, q4i, q4r, q4i)
    s4r, s4i = cmul(s4r, s4i, s4r, s4i)
    four = jnp.zeros((4, 128), F32)
    start = (four, four, jnp.zeros((1, 128), F32) - 1.0)

    def fold(state, m, side, power, passed, near, far, use):
        cr, ci, last = state
        link = jnp.where(m[near : near + 1] == last, 1.0, 0.0) * m[passed : passed + 4]
        nr, ni = cmul(link * power[0], link * power[1], cr, ci)
        cr = jnp.where(use, nr + m[side : side + 4], cr)
        ci = jnp.where(use, ni + m[side + 4 : side + 8], ci)
        return cr, ci, jnp.where(use, m[far : far + 1], last)

    def fold_line(state, backward, use):
        for k in range(NY - 1, -1, -1) if backward else range(NY):
            m = line[k]
            if backward:
                state = fold(state, m, 8, (q4r, q4i), 16, 21, 20, use(k))
            else:
                state = fold(state, m, 0, (q4r, q4i), 16, 20, 21, use(k))
        return state

    def carry_line():
        take(line.at[pl.ds(0, NY - 1)], carry_sem.at[1, 0])
        always = lambda k: k >= 0
        ends = fold_line(start, False, always), fold_line(start, True, always)
        passed = line[0][16:20]
        for k in range(1, NY):
            link = jnp.where(line[k][20:21] == line[k - 1][21:22], 1.0, 0.0)
            passed = passed * (link * line[k][16:20])
        edges = jnp.concatenate(
            [line[0][20:21], line[NY - 1][21:22], jnp.zeros((2, 128), F32)], axis=0)
        for n in range(2):
            message[n, 0:4] = ends[n][0]
            message[n, 4:8] = ends[n][1]
            message[n, 8:12] = passed
            message[n, 12:16] = edges
        column[z] = message[0]
        for k in (4, 3, 5, 2, 6, 1, 7):
            side = jnp.where(lax.rem(z + k, NZ) > z, 0, 1)
            push(message.at[side], column.at[z], carry_sem, 1, at_z(k))

    def carry_column():
        take(column.at[pl.ds(0, NZ - 1)], carry_sem.at[1, 1])
        forward, backward = start, start
        for k in range(NZ):
            forward = fold(forward, column[k], 0, (s4r, s4i), 8, 12, 13, k < z)
            j = NZ - 1 - k
            backward = fold(backward, column[j], 0, (s4r, s4i), 8, 13, 12, j > z)
        into_f = fold_line(forward, False, lambda k: k < y)
        into_b = fold_line(backward, True, lambda k: k > y)
        enter_f = jnp.where(into_f[2] == edge_first, 1.0, 0.0)
        enter_b = jnp.where(into_b[2] == edge_last, 1.0, 0.0)
        enter_f = (flat_of(into_f[0] * enter_f), flat_of(into_f[1] * enter_f))
        enter_b = (flat_of(into_b[0] * enter_b), flat_of(into_b[1] * enter_b))
        entries_f = chunk_entries(enter_f, fr, fi, fp, False)[0]
        entries_b = chunk_entries(enter_b, br, bi, bp, True)[0]
        return tuple(
            jnp.concatenate([e[part_no] for e in entries], axis=0)
            for entries in (entries_f, entries_b) for part_no in (0, 1)
        )

    def second(j, state):
        fr, fi, br, bi = state
        _, fr, fi = advance(j, (fr, fi), 0)
        k = STEPS - 1 - j
        _, br, bi = advance(k, (br, bi), 1)
        at = pl.ds(pl.multiple_of(j * CHUNKS, CHUNKS), CHUNKS)
        states[at, 0:W] = fr
        states[at, 2 * W : 3 * W] = fi
        at = pl.ds(pl.multiple_of(k * CHUNKS, CHUNKS), CHUNKS)
        states[at, W : 2 * W] = br
        states[at, 3 * W : 4 * W] = bi
        return fr, fi, br, bi

    def scan():
        lax.fori_loop(0, STEPS, second, carry_column())

    def mix_out():
        pre = skip[...] * u
        for n in range(4):
            high, low = halves(states[:, W * n : W * (n + 1)])
            pre = pre + dot_nt(high, maps[0, n]) + dot_nt(high, maps[1, n])
            pre = pre + dot_nt(low, maps[0, n])
        mixed = jax.nn.gelu(pre).astype(BF16)
        back = one_hot(t == lax.rem(r, STEPS) * CHUNKS + r // STEPS, BF16)
        mixes[tp] = dot(back, mixed).astype(BF16)
        for k in (2, 1, 3):
            push(mixes.at[tp], mixes.at[tp], mix_sem, 0, at_x(k))
        push(mixes.at[tp], mixes.at[tp], mix_sem, 1, sibling)

    def of_x(k):
        return lax.rem(x + k, NX) * NC + c

    def share():
        take(shared.at[pl.ds(0, 2)], shared_sem.at[1, 0])
        half = (CH + TOK) // 2
        for k, first in ((1, half), (3, 0)):
            ref = shared.at[of_x(k), pl.ds(first, half)]
            push(ref, ref, shared_sem, 1, at_x(NX - k))
        for k in (1, 3):
            push(shared.at[of_x(k)], shared.at[of_x(k)], shared_sem, 2, sibling)

    def share_last():
        take(shared.at[0], shared_sem.at[1, 1])
        push(shared.at[of_x(2)], shared.at[of_x(2)], shared_sem, 2, sibling)

    def mix_pass():
        take(mixes.at[pl.ds(0, 3)], mix_sem.at[1, 0])
        for k in (1, 2, 3):
            push(mixes.at[of_x(k)], mixes.at[of_x(k)], mix_sem, 1, sibling)

    def project():
        take(shared.at[pl.ds(0, 4)], shared_sem.at[1, 2])
        take(mixes.at[pl.ds(0, 4)], mix_sem.at[1, 1])
        both = jnp.concatenate([mixes[k] for k in range(TP)], axis=1)
        branch[...] = dot(both, shared[:, 0:CH].reshape(TP * CH, D))

    def normalize():
        scales = gain[...]
        resid[...] = stream[...].astype(F32) + branch[pl.ds(pl.multiple_of(tp * TOK, TOK), TOK)]

        @pl.loop(0, TP)
        def _(k):
            at = pl.ds(pl.multiple_of(k * TOK, TOK), TOK)
            kept = shared[k, CH : CH + TOK].astype(F32) + branch[at]
            scale = lax.rsqrt(jnp.mean(kept * kept, axis=-1, keepdims=True) + 1e-6)
            normed[at] = (kept * scale * scales).astype(BF16)

    def widen():
        rows = normed[...]
        second_part = dot(rows, gua[...].reshape(D, GUA))
        first_part = dot(rows, gub[...].reshape(D, GUB))
        hidden[:, 0:MAIN] = (jax.nn.silu(first_part) * second_part[:, 0:MAIN]).astype(BF16)
        tail_gate = second_part[:, MAIN:FF]
        tail_up = second_part[:, FF:GUA]
        tail = (jax.nn.silu(tail_gate) * tail_up).astype(BF16)
        hidden[:, MAIN:KPAD] = jnp.concatenate([tail, jnp.zeros((T, KPAD - FF), BF16)], axis=1)

    def down_start():
        dn.send_by(1)
        dn.send_az(1)
        dn.send_ay(0)

    def product(o):
        zi = gu.zi(o)
        at = pl.ds(zi * NY, NY)
        out = dot_nt(hidden[:, 0:DA], dna[at].reshape(NY * ROWS, DA))
        out = out + dot_nt(hidden[:, DA:KPAD], dnb[at].reshape(NY * ROWS, DB))
        ffn_send[zi] = out.astype(BF16).reshape(TP, TOK, NY * ROWS)
        ffn_recv[zi, tp] = ffn_send[zi, tp]

        @pl.loop(1, TP)
        def _(k):
            other, device = tp_peer(k)
            pltpu.make_async_remote_copy(
                src_ref=ffn_send.at[zi, other], dst_ref=ffn_recv.at[zi, tp],
                send_sem=fs_send.at[0], recv_sem=fs_recv.at[zi],
                device_id=device, device_id_type=MESH).start()

    def finish(o):
        zi = gu.zi(o)
        take(ffn_recv.at[zi, pl.ds(0, TP - 1)], fs_recv.at[zi])
        at = pl.ds(pl.multiple_of(zi * (NY * ROWS), NY * ROWS), NY * ROWS)
        ffn = ffn_recv[zi, 0].astype(F32)
        for k in range(1, TP):
            ffn = ffn + ffn_recv[zi, k].astype(F32)
        result[:, at] = (resid[:, at] + 0.5 * ffn).astype(BF16)

    steps = {
        "line": carry_line, "scan": scan, "out": mix_out, "share": share, "last": share_last,
        "pass": mix_pass, "proj": project, "norm": normalize, "widen": widen, "down": down_start,
        "product": product, "finish": finish,
    }
    for step in ORDER:
        name, number = step.split()[0], [int(n) for n in step.split()[1:]]
        if name[0] in "gd" and name[1:] in ("az", "ay", "al", "by", "bz"):
            getattr(gu if name[0] == "g" else dn, name[1:])(*number)
        else:
            steps[name](*number)

    gu.drain()
    dn.drain()
    take(line.at[pl.ds(0, NY - 1)], carry_sem.at[0, 0])
    take(column.at[pl.ds(0, NZ - 1)], carry_sem.at[0, 1])
    take(shared.at[pl.ds(0, 2)], shared_sem.at[0, 0])
    take(shared.at[0], shared_sem.at[0, 1])
    take(shared.at[pl.ds(0, 4)], shared_sem.at[0, 2])
    take(mixes.at[pl.ds(0, 3)], mix_sem.at[0, 0])
    take(mixes.at[pl.ds(0, 4)], mix_sem.at[0, 1])
    take(ffn_recv.at[pl.ds(0, TP - 1)], fs_send.at[0])


def by_channel(maps):
    return jnp.swapaxes(maps, 2, 3).reshape(2 * CH, S)


def local(
    mix_input, stream, doc_ids, log_dt, decay_rate, frequency, input_real, input_imag,
    output_real, output_imag, skip_gain, log_keep, proj_weight, norm_gain, gate_weight,
    up_weight, down_weight,
):
    vmem = pl.BlockSpec(memory_space=pltpu.VMEM)
    smem = pl.BlockSpec(memory_space=pltpu.SMEM)
    specs = [vmem] * 3 + [smem] * 2 + [vmem] * 13
    dma = pltpu.SemaphoreType.DMA
    scratch = [
        pltpu.VMEM((SP, ROWS, GUA), BF16),
        pltpu.VMEM((SP, ROWS, GUB), BF16),
        pltpu.VMEM((SP, ROWS, DA), BF16),
        pltpu.VMEM((SP, ROWS, DB), BF16),
        pltpu.VMEM((T, 4 * W), F32),
        pltpu.VMEM((T, 2 * W), F32),
        pltpu.VMEM((T, 4 * W), F32),
        pltpu.VMEM((2, 4, CH, W), BF16),
        pltpu.VMEM((NY, 24, 128), F32),
        pltpu.VMEM((2, 16, 128), F32),
        pltpu.VMEM((NZ, 16, 128), F32),
        pltpu.VMEM((TP, CH + TOK, D), BF16),
        pltpu.VMEM((TP, T, CH), BF16),
        pltpu.VMEM((T, D), F32),
        pltpu.VMEM((TOK, D), F32),
        pltpu.VMEM((T, D), BF16),
        pltpu.VMEM((T, KPAD), BF16),
        pltpu.VMEM((NZ, TP, TOK, NY * ROWS), BF16),
        pltpu.VMEM((NZ, TP, TOK, NY * ROWS), BF16),
        dma((2,)), dma((RECVS,)), dma((2,)), dma((RECVS,)),
        dma((2, 2)), dma((2, 3)), dma((2, 2)), dma((1,)), dma((NZ,)),
    ]
    return pl.pallas_call(
        kernel,
        out_shape=jax.ShapeDtypeStruct((TOK, D), BF16),
        in_specs=specs,
        out_specs=vmem,
        scratch_shapes=scratch,
        compiler_params=pltpu.CompilerParams(
            collective_id=0, has_side_effects=True, vmem_limit_bytes=60 << 20
        ),
        name="layer",
    )(
        mix_input, stream, doc_ids.reshape(1, T), doc_ids, log_dt, decay_rate, frequency,
        by_channel(input_real), by_channel(input_imag),
        output_real.reshape(2 * CH, S), output_imag.reshape(2 * CH, S),
        skip_gain.reshape(1, CH), log_keep, proj_weight, norm_gain.reshape(1, D),
        gate_weight, up_weight, down_weight.T,
    )


def solution(mesh):
    torus = Mesh(mesh.devices.reshape(NZ, NY, NX, NC), ("z", "y", "x", "c"))
    sp, tp = ("z", "y"), ("x", "c")
    every = ("z", "y", "x", "c")
    in_specs = (
        P(sp, tp), P(every, None), P(sp), P(tp), P(tp, None), P(tp, None),
        P(None, tp, None, None), P(None, tp, None, None),
        P(None, tp, None, None), P(None, tp, None, None),
        P(tp), P(tp, sp), P(tp, None), P(), P(sp, tp), P(sp, tp), P(tp, sp),
    )
    return jax.shard_map(
        local, mesh=torus, in_specs=in_specs, out_specs=P(every, None), check_vma=False
    )
```

```python
import functools

import jax
import jax.numpy as jnp
from jax import lax
from jax.experimental import pallas as pl
from jax.experimental.pallas import tpu as pltpu
from jax.sharding import Mesh
from jax.sharding import PartitionSpec as P

HIGHEST = lax.Precision.HIGHEST
MESH = pl.DeviceIdType.MESH
F32, BF16 = jnp.float32, jnp.bfloat16

NZ, NY, NX, NC = 8, 4, 4, 2
SP, TP = NZ * NY, NX * NC
T, CH, G, S, GW = 256, 128, 8, 64, 16
W = G * S
CHUNKS = 8
STEPS = T // CHUNKS
D = 2048
FF = 704
MAIN = 640
ROWS = D // SP
TOK = T // TP
GUA, GUB = MAIN + 128, MAIN
DA, DB = 512, 128
DROWS = ROWS + ROWS // 2
KPAD = MAIN + 256
NT = (((1,), (1,)), ((), ()))


def dot(a, b, precision=None):
    return jnp.dot(a, b, preferred_element_type=F32, precision=precision)


def dot_nt(a, b, precision=None):
    return lax.dot_general(a, b, NT, preferred_element_type=F32, precision=precision)


def halves(value):
    high = value.astype(BF16)
    return high, (value - high.astype(F32)).astype(BF16)


def iota(shape, dim):
    return lax.broadcasted_iota(jnp.int32, shape, dim)


def one_hot(mask, dtype):
    return jnp.where(mask, 1.0, 0.0).astype(F32).astype(dtype)


def cmul(ar, ai, br, bi):
    return ar * br - ai * bi, ar * bi + ai * br


class Relay:
    def __init__(self, ra, rb, send, recv, z, y):
        self.ra, self.rb, self.send, self.recv = ra, rb, send, recv
        self.z, self.y = z, y

    def zi(self, offset):
        return lax.rem(self.z + (offset + NZ), NZ)

    def yi(self, offset):
        return lax.rem(self.y + (offset + NY), NY)

    def start(self, number, ref, axis, to):
        pltpu.make_async_remote_copy(
            src_ref=ref,
            dst_ref=ref,
            send_sem=self.send.at[0 if number < 20 else 1],
            recv_sem=self.recv.at[number],
            device_id={axis: self.zi(to) if axis == "z" else self.yi(to)},
            device_id_type=MESH,
        ).start()

    def wait(self, number, ref):
        pltpu.make_async_copy(ref, ref, self.recv.at[number]).wait()

    def a(self, dz, dy):
        return self.ra.at[self.zi(dz) * NY + self.yi(dy)]

    def send_az(self, d):
        for way in (1, -1):
            ref = self.a(-way * (d - 1), 0)
            if d == 4:
                ref = self.half(ref, way)
            self.start(d - 1, ref, "z", way)

    def send_ay(self, o):
        for way in (1, -1):
            self.start(4 + o % NZ, self.a(o, 0), "y", way)

    def az(self, d):
        self.wait(d - 1, self.ra.at[0] if d == 4 else self.ra.at[pl.ds(0, 2)])
        if d < 4:
            self.send_az(d + 1)
        for o in (4,) if d == 4 else (-d, d):
            self.send_ay(o)

    def ay(self, o):
        self.wait(4 + o % NZ, self.ra.at[pl.ds(0, 2)])
        way = 1 if o % 2 == 0 else -1
        self.start(12 + o % NZ, self.a(o, -way), "y", way)

    def al(self, o):
        self.wait(12 + o % NZ, self.ra.at[0])

    def send_by(self, d):
        for way in (1, -1):
            ref = self.rb.at[self.z * NY + self.yi(-way * (d - 1))]
            if d == 2:
                ref = self.half(ref, way)
            self.start(19 + d, ref, "y", way)

    def by(self, d):
        self.wait(19 + d, self.rb.at[pl.ds(0, 2)] if d == 1 else self.rb.at[0])
        if d == 1:
            self.send_by(2)
        self.send_bz(1, d)

    def send_bz(self, d, j):
        for way in (1, -1):
            first = self.zi(-way * (d - 1)) * NY
            for dy in ((0,), (1, -1), (2,))[j]:
                if d == 4 and dy == -way:
                    continue
                ref = self.rb.at[first + self.yi(dy)]
                if d == 4 and j != 1:
                    ref = self.half(ref, way)
                self.start(19 + 3 * d + j, ref, "z", way)

    def bz(self, d, j):
        count = (2 if j == 1 else 1) * (1 if d == 4 else 2)
        self.wait(19 + 3 * d + j, self.rb.at[pl.ds(0, count)])
        if d < 4:
            self.send_bz(d + 1, j)

    def half(self, ref, way):
        rows = ref.shape[0] // 2
        return ref.at[pl.ds(0 if way > 0 else rows, rows)]

    def drain(self):
        for n, ref in enumerate((self.ra, self.rb)):
            part = ref.at[pl.ds(0, SP - 1)]
            pltpu.make_async_copy(part, part, self.send.at[n]).wait()


RECVS = 34
OFFSETS = (0, -1, 1, -2, 2, -3, 3, 4)
ORDER = (
    "maps", "gby 1", "gaz 1", "line", "gbz 1 0", "gay 0", "gby 2", "gbz 1 1", "gay -1", "gaz 2",
    "gay 1", "downz", "scan", "gbz 2 0", "out", "share", "gbz 1 2", "gay -2", "gay 2", "gbz 2 1",
    "downy", "gaz 3", "daz 1", "dbz 1 0", "pass", "dby 1", "gbz 3 0", "day 0", "gbz 2 2",
    "gay -3", "gay 3", "gbz 3 1", "last", "day -1", "gaz 4", "day 1", "daz 2", "dby 2", "proj",
    "dbz 2 0", "dbz 1 1", "norm", "gbz 3 2", "gay 4", "daz 3", "day -2", "dbz 1 2", "dbz 3 0",
    "day 2", "dbz 2 1", "gal 0", "gal -1", "gal 1", "gal -2", "gal 2", "gal -3", "gal 3", "gal 4",
    "gbz 4 0", "gbz 4 1", "gbz 4 2", "widen", "daz 4", "dbz 2 2", "day -3", "dal 0", "product 0",
    "dal -1", "product -1", "dal 1", "product 1", "day 3", "dbz 3 1", "combine 0", "dal -2",
    "product -2", "combine -1", "dal 2", "product 2", "combine 1", "combine -2", "dbz 3 2",
    "combine 2", "day 4", "dal -3", "product -3", "dal 3", "product 3", "combine -3", "combine 3",
    "dbz 4 0", "dbz 4 1", "dbz 4 2", "dal 4", "product 4", "combine 4", "finish 0", "finish -1",
    "finish 1", "finish -2", "finish 2", "finish -3", "finish 3", "finish 4",
)


def row_of(block):
    return jnp.concatenate([block[g : g + 1, :] for g in range(G)], axis=1)


def rows_of(row):
    return jnp.concatenate([row[:, 128 * k : 128 * (k + 1)] for k in range(W // 128)], axis=0)


def flat_of(rows):
    return jnp.concatenate([rows[k : k + 1, :] for k in range(W // 128)], axis=1)


def kernel(
    mix_hbm, stream_hbm, docs, doc_scalar, log_dt, decay, freq, in_real_hbm, in_imag_hbm,
    out_real_hbm, out_imag_hbm, skip, keep_hbm, proj_hbm, gain, gate_hbm, up_hbm, down_hbm,
    result,
    mix, stream, in_real, in_imag, out_real, out_imag, log_keep, gate_w, up_w, down_w,
    gua, gub, dna, dnb, drive, factor, states, maps, line, message, column, shared, mixes,
    branch, resid, normed, hidden, ffn_part, ffn_pair, ffn_send, ffn_recv,
    gu_send, gu_recv, dn_send, dn_recv, carry_sem, shared_sem, mix_sem, pair_sem, fs_send, fs_recv, load_sem,
):
    z, y, x, c = (lax.axis_index(a) for a in ("z", "y", "x", "c"))
    sp, tp = z * NY + y, x * NC + c

    def tp_peer(k):
        other = lax.rem(tp + k, TP)
        return other, {"x": other // NC, "c": lax.rem(other, NC)}

    def at_z(k):
        return {"z": lax.rem(z + k, NZ)}

    def at_y(k):
        return {"y": lax.rem(y + k, NY)}

    def at_x(k):
        return {"x": lax.rem(x + k, NX)}

    sibling = {"c": 1 - c}

    barrier = pltpu.get_barrier_semaphore()

    def greet(device):
        pl.semaphore_signal(barrier, inc=1, device_id=device, device_id_type=MESH)

    for k in (1, 7, 2, 6, 3, 5, 4):
        greet(at_z(k))
    for k in (1, 3, 2):
        greet(at_y(k))
    for k in range(1, TP):
        greet(tp_peer(k)[1])

    def push(source, target, sems, n, device):
        pltpu.make_async_remote_copy(
            src_ref=source, dst_ref=target, send_sem=sems.at[0, n], recv_sem=sems.at[1, n],
            device_id=device, device_id_type=MESH).start()

    def take(ref, sem):
        pltpu.make_async_copy(ref, ref, sem).wait()

    loads = []

    def load(source, target):
        loads.append(pltpu.make_async_copy(source, target, load_sem.at[len(loads)]))
        loads[-1].start()
        return loads[-1]

    gate_load = load(gate_hbm, gate_w)
    up_load = load(up_hbm, up_w)
    first_loads = [
        load(gate_hbm.at[:, pl.ds(0, MAIN)], gub.at[sp]),
        load(up_hbm.at[:, pl.ds(0, MAIN)], gua.at[sp, :, pl.ds(0, MAIN)]),
    ]
    scan_loads = [load(mix_hbm, mix), load(keep_hbm, log_keep)]
    scan_loads += [load(in_real_hbm, in_real), load(in_imag_hbm, in_imag)]
    share_loads = [
        load(proj_hbm, shared.at[tp, pl.ds(0, CH)]),
        load(stream_hbm, shared.at[tp, pl.ds(CH, TOK)]),
    ]
    map_loads = [
        load(out_real_hbm, out_real),
        load(out_imag_hbm, out_imag),
        load(stream_hbm, stream),
        load(down_hbm, down_w),
        load(down_hbm.at[:, pl.ds(0, DA)], dna.at[sp]),
        load(down_hbm.at[:, pl.ds(DA, DB)], dnb.at[sp, pl.ds(0, ROWS)]),
    ]
    gate_load.wait()
    up_load.wait()
    gua[sp, :, MAIN:GUA] = jnp.concatenate([gate_w[:, MAIN:FF], up_w[:, MAIN:FF]], axis=1)

    group = iota((G, S), 0)
    steps = jnp.zeros((G, S), F32)
    for g in range(G):
        steps = jnp.where(group == g, log_dt[g], steps)
    steps = jnp.exp(steps)
    rate, turn_rate = decay[...], freq[...]
    magnitude = jnp.exp(-steps * rate)
    angle = steps * turn_rate
    a_real, a_imag = magnitude * jnp.cos(angle), magnitude * jnp.sin(angle)
    below = rate * rate + turn_rate * turn_rate
    shifted = a_real - 1.0
    z_real = (-shifted * rate + a_imag * turn_rate) / below
    z_imag = (-a_imag * rate - shifted * turn_rate) / below
    ar, ai, zr, zi = (row_of(v) for v in (a_real, a_imag, z_real, z_imag))

    gu = Relay(gua, gub, gu_send, gu_recv, z, y)
    dn = Relay(dna, dnb, dn_send, dn_recv, z, y)
    for wait in first_loads:
        wait.wait()
    pl.semaphore_wait(barrier, NZ - 1 + NY - 1 + TP - 1)
    gu.send_by(1)
    gu.send_az(1)
    gu.send_bz(1, 0)
    for wait in share_loads:
        wait.wait()
    for k in (1, 3):
        push(shared.at[tp], shared.at[tp], shared_sem, 0, at_x(k))
    push(shared.at[tp], shared.at[tp], shared_sem, 2, sibling)
    for wait in scan_loads:
        wait.wait()

    r, t = iota((T, T), 0), iota((T, T), 1)
    order = t == lax.rem(r, CHUNKS) * STEPS + r // CHUNKS
    order_f = one_hot(order, F32)
    u = dot(order_f.astype(BF16), mix[...])
    ub = u.astype(BF16)

    tile = one_hot(lax.rem(iota((S, W), 1), S) == iota((S, W), 0), BF16)
    own = lax.rem(iota((2 * CH, W), 0), CH) // GW == iota((2 * CH, W), 1) // S
    for n, ref in enumerate((in_real, in_imag)):
        high, low = (
            jnp.where(own, dot(half, tile), 0.0).astype(BF16) for half in halves(ref[...])
        )
        for d in range(2):
            at = slice(CH * d, CH * (d + 1))
            drive[:, W * (2 * n + d) : W * (2 * n + d + 1)] = dot(ub, high[at]) + dot(ub, low[at])

    doc = docs[...].astype(F32) + jnp.zeros((G, T), F32)
    place = iota((G, T), 1)
    before, after = pltpu.roll(doc, 1, 1), pltpu.roll(doc, T - 1, 1)
    keep = jnp.exp(log_keep[...])
    keep_f = jnp.where((place == 0) | (doc == before), keep, 0.0)
    keep_b = jnp.where((place == T - 1) | (doc == after), keep, 0.0)
    both = dot_nt(order_f, jnp.concatenate([keep_f, keep_b], axis=0), HIGHEST)
    spread = one_hot(iota((2 * G, 2 * W), 0) == iota((2 * G, 2 * W), 1) // S, F32)
    factor[...] = dot(both, spread, HIGHEST)

    zero = jnp.zeros((CHUNKS, W), F32)
    ar8, ai8 = zero + ar, zero + ai

    def advance(j, state, direction):
        at = pl.ds(pl.multiple_of(j * CHUNKS, CHUNKS), CHUNKS)
        f = factor[at, W * direction : W * (direction + 1)]
        dr = drive[at, W * direction : W * (direction + 1)]
        di = drive[at, W * (2 + direction) : W * (3 + direction)]
        hr, hi = state
        nr, ni = cmul(f * ar8, f * ai8, hr, hi)
        return f, nr + dr, ni + di

    def first(j, state):
        fr, fi, fp, br, bi, bp = state
        f, fr, fi = advance(j, (fr, fi), 0)
        b, br, bi = advance(STEPS - 1 - j, (br, bi), 1)
        return fr, fi, fp * f, br, bi, bp * b

    fr, fi, fp, br, bi, bp = lax.fori_loop(
        0, STEPS, first, (zero, zero, zero + 1.0, zero, zero, zero + 1.0)
    )
    pr, pi = ar, ai
    for _ in range(5):
        pr, pi = cmul(pr, pi, pr, pi)

    def chunk_entries(enter, hr, hi, passed, backward):
        er, ei = enter
        entries = [None] * CHUNKS
        chunks = range(CHUNKS - 1, -1, -1) if backward else range(CHUNKS)
        for k in chunks:
            entries[k] = (er, ei)
            f = passed[k : k + 1]
            nr, ni = cmul(f * pr, f * pi, er, ei)
            er, ei = nr + hr[k : k + 1], ni + hi[k : k + 1]
        return entries, (er, ei)

    none = (jnp.zeros((1, W), F32), jnp.zeros((1, W), F32))
    end_f = chunk_entries(none, fr, fi, fp, False)[1]
    end_b = chunk_entries(none, br, bi, bp, True)[1]
    passed = fp[0:1]
    for k in range(1, CHUNKS):
        passed = passed * fp[k : k + 1]
    qr, qi = pr, pi
    for _ in range(3):
        qr, qi = cmul(qr, qi, qr, qi)
    edge_first = doc_scalar[0].astype(F32)
    edge_last = doc_scalar[T - 1].astype(F32)
    passed_rows = rows_of(passed)
    edges = jnp.concatenate(
        [jnp.full((1, 128), edge_first, F32), jnp.full((1, 128), edge_last, F32),
         jnp.zeros((2, 128), F32)], axis=0)
    for n, (er, ei) in enumerate((end_f, end_b)):
        line[y, 8 * n : 8 * n + 4] = rows_of(er)
        line[y, 8 * n + 4 : 8 * n + 8] = rows_of(ei)
    line[y, 16:20] = passed_rows
    line[y, 20:24] = edges

    for k in (2, 1, 3):
        push(line.at[y], line.at[y], carry_sem, 0, at_y(k))
    gu.send_ay(0)

    def output_maps():
        for wait in map_loads:
            wait.wait()
        spread = tile.astype(F32)
        cr = jnp.where(own, dot(out_real[...], spread, HIGHEST), 0.0)
        ci = jnp.where(own, dot(out_imag[...], spread, HIGHEST), 0.0)
        cr, ci = cmul(zr, zi, cr, ci)
        for n in range(4):
            read = (cr if n < 2 else -ci)[CH * (n % 2) : CH * (n % 2 + 1)]
            maps[0, n], maps[1, n] = halves(read)
        rest = down_w[:, MAIN:FF]
        dnb[sp, ROWS:DROWS] = jnp.concatenate([rest[: ROWS // 2], rest[ROWS // 2 :]], axis=1)

    q4r, q4i = rows_of(qr), rows_of(qi)
    s4r, s4i = cmul(q4r, q4i, q4r, q4i)
    s4r, s4i = cmul(s4r, s4i, s4r, s4i)
    four = jnp.zeros((4, 128), F32)
    start = (four, four, jnp.zeros((1, 128), F32) - 1.0)

    def fold(state, m, side, power, passed, near, far, use):
        cr, ci, last = state
        link = jnp.where(m[near : near + 1] == last, 1.0, 0.0) * m[passed : passed + 4]
        nr, ni = cmul(link * power[0], link * power[1], cr, ci)
        cr = jnp.where(use, nr + m[side : side + 4], cr)
        ci = jnp.where(use, ni + m[side + 4 : side + 8], ci)
        return cr, ci, jnp.where(use, m[far : far + 1], last)

    def fold_line(state, backward, use):
        for k in range(NY - 1, -1, -1) if backward else range(NY):
            m = line[k]
            if backward:
                state = fold(state, m, 8, (q4r, q4i), 16, 21, 20, use(k))
            else:
                state = fold(state, m, 0, (q4r, q4i), 16, 20, 21, use(k))
        return state

    def carry_line():
        take(line.at[pl.ds(0, NY - 1)], carry_sem.at[1, 0])
        always = lambda k: k >= 0
        ends = fold_line(start, False, always), fold_line(start, True, always)
        passed = line[0][16:20]
        for k in range(1, NY):
            link = jnp.where(line[k][20:21] == line[k - 1][21:22], 1.0, 0.0)
            passed = passed * (link * line[k][16:20])
        edges = jnp.concatenate(
            [line[0][20:21], line[NY - 1][21:22], jnp.zeros((2, 128), F32)], axis=0)
        for n in range(2):
            message[n, 0:4] = ends[n][0]
            message[n, 4:8] = ends[n][1]
            message[n, 8:12] = passed
            message[n, 12:16] = edges
        column[z] = message[0]
        for k in (4, 3, 5, 2, 6, 1, 7):
            side = jnp.where(lax.rem(z + k, NZ) > z, 0, 1)
            push(message.at[side], column.at[z], carry_sem, 1, at_z(k))

    def carry_column():
        take(column.at[pl.ds(0, NZ - 1)], carry_sem.at[1, 1])
        forward, backward = start, start
        for k in range(NZ):
            forward = fold(forward, column[k], 0, (s4r, s4i), 8, 12, 13, k < z)
            j = NZ - 1 - k
            backward = fold(backward, column[j], 0, (s4r, s4i), 8, 13, 12, j > z)
        into_f = fold_line(forward, False, lambda k: k < y)
        into_b = fold_line(backward, True, lambda k: k > y)
        enter_f = jnp.where(into_f[2] == edge_first, 1.0, 0.0)
        enter_b = jnp.where(into_b[2] == edge_last, 1.0, 0.0)
        enter_f = (flat_of(into_f[0] * enter_f), flat_of(into_f[1] * enter_f))
        enter_b = (flat_of(into_b[0] * enter_b), flat_of(into_b[1] * enter_b))
        entries_f = chunk_entries(enter_f, fr, fi, fp, False)[0]
        entries_b = chunk_entries(enter_b, br, bi, bp, True)[0]
        return tuple(
            jnp.concatenate([e[part_no] for e in entries], axis=0)
            for entries in (entries_f, entries_b) for part_no in (0, 1)
        )

    def second(j, state):
        fr, fi, br, bi = state
        _, fr, fi = advance(j, (fr, fi), 0)
        k = STEPS - 1 - j
        _, br, bi = advance(k, (br, bi), 1)
        at = pl.ds(pl.multiple_of(j * CHUNKS, CHUNKS), CHUNKS)
        states[at, 0:W] = fr
        states[at, 2 * W : 3 * W] = fi
        at = pl.ds(pl.multiple_of(k * CHUNKS, CHUNKS), CHUNKS)
        states[at, W : 2 * W] = br
        states[at, 3 * W : 4 * W] = bi
        return fr, fi, br, bi

    def scan():
        lax.fori_loop(0, STEPS, second, carry_column())

    def mix_out():
        pre = skip[...] * u
        for n in range(4):
            high, low = halves(states[:, W * n : W * (n + 1)])
            pre = pre + dot_nt(high, maps[0, n]) + dot_nt(high, maps[1, n])
            pre = pre + dot_nt(low, maps[0, n])
        mixed = jax.nn.gelu(pre).astype(BF16)
        back = one_hot(t == lax.rem(r, STEPS) * CHUNKS + r // STEPS, BF16)
        mixes[tp] = dot(back, mixed).astype(BF16)
        for k in (2, 1, 3):
            push(mixes.at[tp], mixes.at[tp], mix_sem, 0, at_x(k))
        push(mixes.at[tp], mixes.at[tp], mix_sem, 1, sibling)

    def of_x(k):
        return lax.rem(x + k, NX) * NC + c

    def share():
        take(shared.at[pl.ds(0, 2)], shared_sem.at[1, 0])
        half = (CH + TOK) // 2
        for k, first in ((1, half), (3, 0)):
            ref = shared.at[of_x(k), pl.ds(first, half)]
            push(ref, ref, shared_sem, 1, at_x(NX - k))
        for k in (1, 3):
            push(shared.at[of_x(k)], shared.at[of_x(k)], shared_sem, 2, sibling)

    def share_last():
        take(shared.at[0], shared_sem.at[1, 1])
        push(shared.at[of_x(2)], shared.at[of_x(2)], shared_sem, 2, sibling)

    def mix_pass():
        take(mixes.at[pl.ds(0, 3)], mix_sem.at[1, 0])
        for k in (1, 2, 3):
            push(mixes.at[of_x(k)], mixes.at[of_x(k)], mix_sem, 1, sibling)

    def project():
        take(shared.at[pl.ds(0, 4)], shared_sem.at[1, 2])
        take(mixes.at[pl.ds(0, 4)], mix_sem.at[1, 1])
        both = jnp.concatenate([mixes[k] for k in range(TP)], axis=1)
        branch[...] = dot(both, shared[:, 0:CH].reshape(TP * CH, D))

    def normalize():
        scales = gain[...]
        resid[...] = stream[...].astype(F32) + branch[pl.ds(pl.multiple_of(tp * TOK, TOK), TOK)]

        @pl.loop(0, TP)
        def _(k):
            at = pl.ds(pl.multiple_of(k * TOK, TOK), TOK)
            kept = shared[k, CH : CH + TOK].astype(F32) + branch[at]
            scale = lax.rsqrt(jnp.mean(kept * kept, axis=-1, keepdims=True) + 1e-6)
            normed[at] = (kept * scale * scales).astype(BF16)

    def widen():
        rows = normed[...]
        second_part = dot(rows, gua[...].reshape(D, GUA))
        first_part = dot(rows, gub[...].reshape(D, GUB))
        hidden[:, 0:MAIN] = (jax.nn.silu(first_part) * second_part[:, 0:MAIN]).astype(BF16)
        tail_gate = second_part[:, MAIN:FF]
        tail_up = second_part[:, FF:GUA]
        tail = (jax.nn.silu(tail_gate) * tail_up).astype(BF16)
        empty = jnp.zeros((T, FF - MAIN), BF16)
        hidden[:, MAIN:KPAD] = jnp.concatenate([tail, empty, empty, tail], axis=1)

    def down_y():
        dn.send_by(1)
        dn.send_ay(0)

    def down_z():
        dn.send_az(1)
        dn.send_bz(1, 0)

    def product(o):
        zi = gu.zi(o)
        at = pl.ds(zi * NY, NY)
        out = dot_nt(hidden[:, 0:DA], dna[at].reshape(NY * ROWS, DA))
        out = out + dot_nt(hidden[:, DA:MAIN], dnb[at, 0:ROWS].reshape(NY * ROWS, DB))
        rest = dnb[at, ROWS:DROWS].reshape(NY * ROWS // 2, DB)
        sides = [dot_nt(hidden[:, at : at + 128], rest) for at in (MAIN, MAIN + 128)]
        out = out + jnp.concatenate(
            [side[:, k : k + ROWS // 2] for k in range(0, 128, ROWS // 2) for side in sides], axis=1
        )
        out = out.astype(BF16).reshape(NX, NC, TOK, NY * ROWS)
        for k in range(NC):
            ffn_part[zi, k] = out[:, k]
        pltpu.make_async_remote_copy(
            src_ref=ffn_part.at[zi, 1 - c], dst_ref=ffn_pair.at[zi],
            send_sem=fs_send.at[1], recv_sem=pair_sem.at[zi],
            device_id=sibling, device_id_type=MESH).start()

    def combine(o):
        zi = gu.zi(o)
        take(ffn_pair.at[zi], pair_sem.at[zi])
        total = ffn_part[zi, c].astype(F32) + ffn_pair[zi].astype(F32)
        ffn_send[zi] = total.astype(BF16)
        for k in (2, 1, 3):
            pltpu.make_async_remote_copy(
                src_ref=ffn_send.at[zi, lax.rem(x + k, NX)], dst_ref=ffn_recv.at[zi, x],
                send_sem=fs_send.at[0], recv_sem=fs_recv.at[zi],
                device_id=at_x(k), device_id_type=MESH).start()
        ffn_recv[zi, x] = ffn_send[zi, x]

    def finish(o):
        zi = gu.zi(o)
        take(ffn_recv.at[zi, pl.ds(0, NX - 1)], fs_recv.at[zi])
        at = pl.ds(pl.multiple_of(zi * (NY * ROWS), NY * ROWS), NY * ROWS)
        ffn = ffn_recv[zi, 0].astype(F32)
        for k in range(1, NX):
            ffn = ffn + ffn_recv[zi, k].astype(F32)
        result[:, at] = (resid[:, at] + 0.5 * ffn).astype(BF16)

    steps = {
        "maps": output_maps, "line": carry_line, "scan": scan, "out": mix_out, "share": share, "last": share_last,
        "pass": mix_pass, "proj": project, "norm": normalize, "widen": widen, "downz": down_z,
        "product": product, "combine": combine, "finish": finish,
        "downy": down_y,
    }
    for step in ORDER:
        name, number = step.split()[0], [int(n) for n in step.split()[1:]]
        if name[0] in "gd" and name[1:] in ("az", "ay", "al", "by", "bz"):
            getattr(gu if name[0] == "g" else dn, name[1:])(*number)
        else:
            steps[name](*number)

    gu.drain()
    dn.drain()
    take(line.at[pl.ds(0, NY - 1)], carry_sem.at[0, 0])
    take(column.at[pl.ds(0, NZ - 1)], carry_sem.at[0, 1])
    take(shared.at[pl.ds(0, 2)], shared_sem.at[0, 0])
    take(shared.at[0], shared_sem.at[0, 1])
    take(shared.at[pl.ds(0, 4)], shared_sem.at[0, 2])
    take(mixes.at[pl.ds(0, 3)], mix_sem.at[0, 0])
    take(mixes.at[pl.ds(0, 4)], mix_sem.at[0, 1])
    take(ffn_recv.at[pl.ds(0, NZ * (NX - 1) // NX)], fs_send.at[0])
    take(ffn_pair, fs_send.at[1])


def by_channel(maps):
    return jnp.swapaxes(maps, 2, 3).reshape(2 * CH, S)


def local(
    mix_input, stream, doc_ids, log_dt, decay_rate, frequency, input_real, input_imag,
    output_real, output_imag, skip_gain, log_keep, proj_weight, norm_gain, gate_weight,
    up_weight, down_weight,
):
    vmem = pl.BlockSpec(memory_space=pltpu.VMEM)
    smem = pl.BlockSpec(memory_space=pltpu.SMEM)
    any_ = pl.BlockSpec(memory_space=pl.ANY)
    specs = [any_] * 2 + [vmem] + [smem] * 2 + [vmem] * 2 + [any_] * 4 + [vmem] + [any_] * 2
    specs += [vmem] + [any_] * 3
    dma = pltpu.SemaphoreType.DMA
    scratch = [
        pltpu.VMEM((T, CH), BF16),
        pltpu.VMEM((TOK, D), BF16),
        pltpu.VMEM((2 * CH, S), F32),
        pltpu.VMEM((2 * CH, S), F32),
        pltpu.VMEM((2 * CH, S), F32),
        pltpu.VMEM((2 * CH, S), F32),
        pltpu.VMEM((G, T), F32),
        pltpu.VMEM((ROWS, FF), BF16),
        pltpu.VMEM((ROWS, FF), BF16),
        pltpu.VMEM((ROWS, FF), BF16),
        pltpu.VMEM((SP, ROWS, GUA), BF16),
        pltpu.VMEM((SP, ROWS, GUB), BF16),
        pltpu.VMEM((SP, ROWS, DA), BF16),
        pltpu.VMEM((SP, DROWS, DB), BF16),
        pltpu.VMEM((T, 4 * W), F32),
        pltpu.VMEM((T, 2 * W), F32),
        pltpu.VMEM((T, 4 * W), F32),
        pltpu.VMEM((2, 4, CH, W), BF16),
        pltpu.VMEM((NY, 24, 128), F32),
        pltpu.VMEM((2, 16, 128), F32),
        pltpu.VMEM((NZ, 16, 128), F32),
        pltpu.VMEM((TP, CH + TOK, D), BF16),
        pltpu.VMEM((TP, T, CH), BF16),
        pltpu.VMEM((T, D), F32),
        pltpu.VMEM((TOK, D), F32),
        pltpu.VMEM((T, D), BF16),
        pltpu.VMEM((T, KPAD), BF16),
        pltpu.VMEM((NZ, NC, NX, TOK, NY * ROWS), BF16),
        pltpu.VMEM((NZ, NX, TOK, NY * ROWS), BF16),
        pltpu.VMEM((NZ, NX, TOK, NY * ROWS), BF16),
        pltpu.VMEM((NZ, NX, TOK, NY * ROWS), BF16),
        dma((2,)), dma((RECVS,)), dma((2,)), dma((RECVS,)),
        dma((2, 2)), dma((2, 3)), dma((2, 2)), dma((NZ,)), dma((2,)), dma((NZ,)), dma((16,)),
    ]
    return pl.pallas_call(
        kernel,
        out_shape=pltpu.VMEM((TOK, D), BF16),
        in_specs=specs,
        out_specs=vmem,
        scratch_shapes=scratch,
        compiler_params=pltpu.CompilerParams(
            collective_id=0, has_side_effects=True, vmem_limit_bytes=60 << 20
        ),
        name="layer",
    )(
        mix_input, stream, doc_ids.reshape(1, T), doc_ids, log_dt, decay_rate, frequency,
        by_channel(input_real), by_channel(input_imag),
        output_real.reshape(2 * CH, S), output_imag.reshape(2 * CH, S),
        skip_gain.reshape(1, CH), log_keep, proj_weight, norm_gain.reshape(1, D),
        gate_weight, up_weight, down_weight.T,
    )


def solution(mesh):
    torus = Mesh(mesh.devices.reshape(NZ, NY, NX, NC), ("z", "y", "x", "c"))
    sp, tp = ("z", "y"), ("x", "c")
    every = ("z", "y", "x", "c")
    in_specs = (
        P(sp, tp), P(every, None), P(sp), P(tp), P(tp, None), P(tp, None),
        P(None, tp, None, None), P(None, tp, None, None),
        P(None, tp, None, None), P(None, tp, None, None),
        P(tp), P(tp, sp), P(tp, None), P(), P(sp, tp), P(sp, tp), P(tp, sp),
    )
    return jax.shard_map(
        local, mesh=torus, in_specs=in_specs, out_specs=P(every, None), check_vma=False
    )
```

```python
import functools

import jax
import jax.numpy as jnp
from jax import lax
from jax.experimental import pallas as pl
from jax.experimental.pallas import tpu as pltpu
from jax.sharding import Mesh
from jax.sharding import PartitionSpec as P

HIGHEST = lax.Precision.HIGHEST
MESH = pl.DeviceIdType.MESH
F32, BF16 = jnp.float32, jnp.bfloat16

NZ, NY, NX, NC = 8, 4, 4, 2
SP, TP = NZ * NY, NX * NC
T, CH, G, S, GW = 256, 128, 8, 64, 16
W = G * S
CHUNKS = 8
STEPS = T // CHUNKS
D = 2048
FF = 704
MAIN = 640
ROWS = D // SP
TOK = T // TP
GUA, GUB = MAIN + 128, MAIN
DA, DB = 512, 128
DROWS = ROWS + ROWS // 2
KPAD = MAIN + 256
NT = (((1,), (1,)), ((), ()))


def dot(a, b, precision=None):
    return jnp.dot(a, b, preferred_element_type=F32, precision=precision)


def dot_nt(a, b, precision=None):
    return lax.dot_general(a, b, NT, preferred_element_type=F32, precision=precision)


def halves(value):
    high = value.astype(BF16)
    return high, (value - high.astype(F32)).astype(BF16)


def iota(shape, dim):
    return lax.broadcasted_iota(jnp.int32, shape, dim)


def one_hot(mask, dtype):
    return jnp.where(mask, 1.0, 0.0).astype(F32).astype(dtype)


def cmul(ar, ai, br, bi):
    return ar * br - ai * bi, ar * bi + ai * br


class Relay:
    def __init__(self, ra, rb, send, recv, z, y, joint):
        self.ra, self.rb, self.send, self.recv = ra, rb, send, recv
        self.z, self.y, self.joint = z, y, joint

    def zi(self, offset):
        return lax.rem(self.z + (offset + NZ), NZ)

    def yi(self, offset):
        return lax.rem(self.y + (offset + NY), NY)

    def start(self, number, ref, axis, to):
        pltpu.make_async_remote_copy(
            src_ref=ref,
            dst_ref=ref,
            send_sem=self.send.at[0 if number < 20 else 1],
            recv_sem=self.recv.at[number],
            device_id={axis: self.zi(to) if axis == "z" else self.yi(to)},
            device_id_type=MESH,
        ).start()

    def wait(self, number, ref):
        pltpu.make_async_copy(ref, ref, self.recv.at[number]).wait()

    def a(self, dz, dy):
        return self.ra.at[self.zi(dz) * NY + self.yi(dy)]

    def send_az(self, d):
        for way in (1, -1):
            ref = self.a(-way * (d - 1), 0)
            if d == 4:
                ref = self.half(ref, way)
            self.start(d - 1, ref, "z", way)

    def send_ay(self, o):
        for way in (1, -1):
            self.start(4 + o % NZ, self.a(o, 0), "y", way)

    def az(self, d):
        self.wait(d - 1, self.ra.at[0] if d == 4 else self.ra.at[pl.ds(0, 2)])
        if d < 4:
            self.send_az(d + 1)
        for o in (4,) if d == 4 else (-d, d):
            self.send_ay(o)

    def ay(self, o):
        self.wait(4 + o % NZ, self.ra.at[pl.ds(0, 2)])
        way = 1 if o % 2 == 0 else -1
        self.start(12 + (0 if self.joint else o % NZ), self.a(o, -way), "y", way)

    def al(self, o):
        self.wait(12 + o % NZ, self.ra.at[0])

    def all_al(self):
        self.wait(12, self.ra.at[pl.ds(0, NZ)])

    def send_by(self, d):
        for way in (1, -1):
            ref = self.rb.at[self.z * NY + self.yi(-way * (d - 1))]
            if d == 2:
                ref = self.half(ref, way)
            self.start(19 + d, ref, "y", way)

    def by(self, d):
        self.wait(19 + d, self.rb.at[pl.ds(0, 2)] if d == 1 else self.rb.at[0])
        if d == 1:
            self.send_by(2)
        self.send_bz(1, d)

    def send_bz(self, d, j):
        for way in (1, -1):
            first = self.zi(-way * (d - 1)) * NY
            for dy in ((0,), (1, -1), (2,))[j]:
                if d == 4 and dy == -way:
                    continue
                ref = self.rb.at[first + self.yi(dy)]
                if d == 4 and j != 1:
                    ref = self.half(ref, way)
                self.start(19 + 3 * d + j, ref, "z", way)

    def bz(self, d, j):
        count = (2 if j == 1 else 1) * (1 if d == 4 else 2)
        self.wait(19 + 3 * d + j, self.rb.at[pl.ds(0, count)])
        if d < 4:
            self.send_bz(d + 1, j)

    def half(self, ref, way):
        rows = ref.shape[0] // 2
        return ref.at[pl.ds(0 if way > 0 else rows, rows)]

    def drain(self):
        for n, ref in enumerate((self.ra, self.rb)):
            part = ref.at[pl.ds(0, SP - 1)]
            pltpu.make_async_copy(part, part, self.send.at[n]).wait()


RECVS = 34
OFFSETS = (0, -1, 1, -2, 2, -3, 3, 4)
ORDER = (
    "maps", "gaz 1", "gby 1", "gbz 1 0", "line", "gay 0", "gay -1", "gaz 2", "gay 1", "gby 2",
    "gbz 1 1", "gbz 2 0", "gay -2", "scan", "share", "out", "gbz 1 2", "gay 2", "gaz 3",
    "gbz 2 1", "daz 1", "dbz 1 0", "gbz 3 0", "gay -3", "gbz 2 2", "day 0", "gaz 4", "dby 1",
    "gay 3", "day -1", "last", "day 1", "gbz 3 1", "daz 2", "dbz 2 0", "pass", "gay 4", "dby 2",
    "gbz 3 2", "proj", "dbz 1 1", "norm", "day -2", "dbz 3 0", "day 2", "dbz 1 2", "daz 3",
    "gbz 4 0", "gbz 4 1", "gbz 4 2", "widen", "dal 0", "product 0", "dbz 2 2", "dal 1",
    "product 1", "daz 4", "dbz 2 1", "dal -2", "product -2", "dal 2", "product 2", "day -3",
    "combine 0", "dal -1", "product -1", "day 3", "combine -2", "combine 1", "combine 2",
    "dbz 3 2", "combine -1", "dbz 3 1", "day 4", "dal -3", "product -3", "dal 3", "product 3",
    "combine -3", "dbz 4 0", "dbz 4 1", "dbz 4 2", "dal 4", "product 4", "combine 3", "combine 4",
    "finish 0", "finish -2", "finish 1", "finish 2", "finish -1", "finish -3", "finish 3",
    "finish 4",
)


def row_of(block):
    return jnp.concatenate([block[g : g + 1, :] for g in range(G)], axis=1)


def rows_of(row):
    return jnp.concatenate([row[:, 128 * k : 128 * (k + 1)] for k in range(W // 128)], axis=0)


def flat_of(rows):
    return jnp.concatenate([rows[k : k + 1, :] for k in range(W // 128)], axis=1)


def kernel(
    mix_hbm, stream_hbm, docs_hbm, log_dt_hbm, decay_hbm, freq_hbm, in_real_hbm, in_imag_hbm,
    out_real_hbm, out_imag_hbm, skip_hbm, keep_hbm, proj_hbm, gain_hbm, gate_hbm, up_hbm, down_hbm,
    result,
    mix, stream, docs, log_dt, decay, freq, in_real, in_imag, out_real, out_imag, skip, log_keep,
    gain, gate_w, up_w, down_w,
    gua, gub, dna, dnb, drive, factor, states, maps, line, message, column, shared, mixes,
    branch, resid, normed, hidden, ffn_part, ffn_pair, ffn_send, ffn_recv,
    gu_send, gu_recv, dn_send, dn_recv, carry_sem, shared_sem, mix_sem, pair_sem, fs_send, fs_recv, load_sem,
):
    z, y, x, c = (lax.axis_index(a) for a in ("z", "y", "x", "c"))
    sp, tp = z * NY + y, x * NC + c

    def tp_peer(k):
        other = lax.rem(tp + k, TP)
        return other, {"x": other // NC, "c": lax.rem(other, NC)}

    def at_z(k):
        return {"z": lax.rem(z + k, NZ)}

    def at_y(k):
        return {"y": lax.rem(y + k, NY)}

    def at_x(k):
        return {"x": lax.rem(x + k, NX)}

    sibling = {"c": 1 - c}

    barrier = pltpu.get_barrier_semaphore()

    def greet(device):
        pl.semaphore_signal(barrier, inc=1, device_id=device, device_id_type=MESH)

    for k in (1, 7, 2, 6, 3, 5, 4):
        greet(at_z(k))
    for k in (1, 3, 2):
        greet(at_y(k))
    for k in range(1, TP):
        greet(tp_peer(k)[1])

    def push(source, target, sems, n, device):
        pltpu.make_async_remote_copy(
            src_ref=source, dst_ref=target, send_sem=sems.at[0, n], recv_sem=sems.at[1, n],
            device_id=device, device_id_type=MESH).start()

    def take(ref, sem):
        pltpu.make_async_copy(ref, ref, sem).wait()

    def load(n, *pairs):
        copies = [pltpu.make_async_copy(*pair, load_sem.at[n]) for pair in pairs]
        for copy in copies:
            copy.start()
        return copies

    def loaded(copies):
        for copy in copies:
            copy.wait()

    gate_load = load(0, (gate_hbm, gate_w))
    up_load = load(1, (up_hbm, up_w))
    gate_piece = load(2, (gate_hbm.at[:, pl.ds(0, MAIN)], gub.at[sp]))
    up_piece = load(3, (up_hbm.at[:, pl.ds(0, MAIN)], gua.at[sp, :, pl.ds(0, MAIN)]))
    down_load = load(17, (down_hbm, down_w))
    down_pieces = [
        load(18, (down_hbm.at[:, pl.ds(0, DA)], dna.at[sp])),
        load(19, (down_hbm.at[:, pl.ds(DA, DB)], dnb.at[sp, pl.ds(0, ROWS)])),
    ]
    scan_loads = [
        load(4 + n, pair) for n, pair in enumerate((
            (log_dt_hbm, log_dt), (decay_hbm, decay), (freq_hbm, freq), (mix_hbm, mix),
            (docs_hbm, docs), (keep_hbm, log_keep), (in_real_hbm, in_real), (in_imag_hbm, in_imag),
        ))
    ]
    share_loads = [
        load(12, (proj_hbm, shared.at[tp, pl.ds(0, CH)])),
        load(13, (stream_hbm, shared.at[tp, pl.ds(CH, TOK)])),
    ]
    map_loads = [
        load(n, pair) for n, pair in (
            (14, (out_real_hbm, out_real)), (15, (out_imag_hbm, out_imag)),
            (16, (stream_hbm, stream)), (20, (skip_hbm, skip)), (21, (gain_hbm, gain)),
        )
    ]
    loaded(gate_load)
    loaded(up_load)
    gua[sp, :, MAIN:GUA] = jnp.concatenate([gate_w[:, MAIN:FF], up_w[:, MAIN:FF]], axis=1)
    loaded(down_load)
    rest = down_w[:, MAIN:FF]
    dnb[sp, ROWS:DROWS] = jnp.concatenate([rest[: ROWS // 2], rest[ROWS // 2 :]], axis=1)

    gu = Relay(gua, gub, gu_send, gu_recv, z, y, True)
    dn = Relay(dna, dnb, dn_send, dn_recv, z, y, False)
    loaded(gate_piece)
    loaded(up_piece)
    pl.semaphore_wait(barrier, NZ - 1 + NY - 1 + TP - 1)
    gu.send_by(1)
    gu.send_bz(1, 0)
    gu.send_az(1)
    for copies in down_pieces:
        loaded(copies)
    dn.send_by(1)
    dn.send_ay(0)
    dn.send_az(1)
    dn.send_bz(1, 0)
    for copies in share_loads:
        loaded(copies)
    for k in (1, 3):
        push(shared.at[tp], shared.at[tp], shared_sem, 0, at_x(k))
    push(shared.at[tp], shared.at[tp], shared_sem, 2, sibling)
    for copies in scan_loads:
        loaded(copies)

    group = iota((G, S), 0)
    steps = jnp.zeros((G, S), F32)
    for g in range(G):
        steps = jnp.where(group == g, log_dt[0:1, g : g + 1], steps)
    steps = jnp.exp(steps)
    rate, turn_rate = decay[...], freq[...]
    magnitude = jnp.exp(-steps * rate)
    angle = steps * turn_rate
    a_real, a_imag = magnitude * jnp.cos(angle), magnitude * jnp.sin(angle)
    below = rate * rate + turn_rate * turn_rate
    shifted = a_real - 1.0
    z_real = (-shifted * rate + a_imag * turn_rate) / below
    z_imag = (-a_imag * rate - shifted * turn_rate) / below
    ar, ai, zr, zi = (row_of(v) for v in (a_real, a_imag, z_real, z_imag))

    r, t = iota((T, T), 0), iota((T, T), 1)
    order = t == lax.rem(r, CHUNKS) * STEPS + r // CHUNKS
    order_f = one_hot(order, F32)
    u = dot(order_f.astype(BF16), mix[...])
    ub = u.astype(BF16)

    tile = one_hot(lax.rem(iota((S, W), 1), S) == iota((S, W), 0), BF16)
    own = lax.rem(iota((2 * CH, W), 0), CH) // GW == iota((2 * CH, W), 1) // S
    for n, ref in enumerate((in_real, in_imag)):
        high, low = (
            jnp.where(own, dot(half, tile), 0.0).astype(BF16) for half in halves(ref[...])
        )
        for d in range(2):
            at = slice(CH * d, CH * (d + 1))
            drive[:, W * (2 * n + d) : W * (2 * n + d + 1)] = dot(ub, high[at]) + dot(ub, low[at])

    doc = docs[...].astype(F32) + jnp.zeros((G, T), F32)
    place = iota((G, T), 1)
    before, after = pltpu.roll(doc, 1, 1), pltpu.roll(doc, T - 1, 1)
    keep = jnp.exp(log_keep[...])
    keep_f = jnp.where((place == 0) | (doc == before), keep, 0.0)
    keep_b = jnp.where((place == T - 1) | (doc == after), keep, 0.0)
    both = dot_nt(order_f, jnp.concatenate([keep_f, keep_b], axis=0), HIGHEST)
    spread = one_hot(iota((2 * G, 2 * W), 0) == iota((2 * G, 2 * W), 1) // S, F32)
    factor[...] = dot(both, spread, HIGHEST)

    zero = jnp.zeros((CHUNKS, W), F32)
    ar8, ai8 = zero + ar, zero + ai

    def advance(j, state, direction):
        at = pl.ds(pl.multiple_of(j * CHUNKS, CHUNKS), CHUNKS)
        f = factor[at, W * direction : W * (direction + 1)]
        dr = drive[at, W * direction : W * (direction + 1)]
        di = drive[at, W * (2 + direction) : W * (3 + direction)]
        hr, hi = state
        nr, ni = cmul(f * ar8, f * ai8, hr, hi)
        return f, nr + dr, ni + di

    def first(j, state):
        fr, fi, fp, br, bi, bp = state
        f, fr, fi = advance(j, (fr, fi), 0)
        b, br, bi = advance(STEPS - 1 - j, (br, bi), 1)
        return fr, fi, fp * f, br, bi, bp * b

    fr, fi, fp, br, bi, bp = lax.fori_loop(
        0, STEPS, first, (zero, zero, zero + 1.0, zero, zero, zero + 1.0)
    )
    pr, pi = ar, ai
    for _ in range(5):
        pr, pi = cmul(pr, pi, pr, pi)

    def chunk_entries(enter, hr, hi, passed, backward):
        er, ei = enter
        entries = [None] * CHUNKS
        chunks = range(CHUNKS - 1, -1, -1) if backward else range(CHUNKS)
        for k in chunks:
            entries[k] = (er, ei)
            f = passed[k : k + 1]
            nr, ni = cmul(f * pr, f * pi, er, ei)
            er, ei = nr + hr[k : k + 1], ni + hi[k : k + 1]
        return entries, (er, ei)

    none = (jnp.zeros((1, W), F32), jnp.zeros((1, W), F32))
    end_f = chunk_entries(none, fr, fi, fp, False)[1]
    end_b = chunk_entries(none, br, bi, bp, True)[1]
    passed = fp[0:1]
    for k in range(1, CHUNKS):
        passed = passed * fp[k : k + 1]
    qr, qi = pr, pi
    for _ in range(3):
        qr, qi = cmul(qr, qi, qr, qi)
    edge_first = jnp.broadcast_to(doc[0:1, 0:1], (1, 128))
    edge_last = jnp.broadcast_to(doc[0:1, T - 1 : T], (1, 128))
    passed_rows = rows_of(passed)
    edges = jnp.concatenate(
        [edge_first, edge_last, jnp.zeros((2, 128), F32)], axis=0)
    for n, (er, ei) in enumerate((end_f, end_b)):
        line[y, 8 * n : 8 * n + 4] = rows_of(er)
        line[y, 8 * n + 4 : 8 * n + 8] = rows_of(ei)
    line[y, 16:20] = passed_rows
    line[y, 20:24] = edges

    for k in (2, 1, 3):
        push(line.at[y], line.at[y], carry_sem, 0, at_y(k))
    gu.send_ay(0)

    def output_maps():
        for copies in map_loads:
            loaded(copies)
        spread = tile.astype(F32)
        cr = jnp.where(own, dot(out_real[...], spread, HIGHEST), 0.0)
        ci = jnp.where(own, dot(out_imag[...], spread, HIGHEST), 0.0)
        cr, ci = cmul(zr, zi, cr, ci)
        for n in range(4):
            read = (cr if n < 2 else -ci)[CH * (n % 2) : CH * (n % 2 + 1)]
            maps[0, n], maps[1, n] = halves(read)

    q4r, q4i = rows_of(qr), rows_of(qi)
    s4r, s4i = cmul(q4r, q4i, q4r, q4i)
    s4r, s4i = cmul(s4r, s4i, s4r, s4i)
    four = jnp.zeros((4, 128), F32)
    start = (four, four, jnp.zeros((1, 128), F32) - 1.0)

    def fold(state, m, side, power, passed, near, far, use):
        cr, ci, last = state
        link = jnp.where(m[near : near + 1] == last, 1.0, 0.0) * m[passed : passed + 4]
        nr, ni = cmul(link * power[0], link * power[1], cr, ci)
        cr = jnp.where(use, nr + m[side : side + 4], cr)
        ci = jnp.where(use, ni + m[side + 4 : side + 8], ci)
        return cr, ci, jnp.where(use, m[far : far + 1], last)

    def fold_line(state, backward, use):
        for k in range(NY - 1, -1, -1) if backward else range(NY):
            m = line[k]
            if backward:
                state = fold(state, m, 8, (q4r, q4i), 16, 21, 20, use(k))
            else:
                state = fold(state, m, 0, (q4r, q4i), 16, 20, 21, use(k))
        return state

    def carry_line():
        take(line.at[pl.ds(0, NY - 1)], carry_sem.at[1, 0])
        always = lambda k: k >= 0
        ends = fold_line(start, False, always), fold_line(start, True, always)
        passed = line[0][16:20]
        for k in range(1, NY):
            link = jnp.where(line[k][20:21] == line[k - 1][21:22], 1.0, 0.0)
            passed = passed * (link * line[k][16:20])
        edges = jnp.concatenate(
            [line[0][20:21], line[NY - 1][21:22], jnp.zeros((2, 128), F32)], axis=0)
        for n in range(2):
            message[n, 0:4] = ends[n][0]
            message[n, 4:8] = ends[n][1]
            message[n, 8:12] = passed
            message[n, 12:16] = edges
        column[z] = message[0]
        for k in (4, 3, 5, 2, 6, 1, 7):
            side = jnp.where(lax.rem(z + k, NZ) > z, 0, 1)
            push(message.at[side], column.at[z], carry_sem, 1, at_z(k))

    def carry_column():
        take(column.at[pl.ds(0, NZ - 1)], carry_sem.at[1, 1])
        forward, backward = start, start
        for k in range(NZ):
            forward = fold(forward, column[k], 0, (s4r, s4i), 8, 12, 13, k < z)
            j = NZ - 1 - k
            backward = fold(backward, column[j], 0, (s4r, s4i), 8, 13, 12, j > z)
        into_f = fold_line(forward, False, lambda k: k < y)
        into_b = fold_line(backward, True, lambda k: k > y)
        enter_f = jnp.where(into_f[2] == edge_first, 1.0, 0.0)
        enter_b = jnp.where(into_b[2] == edge_last, 1.0, 0.0)
        enter_f = (flat_of(into_f[0] * enter_f), flat_of(into_f[1] * enter_f))
        enter_b = (flat_of(into_b[0] * enter_b), flat_of(into_b[1] * enter_b))
        entries_f = chunk_entries(enter_f, fr, fi, fp, False)[0]
        entries_b = chunk_entries(enter_b, br, bi, bp, True)[0]
        return tuple(
            jnp.concatenate([e[part_no] for e in entries], axis=0)
            for entries in (entries_f, entries_b) for part_no in (0, 1)
        )

    def second(j, state):
        fr, fi, br, bi = state
        _, fr, fi = advance(j, (fr, fi), 0)
        k = STEPS - 1 - j
        _, br, bi = advance(k, (br, bi), 1)
        at = pl.ds(pl.multiple_of(j * CHUNKS, CHUNKS), CHUNKS)
        states[at, 0:W] = fr
        states[at, 2 * W : 3 * W] = fi
        at = pl.ds(pl.multiple_of(k * CHUNKS, CHUNKS), CHUNKS)
        states[at, W : 2 * W] = br
        states[at, 3 * W : 4 * W] = bi
        return fr, fi, br, bi

    def scan():
        lax.fori_loop(0, STEPS, second, carry_column())

    def mix_out():
        pre = skip[...] * u
        for n in range(4):
            high, low = halves(states[:, W * n : W * (n + 1)])
            pre = pre + dot_nt(high, maps[0, n]) + dot_nt(high, maps[1, n])
            pre = pre + dot_nt(low, maps[0, n])
        mixed = jax.nn.gelu(pre).astype(BF16)
        back = one_hot(t == lax.rem(r, STEPS) * CHUNKS + r // STEPS, BF16)
        mixes[tp] = dot(back, mixed).astype(BF16)
        for k in (2, 1, 3):
            push(mixes.at[tp], mixes.at[tp], mix_sem, 0, at_x(k))
        push(mixes.at[tp], mixes.at[tp], mix_sem, 1, sibling)

    def of_x(k):
        return lax.rem(x + k, NX) * NC + c

    def share():
        take(shared.at[pl.ds(0, 2)], shared_sem.at[1, 0])
        half = (CH + TOK) // 2
        for k, first in ((1, half), (3, 0)):
            ref = shared.at[of_x(k), pl.ds(first, half)]
            push(ref, ref, shared_sem, 1, at_x(NX - k))
        for k in (1, 3):
            push(shared.at[of_x(k)], shared.at[of_x(k)], shared_sem, 2, sibling)

    def share_last():
        take(shared.at[0], shared_sem.at[1, 1])
        push(shared.at[of_x(2)], shared.at[of_x(2)], shared_sem, 2, sibling)

    def mix_pass():
        take(mixes.at[pl.ds(0, 3)], mix_sem.at[1, 0])
        for k in (1, 2, 3):
            push(mixes.at[of_x(k)], mixes.at[of_x(k)], mix_sem, 1, sibling)

    def project():
        take(shared.at[pl.ds(0, 4)], shared_sem.at[1, 2])
        take(mixes.at[pl.ds(0, 4)], mix_sem.at[1, 1])
        both = jnp.concatenate([mixes[k] for k in range(TP)], axis=1)
        branch[...] = dot(both, shared[:, 0:CH].reshape(TP * CH, D))

    def normalize():
        scales = gain[...]
        resid[...] = stream[...].astype(F32) + branch[pl.ds(pl.multiple_of(tp * TOK, TOK), TOK)]

        @pl.loop(0, TP)
        def _(k):
            at = pl.ds(pl.multiple_of(k * TOK, TOK), TOK)
            kept = shared[k, CH : CH + TOK].astype(F32) + branch[at]
            scale = lax.rsqrt(jnp.mean(kept * kept, axis=-1, keepdims=True) + 1e-6)
            normed[at] = (kept * scale * scales).astype(BF16)

    def widen():
        gu.all_al()
        rows = normed[...]
        second_part = dot(rows, gua[...].reshape(D, GUA))
        first_part = dot(rows, gub[...].reshape(D, GUB))
        hidden[:, 0:MAIN] = (jax.nn.silu(first_part) * second_part[:, 0:MAIN]).astype(BF16)
        tail_gate = second_part[:, MAIN:FF]
        tail_up = second_part[:, FF:GUA]
        tail = (jax.nn.silu(tail_gate) * tail_up).astype(BF16)
        empty = jnp.zeros((T, FF - MAIN), BF16)
        hidden[:, MAIN:KPAD] = jnp.concatenate([tail, empty, empty, tail], axis=1)

    def product(o):
        zi = gu.zi(o)
        at = pl.ds(zi * NY, NY)
        out = dot_nt(hidden[:, 0:DA], dna[at].reshape(NY * ROWS, DA))
        out = out + dot_nt(hidden[:, DA:MAIN], dnb[at, 0:ROWS].reshape(NY * ROWS, DB))
        rest = dnb[at, ROWS:DROWS].reshape(NY * ROWS // 2, DB)
        sides = [dot_nt(hidden[:, at : at + 128], rest) for at in (MAIN, MAIN + 128)]
        out = out + jnp.concatenate(
            [side[:, k : k + ROWS // 2] for k in range(0, 128, ROWS // 2) for side in sides], axis=1
        )
        out = out.astype(BF16).reshape(NX, NC, TOK, NY * ROWS)
        for k in range(NC):
            ffn_part[zi, k] = out[:, k]
        pltpu.make_async_remote_copy(
            src_ref=ffn_part.at[zi, 1 - c], dst_ref=ffn_pair.at[zi],
            send_sem=fs_send.at[1], recv_sem=pair_sem.at[zi],
            device_id=sibling, device_id_type=MESH).start()

    def combine(o):
        zi = gu.zi(o)
        take(ffn_pair.at[zi], pair_sem.at[zi])
        total = ffn_part[zi, c].astype(F32) + ffn_pair[zi].astype(F32)
        ffn_send[zi] = total.astype(BF16)
        for k in (2, 1, 3):
            pltpu.make_async_remote_copy(
                src_ref=ffn_send.at[zi, lax.rem(x + k, NX)], dst_ref=ffn_recv.at[zi, x],
                send_sem=fs_send.at[0], recv_sem=fs_recv.at[zi],
                device_id=at_x(k), device_id_type=MESH).start()
        ffn_recv[zi, x] = ffn_send[zi, x]

    def finish(o):
        zi = gu.zi(o)
        take(ffn_recv.at[zi, pl.ds(0, NX - 1)], fs_recv.at[zi])
        at = pl.ds(pl.multiple_of(zi * (NY * ROWS), NY * ROWS), NY * ROWS)
        ffn = ffn_recv[zi, 0].astype(F32)
        for k in range(1, NX):
            ffn = ffn + ffn_recv[zi, k].astype(F32)
        result[:, at] = (resid[:, at] + 0.5 * ffn).astype(BF16)

    steps = {
        "maps": output_maps, "line": carry_line, "scan": scan, "out": mix_out, "share": share, "last": share_last,
        "pass": mix_pass, "proj": project, "norm": normalize, "widen": widen,
        "product": product, "combine": combine, "finish": finish,

    }
    for step in ORDER:
        name, number = step.split()[0], [int(n) for n in step.split()[1:]]
        if name[0] in "gd" and name[1:] in ("az", "ay", "al", "by", "bz"):
            getattr(gu if name[0] == "g" else dn, name[1:])(*number)
        else:
            steps[name](*number)

    gu.drain()
    dn.drain()
    take(line.at[pl.ds(0, NY - 1)], carry_sem.at[0, 0])
    take(column.at[pl.ds(0, NZ - 1)], carry_sem.at[0, 1])
    take(shared.at[pl.ds(0, 2)], shared_sem.at[0, 0])
    take(shared.at[0], shared_sem.at[0, 1])
    take(shared.at[pl.ds(0, 4)], shared_sem.at[0, 2])
    take(mixes.at[pl.ds(0, 3)], mix_sem.at[0, 0])
    take(mixes.at[pl.ds(0, 4)], mix_sem.at[0, 1])
    take(ffn_recv.at[pl.ds(0, NZ * (NX - 1) // NX)], fs_send.at[0])
    take(ffn_pair, fs_send.at[1])


def by_channel(maps):
    return jnp.swapaxes(maps, 2, 3).reshape(2 * CH, S)


def local(
    mix_input, stream, doc_ids, log_dt, decay_rate, frequency, input_real, input_imag,
    output_real, output_imag, skip_gain, log_keep, proj_weight, norm_gain, gate_weight,
    up_weight, down_weight,
):
    vmem = pl.BlockSpec(memory_space=pltpu.VMEM)
    specs = [pl.BlockSpec(memory_space=pl.ANY)] * 17
    dma = pltpu.SemaphoreType.DMA
    scratch = [
        pltpu.VMEM((T, CH), BF16),
        pltpu.VMEM((TOK, D), BF16),
        pltpu.VMEM((1, T), jnp.int32),
        pltpu.VMEM((1, G), F32),
        pltpu.VMEM((G, S), F32),
        pltpu.VMEM((G, S), F32),
        pltpu.VMEM((2 * CH, S), F32),
        pltpu.VMEM((2 * CH, S), F32),
        pltpu.VMEM((2 * CH, S), F32),
        pltpu.VMEM((2 * CH, S), F32),
        pltpu.VMEM((1, CH), F32),
        pltpu.VMEM((G, T), F32),
        pltpu.VMEM((1, D), F32),
        pltpu.VMEM((ROWS, FF), BF16),
        pltpu.VMEM((ROWS, FF), BF16),
        pltpu.VMEM((ROWS, FF), BF16),
        pltpu.VMEM((SP, ROWS, GUA), BF16),
        pltpu.VMEM((SP, ROWS, GUB), BF16),
        pltpu.VMEM((SP, ROWS, DA), BF16),
        pltpu.VMEM((SP, DROWS, DB), BF16),
        pltpu.VMEM((T, 4 * W), F32),
        pltpu.VMEM((T, 2 * W), F32),
        pltpu.VMEM((T, 4 * W), F32),
        pltpu.VMEM((2, 4, CH, W), BF16),
        pltpu.VMEM((NY, 24, 128), F32),
        pltpu.VMEM((2, 16, 128), F32),
        pltpu.VMEM((NZ, 16, 128), F32),
        pltpu.VMEM((TP, CH + TOK, D), BF16),
        pltpu.VMEM((TP, T, CH), BF16),
        pltpu.VMEM((T, D), F32),
        pltpu.VMEM((TOK, D), F32),
        pltpu.VMEM((T, D), BF16),
        pltpu.VMEM((T, KPAD), BF16),
        pltpu.VMEM((NZ, NC, NX, TOK, NY * ROWS), BF16),
        pltpu.VMEM((NZ, NX, TOK, NY * ROWS), BF16),
        pltpu.VMEM((NZ, NX, TOK, NY * ROWS), BF16),
        pltpu.VMEM((NZ, NX, TOK, NY * ROWS), BF16),
        dma((2,)), dma((RECVS,)), dma((2,)), dma((RECVS,)),
        dma((2, 2)), dma((2, 3)), dma((2, 2)), dma((NZ,)), dma((2,)), dma((NZ,)), dma((22,)),
    ]
    return pl.pallas_call(
        kernel,
        out_shape=pltpu.VMEM((TOK, D), BF16),
        in_specs=specs,
        out_specs=vmem,
        scratch_shapes=scratch,
        compiler_params=pltpu.CompilerParams(
            collective_id=0, has_side_effects=True, vmem_limit_bytes=60 << 20
        ),
        name="layer",
    )(
        mix_input, stream, doc_ids.reshape(1, T), log_dt.reshape(1, G), decay_rate, frequency,
        by_channel(input_real), by_channel(input_imag),
        output_real.reshape(2 * CH, S), output_imag.reshape(2 * CH, S),
        skip_gain.reshape(1, CH), log_keep, proj_weight, norm_gain.reshape(1, D),
        gate_weight, up_weight, down_weight.T,
    )


def solution(mesh):
    torus = Mesh(mesh.devices.reshape(NZ, NY, NX, NC), ("z", "y", "x", "c"))
    sp, tp = ("z", "y"), ("x", "c")
    every = ("z", "y", "x", "c")
    in_specs = (
        P(sp, tp), P(every, None), P(sp), P(tp), P(tp, None), P(tp, None),
        P(None, tp, None, None), P(None, tp, None, None),
        P(None, tp, None, None), P(None, tp, None, None),
        P(tp), P(tp, sp), P(tp, None), P(), P(sp, tp), P(sp, tp), P(tp, sp),
    )
    return jax.shard_map(
        local, mesh=torus, in_specs=in_specs, out_specs=P(every, None), check_vma=False
    )
```

```python
import functools

import jax
import jax.numpy as jnp
from jax import lax
from jax.experimental import pallas as pl
from jax.experimental.pallas import tpu as pltpu
from jax.sharding import Mesh
from jax.sharding import PartitionSpec as P

HIGHEST = lax.Precision.HIGHEST
MESH = pl.DeviceIdType.MESH
F32, BF16 = jnp.float32, jnp.bfloat16

NZ, NY, NX, NC = 8, 4, 4, 2
SP, TP = NZ * NY, NX * NC
T, CH, G, S, GW = 256, 128, 8, 64, 16
W = G * S
CHUNKS = 8
STEPS = T // CHUNKS
D = 2048
FF = 704
MAIN = 640
ROWS = D // SP
TOK = T // TP
GUA, GUB = MAIN + 128, MAIN
DA, DB = 512, 128
DROWS = ROWS + ROWS // 2
KPAD = MAIN + 256
NT = (((1,), (1,)), ((), ()))


def dot(a, b, precision=None):
    return jnp.dot(a, b, preferred_element_type=F32, precision=precision)


def dot_nt(a, b, precision=None):
    return lax.dot_general(a, b, NT, preferred_element_type=F32, precision=precision)


def halves(value):
    high = value.astype(BF16)
    return high, (value - high.astype(F32)).astype(BF16)


def iota(shape, dim):
    return lax.broadcasted_iota(jnp.int32, shape, dim)


def one_hot(mask, dtype):
    return jnp.where(mask, 1.0, 0.0).astype(F32).astype(dtype)


def cmul(ar, ai, br, bi):
    return ar * br - ai * bi, ar * bi + ai * br


class Relay:
    def __init__(self, ra, rb, send, recv, z, y, joint):
        self.ra, self.rb, self.send, self.recv = ra, rb, send, recv
        self.z, self.y, self.joint = z, y, joint

    def zi(self, offset):
        return lax.rem(self.z + (offset + NZ), NZ)

    def yi(self, offset):
        return lax.rem(self.y + (offset + NY), NY)

    def start(self, number, ref, axis, to):
        pltpu.make_async_remote_copy(
            src_ref=ref,
            dst_ref=ref,
            send_sem=self.send.at[0 if number < 20 else 1],
            recv_sem=self.recv.at[number],
            device_id={axis: self.zi(to) if axis == "z" else self.yi(to)},
            device_id_type=MESH,
        ).start()

    def wait(self, number, ref):
        pltpu.make_async_copy(ref, ref, self.recv.at[number]).wait()

    def a(self, dz, dy):
        return self.ra.at[self.zi(dz) * NY + self.yi(dy)]

    def send_az(self, d):
        for way in (1, -1):
            ref = self.a(-way * (d - 1), 0)
            if d == 4:
                ref = self.half(ref, way)
            self.start(d - 1, ref, "z", way)

    def send_ay(self, o):
        for way in (1, -1):
            self.start(4 + o % NZ, self.a(o, 0), "y", way)

    def az(self, d):
        self.wait(d - 1, self.ra.at[0] if d == 4 else self.ra.at[pl.ds(0, 2)])
        if d < 4:
            self.send_az(d + 1)
        for o in (4,) if d == 4 else (-d, d):
            self.send_ay(o)

    def ay(self, o):
        self.wait(4 + o % NZ, self.ra.at[pl.ds(0, 2)])
        way = 1 if o % 2 == 0 else -1
        self.start(12 + (0 if self.joint else o % NZ), self.a(o, -way), "y", way)

    def al(self, o):
        self.wait(12 + o % NZ, self.ra.at[0])

    def all_al(self):
        self.wait(12, self.ra.at[pl.ds(0, NZ)])

    def send_by(self, d):
        for way in (1, -1):
            ref = self.rb.at[self.z * NY + self.yi(-way * (d - 1))]
            if d == 2:
                ref = self.half(ref, way)
            self.start(19 + d, ref, "y", way)

    def by(self, d):
        self.wait(19 + d, self.rb.at[pl.ds(0, 2)] if d == 1 else self.rb.at[0])
        if d == 1:
            self.send_by(2)
        self.send_bz(1, d)

    def send_bz(self, d, j):
        for way in (1, -1):
            first = self.zi(-way * (d - 1)) * NY
            for dy in ((0,), (1, -1), (2,))[j]:
                if d == 4 and dy == -way:
                    continue
                ref = self.rb.at[first + self.yi(dy)]
                if d == 4 and j != 1:
                    ref = self.half(ref, way)
                self.start(19 + 3 * d + j, ref, "z", way)

    def bz(self, d, j):
        count = (2 if j == 1 else 1) * (1 if d == 4 else 2)
        self.wait(19 + 3 * d + j, self.rb.at[pl.ds(0, count)])
        if d < 4:
            self.send_bz(d + 1, j)

    def half(self, ref, way):
        rows = ref.shape[0] // 2
        return ref.at[pl.ds(0 if way > 0 else rows, rows)]

    def drain(self):
        for n, ref in enumerate((self.ra, self.rb)):
            part = ref.at[pl.ds(0, SP - 1)]
            pltpu.make_async_copy(part, part, self.send.at[n]).wait()


RECVS = 34
OFFSETS = (0, -1, 1, -2, 2, -3, 3, 4)
ORDER = (
    "maps", "gaz 1", "gby 1", "line", "gbz 1 0", "gay 0", "gay -1", "gaz 2", "share", "gay 1",
    "gby 2", "gbz 1 1", "gbz 2 0", "scan", "out", "share2", "gay 2", "gaz 3", "gay -2", "gbz 1 2",
    "dbz 1 0", "daz 1", "last", "gbz 2 1", "gay -3", "gbz 3 0", "gaz 4", "gay 3", "gbz 2 2",
    "dby 1", "pass", "dbz 2 0", "day 0", "day -1", "proj", "day 1", "daz 2", "norm", "gbz 3 1",
    "gay 4", "dby 2", "gbz 3 2", "dbz 1 1", "dbz 3 0", "day -2", "daz 3", "day 2", "dbz 1 2",
    "gbz 4 0", "gbz 4 1", "gbz 4 2", "widen", "dal 1", "product 1", "dbz 2 1", "daz 4", "day -3",
    "day 3", "dbz 2 2", "dal -2", "product -2", "dal -1", "product -1", "combine 1", "dal 2",
    "product 2", "combine -2", "dal 0", "product 0", "combine -1", "combine 2", "dbz 3 1",
    "combine 0", "day 4", "dbz 3 2", "dal -3", "product -3", "dal 3", "product 3", "combine -3",
    "combine 3", "dbz 4 0", "dbz 4 1", "dbz 4 2", "dal 4", "product 4", "combine 4", "finish 1",
    "finish -2", "finish -1", "finish 2", "finish 0", "finish -3", "finish 3", "finish 4",
)


def row_of(block):
    return jnp.concatenate([block[g : g + 1, :] for g in range(G)], axis=1)


def rows_of(row):
    return jnp.concatenate([row[:, 128 * k : 128 * (k + 1)] for k in range(W // 128)], axis=0)


def flat_of(rows):
    return jnp.concatenate([rows[k : k + 1, :] for k in range(W // 128)], axis=1)


def kernel(
    mix_hbm, stream_hbm, docs_hbm, log_dt_hbm, decay_hbm, freq_hbm, in_real_hbm, in_imag_hbm,
    out_real_hbm, out_imag_hbm, skip_hbm, keep_hbm, proj_hbm, gain_hbm, gate_hbm, up_hbm, down_hbm,
    result,
    mix, stream, docs, log_dt, decay, freq, in_real, in_imag, out_real, out_imag, skip, log_keep,
    gain, gate_w, up_w, down_w,
    gua, gub, dna, dnb, drive, factor, states, maps, line, message, column, shared, mixes,
    branch, resid, normed, hidden, ffn_part, ffn_pair, ffn_send, ffn_recv,
    gu_send, gu_recv, dn_send, dn_recv, carry_sem, shared_sem, mix_sem, pair_sem, fs_send, fs_recv, load_sem,
):
    z, y, x, c = (lax.axis_index(a) for a in ("z", "y", "x", "c"))
    sp, tp = z * NY + y, x * NC + c

    def tp_peer(k):
        other = lax.rem(tp + k, TP)
        return other, {"x": other // NC, "c": lax.rem(other, NC)}

    def at_z(k):
        return {"z": lax.rem(z + k, NZ)}

    def at_y(k):
        return {"y": lax.rem(y + k, NY)}

    def at_x(k):
        return {"x": lax.rem(x + k, NX)}

    sibling = {"c": 1 - c}

    barrier = pltpu.get_barrier_semaphore()

    def greet(device):
        pl.semaphore_signal(barrier, inc=1, device_id=device, device_id_type=MESH)

    for k in (1, 7, 2, 6, 3, 5, 4):
        greet(at_z(k))
    for k in (1, 3, 2):
        greet(at_y(k))
    for k in range(1, TP):
        greet(tp_peer(k)[1])

    def push(source, target, sems, n, device):
        pltpu.make_async_remote_copy(
            src_ref=source, dst_ref=target, send_sem=sems.at[0, n], recv_sem=sems.at[1, n],
            device_id=device, device_id_type=MESH).start()

    def take(ref, sem):
        pltpu.make_async_copy(ref, ref, sem).wait()

    def load(n, *pairs):
        copies = [pltpu.make_async_copy(*pair, load_sem.at[n]) for pair in pairs]
        for copy in copies:
            copy.start()
        return copies

    def loaded(copies):
        for copy in copies:
            copy.wait()

    gate_load = load(0, (gate_hbm, gate_w))
    up_load = load(1, (up_hbm, up_w))
    gate_piece = load(2, (gate_hbm.at[:, pl.ds(0, MAIN)], gub.at[sp]))
    up_piece = load(3, (up_hbm.at[:, pl.ds(0, MAIN)], gua.at[sp, :, pl.ds(0, MAIN)]))
    down_load = load(17, (down_hbm, down_w))
    down_pieces = [
        load(18, (down_hbm.at[:, pl.ds(0, DA)], dna.at[sp])),
        load(19, (down_hbm.at[:, pl.ds(DA, DB)], dnb.at[sp, pl.ds(0, ROWS)])),
    ]
    scan_loads = [
        load(4 + n, pair) for n, pair in enumerate((
            (log_dt_hbm, log_dt), (decay_hbm, decay), (freq_hbm, freq), (mix_hbm, mix),
            (docs_hbm, docs), (keep_hbm, log_keep), (in_real_hbm, in_real), (in_imag_hbm, in_imag),
        ))
    ]
    share_loads = [
        load(12, (proj_hbm, shared.at[tp, pl.ds(0, CH)])),
        load(13, (stream_hbm, shared.at[tp, pl.ds(CH, TOK)])),
    ]
    map_loads = [
        load(n, pair) for n, pair in (
            (14, (out_real_hbm, out_real)), (15, (out_imag_hbm, out_imag)),
            (16, (stream_hbm, stream)), (20, (skip_hbm, skip)), (21, (gain_hbm, gain)),
        )
    ]
    loaded(gate_load)
    loaded(up_load)
    gua[sp, :, MAIN:GUA] = jnp.concatenate([gate_w[:, MAIN:FF], up_w[:, MAIN:FF]], axis=1)
    loaded(down_load)
    rest = down_w[:, MAIN:FF]
    dnb[sp, ROWS:DROWS] = jnp.concatenate([rest[: ROWS // 2], rest[ROWS // 2 :]], axis=1)

    gu = Relay(gua, gub, gu_send, gu_recv, z, y, True)
    dn = Relay(dna, dnb, dn_send, dn_recv, z, y, False)
    loaded(gate_piece)
    loaded(up_piece)
    pl.semaphore_wait(barrier, NZ - 1 + NY - 1 + TP - 1)
    gu.send_by(1)
    gu.send_bz(1, 0)
    gu.send_az(1)
    for copies in down_pieces:
        loaded(copies)
    dn.send_by(1)
    dn.send_ay(0)
    dn.send_az(1)
    dn.send_bz(1, 0)
    for copies in share_loads:
        loaded(copies)
    half = (CH + TOK) // 2
    for n, rows in ((0, (0, half)), (3, (half, 0))):
        for k, first in zip((1, 3), rows):
            ref = shared.at[tp, pl.ds(first, half)]
            push(ref, ref, shared_sem, n, at_x(k))
    push(shared.at[tp], shared.at[tp], shared_sem, 2, sibling)
    for copies in scan_loads:
        loaded(copies)

    group = iota((G, S), 0)
    steps = jnp.zeros((G, S), F32)
    for g in range(G):
        steps = jnp.where(group == g, log_dt[0:1, g : g + 1], steps)
    steps = jnp.exp(steps)
    rate, turn_rate = decay[...], freq[...]
    magnitude = jnp.exp(-steps * rate)
    angle = steps * turn_rate
    a_real, a_imag = magnitude * jnp.cos(angle), magnitude * jnp.sin(angle)
    below = rate * rate + turn_rate * turn_rate
    shifted = a_real - 1.0
    z_real = (-shifted * rate + a_imag * turn_rate) / below
    z_imag = (-a_imag * rate - shifted * turn_rate) / below
    ar, ai, zr, zi = (row_of(v) for v in (a_real, a_imag, z_real, z_imag))

    r, t = iota((T, T), 0), iota((T, T), 1)
    order = t == lax.rem(r, CHUNKS) * STEPS + r // CHUNKS
    order_f = one_hot(order, F32)
    u = dot(order_f.astype(BF16), mix[...])
    ub = u.astype(BF16)

    tile = one_hot(lax.rem(iota((S, W), 1), S) == iota((S, W), 0), BF16)
    own = lax.rem(iota((2 * CH, W), 0), CH) // GW == iota((2 * CH, W), 1) // S
    for n, ref in enumerate((in_real, in_imag)):
        high, low = (
            jnp.where(own, dot(half, tile), 0.0).astype(BF16) for half in halves(ref[...])
        )
        for d in range(2):
            at = slice(CH * d, CH * (d + 1))
            drive[:, W * (2 * n + d) : W * (2 * n + d + 1)] = dot(ub, high[at]) + dot(ub, low[at])

    doc = docs[...].astype(F32) + jnp.zeros((G, T), F32)
    place = iota((G, T), 1)
    before, after = pltpu.roll(doc, 1, 1), pltpu.roll(doc, T - 1, 1)
    keep = jnp.exp(log_keep[...])
    keep_f = jnp.where((place == 0) | (doc == before), keep, 0.0)
    keep_b = jnp.where((place == T - 1) | (doc == after), keep, 0.0)
    both = dot_nt(order_f, jnp.concatenate([keep_f, keep_b], axis=0), HIGHEST)
    spread = one_hot(iota((2 * G, 2 * W), 0) == iota((2 * G, 2 * W), 1) // S, F32)
    factor[...] = dot(both, spread, HIGHEST)

    zero = jnp.zeros((CHUNKS, W), F32)
    ar8, ai8 = zero + ar, zero + ai

    def advance(j, state, direction):
        at = pl.ds(pl.multiple_of(j * CHUNKS, CHUNKS), CHUNKS)
        f = factor[at, W * direction : W * (direction + 1)]
        dr = drive[at, W * direction : W * (direction + 1)]
        di = drive[at, W * (2 + direction) : W * (3 + direction)]
        hr, hi = state
        nr, ni = cmul(f * ar8, f * ai8, hr, hi)
        return f, nr + dr, ni + di

    def first(j, state):
        fr, fi, fp, br, bi, bp = state
        f, fr, fi = advance(j, (fr, fi), 0)
        b, br, bi = advance(STEPS - 1 - j, (br, bi), 1)
        return fr, fi, fp * f, br, bi, bp * b

    fr, fi, fp, br, bi, bp = lax.fori_loop(
        0, STEPS, first, (zero, zero, zero + 1.0, zero, zero, zero + 1.0)
    )
    pr, pi = ar, ai
    for _ in range(5):
        pr, pi = cmul(pr, pi, pr, pi)

    def chunk_entries(enter, hr, hi, passed, backward):
        er, ei = enter
        entries = [None] * CHUNKS
        chunks = range(CHUNKS - 1, -1, -1) if backward else range(CHUNKS)
        for k in chunks:
            entries[k] = (er, ei)
            f = passed[k : k + 1]
            nr, ni = cmul(f * pr, f * pi, er, ei)
            er, ei = nr + hr[k : k + 1], ni + hi[k : k + 1]
        return entries, (er, ei)

    none = (jnp.zeros((1, W), F32), jnp.zeros((1, W), F32))
    end_f = chunk_entries(none, fr, fi, fp, False)[1]
    end_b = chunk_entries(none, br, bi, bp, True)[1]
    passed = fp[0:1]
    for k in range(1, CHUNKS):
        passed = passed * fp[k : k + 1]
    qr, qi = pr, pi
    for _ in range(3):
        qr, qi = cmul(qr, qi, qr, qi)
    edge_first = jnp.broadcast_to(doc[0:1, 0:1], (1, 128))
    edge_last = jnp.broadcast_to(doc[0:1, T - 1 : T], (1, 128))
    passed_rows = rows_of(passed)
    edges = jnp.concatenate(
        [edge_first, edge_last, jnp.zeros((2, 128), F32)], axis=0)
    for n, (er, ei) in enumerate((end_f, end_b)):
        line[y, 8 * n : 8 * n + 4] = rows_of(er)
        line[y, 8 * n + 4 : 8 * n + 8] = rows_of(ei)
    line[y, 16:20] = passed_rows
    line[y, 20:24] = edges

    for k in (2, 1, 3):
        push(line.at[y], line.at[y], carry_sem, 0, at_y(k))
    gu.send_ay(0)

    def output_maps():
        for copies in map_loads:
            loaded(copies)
        spread = tile.astype(F32)
        cr = jnp.where(own, dot(out_real[...], spread, HIGHEST), 0.0)
        ci = jnp.where(own, dot(out_imag[...], spread, HIGHEST), 0.0)
        cr, ci = cmul(zr, zi, cr, ci)
        for n in range(4):
            read = (cr if n < 2 else -ci)[CH * (n % 2) : CH * (n % 2 + 1)]
            maps[0, n], maps[1, n] = halves(read)

    q4r, q4i = rows_of(qr), rows_of(qi)
    s4r, s4i = cmul(q4r, q4i, q4r, q4i)
    s4r, s4i = cmul(s4r, s4i, s4r, s4i)
    four = jnp.zeros((4, 128), F32)
    start = (four, four, jnp.zeros((1, 128), F32) - 1.0)

    def fold(state, m, side, power, passed, near, far, use):
        cr, ci, last = state
        link = jnp.where(m[near : near + 1] == last, 1.0, 0.0) * m[passed : passed + 4]
        nr, ni = cmul(link * power[0], link * power[1], cr, ci)
        cr = jnp.where(use, nr + m[side : side + 4], cr)
        ci = jnp.where(use, ni + m[side + 4 : side + 8], ci)
        return cr, ci, jnp.where(use, m[far : far + 1], last)

    def fold_line(state, backward, use):
        for k in range(NY - 1, -1, -1) if backward else range(NY):
            m = line[k]
            if backward:
                state = fold(state, m, 8, (q4r, q4i), 16, 21, 20, use(k))
            else:
                state = fold(state, m, 0, (q4r, q4i), 16, 20, 21, use(k))
        return state

    def carry_line():
        take(line.at[pl.ds(0, NY - 1)], carry_sem.at[1, 0])
        always = lambda k: k >= 0
        ends = fold_line(start, False, always), fold_line(start, True, always)
        passed = line[0][16:20]
        for k in range(1, NY):
            link = jnp.where(line[k][20:21] == line[k - 1][21:22], 1.0, 0.0)
            passed = passed * (link * line[k][16:20])
        edges = jnp.concatenate(
            [line[0][20:21], line[NY - 1][21:22], jnp.zeros((2, 128), F32)], axis=0)
        for n in range(2):
            message[n, 0:4] = ends[n][0]
            message[n, 4:8] = ends[n][1]
            message[n, 8:12] = passed
            message[n, 12:16] = edges
        column[z] = message[0]
        for k in (4, 3, 5, 2, 6, 1, 7):
            side = jnp.where(lax.rem(z + k, NZ) > z, 0, 1)
            push(message.at[side], column.at[z], carry_sem, 1, at_z(k))

    def carry_column():
        take(column.at[pl.ds(0, NZ - 1)], carry_sem.at[1, 1])
        forward, backward = start, start
        for k in range(NZ):
            forward = fold(forward, column[k], 0, (s4r, s4i), 8, 12, 13, k < z)
            j = NZ - 1 - k
            backward = fold(backward, column[j], 0, (s4r, s4i), 8, 13, 12, j > z)
        into_f = fold_line(forward, False, lambda k: k < y)
        into_b = fold_line(backward, True, lambda k: k > y)
        enter_f = jnp.where(into_f[2] == edge_first, 1.0, 0.0)
        enter_b = jnp.where(into_b[2] == edge_last, 1.0, 0.0)
        enter_f = (flat_of(into_f[0] * enter_f), flat_of(into_f[1] * enter_f))
        enter_b = (flat_of(into_b[0] * enter_b), flat_of(into_b[1] * enter_b))
        entries_f = chunk_entries(enter_f, fr, fi, fp, False)[0]
        entries_b = chunk_entries(enter_b, br, bi, bp, True)[0]
        return tuple(
            jnp.concatenate([e[part_no] for e in entries], axis=0)
            for entries in (entries_f, entries_b) for part_no in (0, 1)
        )

    def second(j, state):
        fr, fi, br, bi = state
        _, fr, fi = advance(j, (fr, fi), 0)
        k = STEPS - 1 - j
        _, br, bi = advance(k, (br, bi), 1)
        at = pl.ds(pl.multiple_of(j * CHUNKS, CHUNKS), CHUNKS)
        states[at, 0:W] = fr
        states[at, 2 * W : 3 * W] = fi
        at = pl.ds(pl.multiple_of(k * CHUNKS, CHUNKS), CHUNKS)
        states[at, W : 2 * W] = br
        states[at, 3 * W : 4 * W] = bi
        return fr, fi, br, bi

    def scan():
        lax.fori_loop(0, STEPS, second, carry_column())

    def mix_out():
        pre = skip[...] * u
        for n in range(4):
            high, low = halves(states[:, W * n : W * (n + 1)])
            pre = pre + dot_nt(high, maps[0, n]) + dot_nt(high, maps[1, n])
            pre = pre + dot_nt(low, maps[0, n])
        mixed = jax.nn.gelu(pre).astype(BF16)
        back = one_hot(t == lax.rem(r, STEPS) * CHUNKS + r // STEPS, BF16)
        mixes[tp] = dot(back, mixed).astype(BF16)
        for k in (2, 1, 3):
            push(mixes.at[tp], mixes.at[tp], mix_sem, 0, at_x(k))
        push(mixes.at[tp], mixes.at[tp], mix_sem, 1, sibling)

    def of_x(k):
        return lax.rem(x + k, NX) * NC + c

    def share():
        take(shared.at[0], shared_sem.at[1, 0])
        for k, first in ((1, half), (3, 0)):
            ref = shared.at[of_x(k), pl.ds(first, half)]
            push(ref, ref, shared_sem, 1, at_x(NX - k))

    def share_rest():
        take(shared.at[0], shared_sem.at[1, 3])
        for k in (1, 3):
            push(shared.at[of_x(k)], shared.at[of_x(k)], shared_sem, 2, sibling)

    def share_last():
        take(shared.at[0], shared_sem.at[1, 1])
        push(shared.at[of_x(2)], shared.at[of_x(2)], shared_sem, 2, sibling)

    def mix_pass():
        take(mixes.at[pl.ds(0, 3)], mix_sem.at[1, 0])
        for k in (1, 2, 3):
            push(mixes.at[of_x(k)], mixes.at[of_x(k)], mix_sem, 1, sibling)

    def project():
        take(shared.at[pl.ds(0, 4)], shared_sem.at[1, 2])
        take(mixes.at[pl.ds(0, 4)], mix_sem.at[1, 1])
        both = jnp.concatenate([mixes[k] for k in range(TP)], axis=1)
        branch[...] = dot(both, shared[:, 0:CH].reshape(TP * CH, D))

    def normalize():
        scales = gain[...]
        resid[...] = stream[...].astype(F32) + branch[pl.ds(pl.multiple_of(tp * TOK, TOK), TOK)]

        @pl.loop(0, TP)
        def _(k):
            at = pl.ds(pl.multiple_of(k * TOK, TOK), TOK)
            kept = shared[k, CH : CH + TOK].astype(F32) + branch[at]
            scale = lax.rsqrt(jnp.mean(kept * kept, axis=-1, keepdims=True) + 1e-6)
            normed[at] = (kept * scale * scales).astype(BF16)

    def widen():
        gu.all_al()
        rows = normed[...]
        second_part = dot(rows, gua[...].reshape(D, GUA))
        first_part = dot(rows, gub[...].reshape(D, GUB))
        hidden[:, 0:MAIN] = (jax.nn.silu(first_part) * second_part[:, 0:MAIN]).astype(BF16)
        tail_gate = second_part[:, MAIN:FF]
        tail_up = second_part[:, FF:GUA]
        tail = (jax.nn.silu(tail_gate) * tail_up).astype(BF16)
        empty = jnp.zeros((T, FF - MAIN), BF16)
        hidden[:, MAIN:KPAD] = jnp.concatenate([tail, empty, empty, tail], axis=1)

    def product(o):
        zi = gu.zi(o)
        at = pl.ds(zi * NY, NY)
        out = dot_nt(hidden[:, 0:DA], dna[at].reshape(NY * ROWS, DA))
        out = out + dot_nt(hidden[:, DA:MAIN], dnb[at, 0:ROWS].reshape(NY * ROWS, DB))
        rest = dnb[at, ROWS:DROWS].reshape(NY * ROWS // 2, DB)
        sides = [dot_nt(hidden[:, at : at + 128], rest) for at in (MAIN, MAIN + 128)]
        out = out + jnp.concatenate(
            [side[:, k : k + ROWS // 2] for k in range(0, 128, ROWS // 2) for side in sides], axis=1
        )
        out = out.astype(BF16).reshape(NX, NC, TOK, NY * ROWS)
        for k in range(NC):
            ffn_part[zi, k] = out[:, k]
        pltpu.make_async_remote_copy(
            src_ref=ffn_part.at[zi, 1 - c], dst_ref=ffn_pair.at[zi],
            send_sem=fs_send.at[1], recv_sem=pair_sem.at[zi],
            device_id=sibling, device_id_type=MESH).start()

    def combine(o):
        zi = gu.zi(o)
        take(ffn_pair.at[zi], pair_sem.at[zi])
        total = ffn_part[zi, c].astype(F32) + ffn_pair[zi].astype(F32)
        ffn_send[zi] = total.astype(BF16)
        for k in (2, 1, 3):
            pltpu.make_async_remote_copy(
                src_ref=ffn_send.at[zi, lax.rem(x + k, NX)], dst_ref=ffn_recv.at[zi, x],
                send_sem=fs_send.at[0], recv_sem=fs_recv.at[zi],
                device_id=at_x(k), device_id_type=MESH).start()
        ffn_recv[zi, x] = ffn_send[zi, x]

    def finish(o):
        zi = gu.zi(o)
        take(ffn_recv.at[zi, pl.ds(0, NX - 1)], fs_recv.at[zi])
        at = pl.ds(pl.multiple_of(zi * (NY * ROWS), NY * ROWS), NY * ROWS)
        ffn = ffn_recv[zi, 0].astype(F32)
        for k in range(1, NX):
            ffn = ffn + ffn_recv[zi, k].astype(F32)
        result[:, at] = (resid[:, at] + 0.5 * ffn).astype(BF16)

    steps = {
        "maps": output_maps, "line": carry_line, "scan": scan, "out": mix_out, "share": share,
        "share2": share_rest, "last": share_last,
        "pass": mix_pass, "proj": project, "norm": normalize, "widen": widen,
        "product": product, "combine": combine, "finish": finish,
    }
    for step in ORDER:
        name, number = step.split()[0], [int(n) for n in step.split()[1:]]
        if name[0] in "gd" and name[1:] in ("az", "ay", "al", "by", "bz"):
            getattr(gu if name[0] == "g" else dn, name[1:])(*number)
        else:
            steps[name](*number)

    gu.drain()
    dn.drain()
    take(line.at[pl.ds(0, NY - 1)], carry_sem.at[0, 0])
    take(column.at[pl.ds(0, NZ - 1)], carry_sem.at[0, 1])
    take(shared.at[0], shared_sem.at[0, 0])
    take(shared.at[0], shared_sem.at[0, 3])
    take(shared.at[0], shared_sem.at[0, 1])
    take(shared.at[pl.ds(0, 4)], shared_sem.at[0, 2])
    take(mixes.at[pl.ds(0, 3)], mix_sem.at[0, 0])
    take(mixes.at[pl.ds(0, 4)], mix_sem.at[0, 1])
    take(ffn_recv.at[pl.ds(0, NZ * (NX - 1) // NX)], fs_send.at[0])
    take(ffn_pair, fs_send.at[1])


def by_channel(maps):
    return jnp.swapaxes(maps, 2, 3).reshape(2 * CH, S)


def local(
    mix_input, stream, doc_ids, log_dt, decay_rate, frequency, input_real, input_imag,
    output_real, output_imag, skip_gain, log_keep, proj_weight, norm_gain, gate_weight,
    up_weight, down_weight,
):
    vmem = pl.BlockSpec(memory_space=pltpu.VMEM)
    specs = [pl.BlockSpec(memory_space=pl.ANY)] * 17
    dma = pltpu.SemaphoreType.DMA
    scratch = [
        pltpu.VMEM((T, CH), BF16),
        pltpu.VMEM((TOK, D), BF16),
        pltpu.VMEM((1, T), jnp.int32),
        pltpu.VMEM((1, G), F32),
        pltpu.VMEM((G, S), F32),
        pltpu.VMEM((G, S), F32),
        pltpu.VMEM((2 * CH, S), F32),
        pltpu.VMEM((2 * CH, S), F32),
        pltpu.VMEM((2 * CH, S), F32),
        pltpu.VMEM((2 * CH, S), F32),
        pltpu.VMEM((1, CH), F32),
        pltpu.VMEM((G, T), F32),
        pltpu.VMEM((1, D), F32),
        pltpu.VMEM((ROWS, FF), BF16),
        pltpu.VMEM((ROWS, FF), BF16),
        pltpu.VMEM((ROWS, FF), BF16),
        pltpu.VMEM((SP, ROWS, GUA), BF16),
        pltpu.VMEM((SP, ROWS, GUB), BF16),
        pltpu.VMEM((SP, ROWS, DA), BF16),
        pltpu.VMEM((SP, DROWS, DB), BF16),
        pltpu.VMEM((T, 4 * W), F32),
        pltpu.VMEM((T, 2 * W), F32),
        pltpu.VMEM((T, 4 * W), F32),
        pltpu.VMEM((2, 4, CH, W), BF16),
        pltpu.VMEM((NY, 24, 128), F32),
        pltpu.VMEM((2, 16, 128), F32),
        pltpu.VMEM((NZ, 16, 128), F32),
        pltpu.VMEM((TP, CH + TOK, D), BF16),
        pltpu.VMEM((TP, T, CH), BF16),
        pltpu.VMEM((T, D), F32),
        pltpu.VMEM((TOK, D), F32),
        pltpu.VMEM((T, D), BF16),
        pltpu.VMEM((T, KPAD), BF16),
        pltpu.VMEM((NZ, NC, NX, TOK, NY * ROWS), BF16),
        pltpu.VMEM((NZ, NX, TOK, NY * ROWS), BF16),
        pltpu.VMEM((NZ, NX, TOK, NY * ROWS), BF16),
        pltpu.VMEM((NZ, NX, TOK, NY * ROWS), BF16),
        dma((2,)), dma((RECVS,)), dma((2,)), dma((RECVS,)),
        dma((2, 2)), dma((2, 4)), dma((2, 2)), dma((NZ,)), dma((2,)), dma((NZ,)), dma((22,)),
    ]
    return pl.pallas_call(
        kernel,
        out_shape=pltpu.VMEM((TOK, D), BF16),
        in_specs=specs,
        out_specs=vmem,
        scratch_shapes=scratch,
        compiler_params=pltpu.CompilerParams(
            collective_id=0, has_side_effects=True, vmem_limit_bytes=60 << 20
        ),
        name="layer",
    )(
        mix_input, stream, doc_ids.reshape(1, T), log_dt.reshape(1, G), decay_rate, frequency,
        by_channel(input_real), by_channel(input_imag),
        output_real.reshape(2 * CH, S), output_imag.reshape(2 * CH, S),
        skip_gain.reshape(1, CH), log_keep, proj_weight, norm_gain.reshape(1, D),
        gate_weight, up_weight, down_weight.T,
    )


def solution(mesh):
    torus = Mesh(mesh.devices.reshape(NZ, NY, NX, NC), ("z", "y", "x", "c"))
    sp, tp = ("z", "y"), ("x", "c")
    every = ("z", "y", "x", "c")
    in_specs = (
        P(sp, tp), P(every, None), P(sp), P(tp), P(tp, None), P(tp, None),
        P(None, tp, None, None), P(None, tp, None, None),
        P(None, tp, None, None), P(None, tp, None, None),
        P(tp), P(tp, sp), P(tp, None), P(), P(sp, tp), P(sp, tp), P(tp, sp),
    )
    return jax.shard_map(
        local, mesh=torus, in_specs=in_specs, out_specs=P(every, None), check_vma=False
    )
```

```python
import functools

import jax
import jax.numpy as jnp
from jax import lax
from jax.experimental import pallas as pl
from jax.experimental.pallas import tpu as pltpu
from jax.sharding import Mesh
from jax.sharding import PartitionSpec as P

HIGHEST = lax.Precision.HIGHEST
MESH = pl.DeviceIdType.MESH
F32, BF16 = jnp.float32, jnp.bfloat16

NZ, NY, NX, NC = 8, 4, 4, 2
SP, TP = NZ * NY, NX * NC
T, CH, G, S, GW = 256, 128, 8, 64, 16
W = G * S
CHUNKS = 8
STEPS = T // CHUNKS
D = 2048
FF = 704
MAIN = 640
ROWS = D // SP
TOK = T // TP
GUA, GUB = MAIN + 128, MAIN
DA, DB = 512, 128
DROWS = ROWS + ROWS // 2
KPAD = MAIN + 256
NT = (((1,), (1,)), ((), ()))


def dot(a, b, precision=None):
    return jnp.dot(a, b, preferred_element_type=F32, precision=precision)


def dot_nt(a, b, precision=None):
    return lax.dot_general(a, b, NT, preferred_element_type=F32, precision=precision)


def halves(value):
    high = value.astype(BF16)
    return high, (value - high.astype(F32)).astype(BF16)


def iota(shape, dim):
    return lax.broadcasted_iota(jnp.int32, shape, dim)


def one_hot(mask, dtype):
    return jnp.where(mask, 1.0, 0.0).astype(F32).astype(dtype)


def cmul(ar, ai, br, bi):
    return ar * br - ai * bi, ar * bi + ai * br


class Relay:
    def __init__(self, ra, rb, send, recv, z, y, joint):
        self.ra, self.rb, self.send, self.recv = ra, rb, send, recv
        self.z, self.y, self.joint = z, y, joint

    def zi(self, offset):
        return lax.rem(self.z + (offset + NZ), NZ)

    def yi(self, offset):
        return lax.rem(self.y + (offset + NY), NY)

    def start(self, number, ref, axis, to):
        pltpu.make_async_remote_copy(
            src_ref=ref,
            dst_ref=ref,
            send_sem=self.send.at[0 if number < 20 else 1],
            recv_sem=self.recv.at[number],
            device_id={axis: self.zi(to) if axis == "z" else self.yi(to)},
            device_id_type=MESH,
        ).start()

    def wait(self, number, ref):
        pltpu.make_async_copy(ref, ref, self.recv.at[number]).wait()

    def a(self, dz, dy):
        return self.ra.at[self.zi(dz) * NY + self.yi(dy)]

    def send_az(self, d):
        for way in (1, -1):
            ref = self.a(-way * (d - 1), 0)
            if d == 4:
                ref = self.half(ref, way)
            self.start(d - 1, ref, "z", way)

    def send_ay(self, o):
        for way in (1, -1):
            self.start(4 + o % NZ, self.a(o, 0), "y", way)

    def az(self, d):
        self.wait(d - 1, self.ra.at[0] if d == 4 else self.ra.at[pl.ds(0, 2)])
        if d < 4:
            self.send_az(d + 1)
        for o in (4,) if d == 4 else (-d, d):
            self.send_ay(o)

    def ay(self, o):
        self.wait(4 + o % NZ, self.ra.at[pl.ds(0, 2)])
        way = 1 if o % 2 == 0 else -1
        self.start(12 + (0 if self.joint else o % NZ), self.a(o, -way), "y", way)

    def al(self, o):
        self.wait(12 + o % NZ, self.ra.at[0])

    def all_al(self):
        self.wait(12, self.ra.at[pl.ds(0, NZ)])

    def send_by(self, d):
        for way in (1, -1):
            ref = self.rb.at[self.z * NY + self.yi(-way * (d - 1))]
            if d == 2:
                ref = self.half(ref, way)
            self.start(19 + d, ref, "y", way)

    def by(self, d):
        self.wait(19 + d, self.rb.at[pl.ds(0, 2)] if d == 1 else self.rb.at[0])
        if d == 1:
            self.send_by(2)
        self.send_bz(1, d)

    def send_bz(self, d, j):
        for way in (1, -1):
            first = self.zi(-way * (d - 1)) * NY
            for dy in ((0,), (1, -1), (2,))[j]:
                if d == 4 and dy == -way:
                    continue
                ref = self.rb.at[first + self.yi(dy)]
                if d == 4 and j != 1:
                    ref = self.half(ref, way)
                self.start(19 + 3 * d + j, ref, "z", way)

    def bz(self, d, j):
        count = (2 if j == 1 else 1) * (1 if d == 4 else 2)
        self.wait(19 + 3 * d + j, self.rb.at[pl.ds(0, count)])
        if d < 4:
            self.send_bz(d + 1, j)

    def half(self, ref, way):
        rows = ref.shape[0] // 2
        return ref.at[pl.ds(0 if way > 0 else rows, rows)]

    def drain(self):
        for n, ref in enumerate((self.ra, self.rb)):
            part = ref.at[pl.ds(0, SP - 1)]
            pltpu.make_async_copy(part, part, self.send.at[n]).wait()


RECVS = 34
OFFSETS = (0, -1, 1, -2, 2, -3, 3, 4)
ORDER = (
    "gby 1", "dby 1", "gaz 1", "line", "day 0", "gby 2", "daz 1", "gaz 2", "gbz 1 0", "gay 0",
    "share", "gbz 1 2", "gay -1", "share2", "gay -2", "day -1", "maps", "gbz 1 1", "gaz 3",
    "scan", "gbz 2 0", "gay 1", "out", "gay 2", "gbz 2 2", "gbz 2 1", "gay -3", "last", "gaz 4",
    "daz 2", "gbz 3 0", "gbz 3 2", "dby 2", "gay 3", "pass", "gbz 3 1", "gay 4", "day 1", "day 2",
    "daz 3", "dbz 1 1", "proj", "dbz 1 0", "dbz 1 2", "day -2", "norm", "gbz 4 0", "gbz 4 1",
    "gbz 4 2", "widen", "daz 4", "dbz 2 1", "dal 1", "product 1", "dbz 2 0", "dal -1",
    "product -1", "day -3", "day 3", "dbz 2 2", "combine 1", "dal 0", "product 0", "combine -1",
    "dal 2", "product 2", "dal -2", "product -2", "dbz 3 1", "combine 0", "dbz 3 0", "day 4",
    "dbz 3 2", "combine -2", "dal -3", "product -3", "dal 3", "product 3", "combine 2",
    "combine -3", "dbz 4 0", "dbz 4 1", "dbz 4 2", "dal 4", "product 4", "combine 3", "combine 4",
    "finish 1", "finish -1", "finish 0", "finish -2", "finish 2", "finish -3", "finish 3",
    "finish 4",
)


def row_of(block):
    return jnp.concatenate([block[g : g + 1, :] for g in range(G)], axis=1)


def rows_of(row):
    return jnp.concatenate([row[:, 128 * k : 128 * (k + 1)] for k in range(W // 128)], axis=0)


def flat_of(rows):
    return jnp.concatenate([rows[k : k + 1, :] for k in range(W // 128)], axis=1)


def kernel(
    mix_hbm, stream_hbm, docs_hbm, log_dt_hbm, decay_hbm, freq_hbm, in_real_hbm, in_imag_hbm,
    out_real_hbm, out_imag_hbm, skip_hbm, keep_hbm, proj_hbm, gain_hbm, gate_hbm, up_hbm, down_hbm,
    result,
    mix, stream, docs, log_dt, decay, freq, in_real, in_imag, out_real, out_imag, skip, log_keep,
    gain, gate_w, up_w, down_w,
    gua, gub, dna, dnb, drive, factor, states, maps, line, message, column, shared, mixes,
    branch, resid, normed, hidden, ffn_part, ffn_pair, ffn_send, ffn_recv,
    gu_send, gu_recv, dn_send, dn_recv, carry_sem, shared_sem, mix_sem, pair_sem, fs_send, fs_recv, load_sem,
):
    z, y, x, c = (lax.axis_index(a) for a in ("z", "y", "x", "c"))
    sp, tp = z * NY + y, x * NC + c

    def tp_peer(k):
        other = lax.rem(tp + k, TP)
        return other, {"x": other // NC, "c": lax.rem(other, NC)}

    def at_z(k):
        return {"z": lax.rem(z + k, NZ)}

    def at_y(k):
        return {"y": lax.rem(y + k, NY)}

    def at_x(k):
        return {"x": lax.rem(x + k, NX)}

    sibling = {"c": 1 - c}

    barrier = pltpu.get_barrier_semaphore()

    def greet(device):
        pl.semaphore_signal(barrier, inc=1, device_id=device, device_id_type=MESH)

    for k in (1, 7, 2, 6, 3, 5, 4):
        greet(at_z(k))
    for k in (1, 3, 2):
        greet(at_y(k))
    for k in range(1, TP):
        greet(tp_peer(k)[1])

    def push(source, target, sems, n, device):
        pltpu.make_async_remote_copy(
            src_ref=source, dst_ref=target, send_sem=sems.at[0, n], recv_sem=sems.at[1, n],
            device_id=device, device_id_type=MESH).start()

    def take(ref, sem):
        pltpu.make_async_copy(ref, ref, sem).wait()

    def load(n, *pairs):
        copies = [pltpu.make_async_copy(*pair, load_sem.at[n]) for pair in pairs]
        for copy in copies:
            copy.start()
        return copies

    def loaded(copies):
        for copy in copies:
            copy.wait()

    gate_load = load(0, (gate_hbm, gate_w))
    up_load = load(1, (up_hbm, up_w))
    gate_piece = load(2, (gate_hbm.at[:, pl.ds(0, MAIN)], gub.at[sp]))
    up_piece = load(3, (up_hbm.at[:, pl.ds(0, MAIN)], gua.at[sp, :, pl.ds(0, MAIN)]))
    down_load = load(17, (down_hbm, down_w))
    down_pieces = [
        load(18, (down_hbm.at[:, pl.ds(0, DA)], dna.at[sp])),
        load(19, (down_hbm.at[:, pl.ds(DA, DB)], dnb.at[sp, pl.ds(0, ROWS)])),
    ]
    scan_loads = [
        load(4 + n, pair) for n, pair in enumerate((
            (log_dt_hbm, log_dt), (decay_hbm, decay), (freq_hbm, freq), (mix_hbm, mix),
            (docs_hbm, docs), (keep_hbm, log_keep), (in_real_hbm, in_real), (in_imag_hbm, in_imag),
        ))
    ]
    share_loads = [
        load(12, (proj_hbm, shared.at[tp, pl.ds(0, CH)])),
        load(13, (stream_hbm, shared.at[tp, pl.ds(CH, TOK)])),
    ]
    map_loads = [
        load(n, pair) for n, pair in (
            (14, (out_real_hbm, out_real)), (15, (out_imag_hbm, out_imag)),
            (16, (stream_hbm, stream)), (20, (skip_hbm, skip)), (21, (gain_hbm, gain)),
        )
    ]
    loaded(gate_load)
    loaded(up_load)
    gua[sp, :, MAIN:GUA] = jnp.concatenate([gate_w[:, MAIN:FF], up_w[:, MAIN:FF]], axis=1)
    loaded(down_load)
    rest = down_w[:, MAIN:FF]
    dnb[sp, ROWS:DROWS] = jnp.concatenate([rest[: ROWS // 2], rest[ROWS // 2 :]], axis=1)

    gu = Relay(gua, gub, gu_send, gu_recv, z, y, True)
    dn = Relay(dna, dnb, dn_send, dn_recv, z, y, False)
    loaded(gate_piece)
    loaded(up_piece)
    pl.semaphore_wait(barrier, NZ - 1 + NY - 1 + TP - 1)
    gu.send_by(1)
    gu.send_bz(1, 0)
    gu.send_az(1)
    for copies in down_pieces:
        loaded(copies)
    dn.send_by(1)
    dn.send_ay(0)
    dn.send_az(1)
    dn.send_bz(1, 0)
    for copies in share_loads:
        loaded(copies)
    half = (CH + TOK) // 2
    for n, rows in ((0, (0, half)), (3, (half, 0))):
        for k, first in zip((1, 3), rows):
            ref = shared.at[tp, pl.ds(first, half)]
            push(ref, ref, shared_sem, n, at_x(k))
    push(shared.at[tp], shared.at[tp], shared_sem, 2, sibling)
    for copies in scan_loads:
        loaded(copies)

    group = iota((G, S), 0)
    steps = jnp.zeros((G, S), F32)
    for g in range(G):
        steps = jnp.where(group == g, log_dt[0:1, g : g + 1], steps)
    steps = jnp.exp(steps)
    rate, turn_rate = decay[...], freq[...]
    magnitude = jnp.exp(-steps * rate)
    angle = steps * turn_rate
    a_real, a_imag = magnitude * jnp.cos(angle), magnitude * jnp.sin(angle)
    below = rate * rate + turn_rate * turn_rate
    shifted = a_real - 1.0
    z_real = (-shifted * rate + a_imag * turn_rate) / below
    z_imag = (-a_imag * rate - shifted * turn_rate) / below
    ar, ai, zr, zi = (row_of(v) for v in (a_real, a_imag, z_real, z_imag))

    r, t = iota((T, T), 0), iota((T, T), 1)
    order = t == lax.rem(r, CHUNKS) * STEPS + r // CHUNKS
    order_f = one_hot(order, F32)
    u = dot(order_f.astype(BF16), mix[...])
    ub = u.astype(BF16)

    tile = one_hot(lax.rem(iota((S, W), 1), S) == iota((S, W), 0), BF16)
    own = lax.rem(iota((2 * CH, W), 0), CH) // GW == iota((2 * CH, W), 1) // S
    for n, ref in enumerate((in_real, in_imag)):
        high, low = (
            jnp.where(own, dot(half, tile), 0.0).astype(BF16) for half in halves(ref[...])
        )
        for d in range(2):
            at = slice(CH * d, CH * (d + 1))
            drive[:, W * (2 * n + d) : W * (2 * n + d + 1)] = dot(ub, high[at]) + dot(ub, low[at])

    doc = docs[...].astype(F32) + jnp.zeros((G, T), F32)
    place = iota((G, T), 1)
    before, after = pltpu.roll(doc, 1, 1), pltpu.roll(doc, T - 1, 1)
    keep = jnp.exp(log_keep[...])
    keep_f = jnp.where((place == 0) | (doc == before), keep, 0.0)
    keep_b = jnp.where((place == T - 1) | (doc == after), keep, 0.0)
    both = dot_nt(order_f, jnp.concatenate([keep_f, keep_b], axis=0), HIGHEST)
    spread = one_hot(iota((2 * G, 2 * W), 0) == iota((2 * G, 2 * W), 1) // S, F32)
    factor[...] = dot(both, spread, HIGHEST)

    zero = jnp.zeros((CHUNKS, W), F32)
    ar8, ai8 = zero + ar, zero + ai

    def advance(j, state, direction):
        at = pl.ds(pl.multiple_of(j * CHUNKS, CHUNKS), CHUNKS)
        f = factor[at, W * direction : W * (direction + 1)]
        dr = drive[at, W * direction : W * (direction + 1)]
        di = drive[at, W * (2 + direction) : W * (3 + direction)]
        hr, hi = state
        nr, ni = cmul(f * ar8, f * ai8, hr, hi)
        return f, nr + dr, ni + di

    def first(j, state):
        fr, fi, fp, br, bi, bp = state
        f, fr, fi = advance(j, (fr, fi), 0)
        b, br, bi = advance(STEPS - 1 - j, (br, bi), 1)
        return fr, fi, fp * f, br, bi, bp * b

    fr, fi, fp, br, bi, bp = lax.fori_loop(
        0, STEPS, first, (zero, zero, zero + 1.0, zero, zero, zero + 1.0)
    )
    pr, pi = ar, ai
    for _ in range(5):
        pr, pi = cmul(pr, pi, pr, pi)

    def chunk_entries(enter, hr, hi, passed, backward):
        er, ei = enter
        entries = [None] * CHUNKS
        chunks = range(CHUNKS - 1, -1, -1) if backward else range(CHUNKS)
        for k in chunks:
            entries[k] = (er, ei)
            f = passed[k : k + 1]
            nr, ni = cmul(f * pr, f * pi, er, ei)
            er, ei = nr + hr[k : k + 1], ni + hi[k : k + 1]
        return entries, (er, ei)

    none = (jnp.zeros((1, W), F32), jnp.zeros((1, W), F32))
    end_f = chunk_entries(none, fr, fi, fp, False)[1]
    end_b = chunk_entries(none, br, bi, bp, True)[1]
    passed = fp[0:1]
    for k in range(1, CHUNKS):
        passed = passed * fp[k : k + 1]
    qr, qi = pr, pi
    for _ in range(3):
        qr, qi = cmul(qr, qi, qr, qi)
    edge_first = jnp.broadcast_to(doc[0:1, 0:1], (1, 128))
    edge_last = jnp.broadcast_to(doc[0:1, T - 1 : T], (1, 128))
    passed_rows = rows_of(passed)
    edges = jnp.concatenate(
        [edge_first, edge_last, jnp.zeros((2, 128), F32)], axis=0)
    for n, (er, ei) in enumerate((end_f, end_b)):
        line[y, 8 * n : 8 * n + 4] = rows_of(er)
        line[y, 8 * n + 4 : 8 * n + 8] = rows_of(ei)
    line[y, 16:20] = passed_rows
    line[y, 20:24] = edges

    for k in (2, 1, 3):
        push(line.at[y], line.at[y], carry_sem, 0, at_y(k))
    gu.send_ay(0)

    def output_maps():
        for copies in map_loads:
            loaded(copies)
        spread = tile.astype(F32)
        cr = jnp.where(own, dot(out_real[...], spread, HIGHEST), 0.0)
        ci = jnp.where(own, dot(out_imag[...], spread, HIGHEST), 0.0)
        cr, ci = cmul(zr, zi, cr, ci)
        for n in range(4):
            read = (cr if n < 2 else -ci)[CH * (n % 2) : CH * (n % 2 + 1)]
            maps[0, n], maps[1, n] = halves(read)

    q4r, q4i = rows_of(qr), rows_of(qi)
    s4r, s4i = cmul(q4r, q4i, q4r, q4i)
    s4r, s4i = cmul(s4r, s4i, s4r, s4i)
    four = jnp.zeros((4, 128), F32)
    start = (four, four, jnp.zeros((1, 128), F32) - 1.0)

    def fold(state, m, side, power, passed, near, far, use):
        cr, ci, last = state
        link = jnp.where(m[near : near + 1] == last, 1.0, 0.0) * m[passed : passed + 4]
        nr, ni = cmul(link * power[0], link * power[1], cr, ci)
        cr = jnp.where(use, nr + m[side : side + 4], cr)
        ci = jnp.where(use, ni + m[side + 4 : side + 8], ci)
        return cr, ci, jnp.where(use, m[far : far + 1], last)

    def fold_line(state, backward, use):
        for k in range(NY - 1, -1, -1) if backward else range(NY):
            m = line[k]
            if backward:
                state = fold(state, m, 8, (q4r, q4i), 16, 21, 20, use(k))
            else:
                state = fold(state, m, 0, (q4r, q4i), 16, 20, 21, use(k))
        return state

    def carry_line():
        take(line.at[pl.ds(0, NY - 1)], carry_sem.at[1, 0])
        always = lambda k: k >= 0
        ends = fold_line(start, False, always), fold_line(start, True, always)
        passed = line[0][16:20]
        for k in range(1, NY):
            link = jnp.where(line[k][20:21] == line[k - 1][21:22], 1.0, 0.0)
            passed = passed * (link * line[k][16:20])
        edges = jnp.concatenate(
            [line[0][20:21], line[NY - 1][21:22], jnp.zeros((2, 128), F32)], axis=0)
        for n in range(2):
            message[n, 0:4] = ends[n][0]
            message[n, 4:8] = ends[n][1]
            message[n, 8:12] = passed
            message[n, 12:16] = edges
        column[z] = message[0]
        for k in (4, 3, 5, 2, 6, 1, 7):
            side = jnp.where(lax.rem(z + k, NZ) > z, 0, 1)
            push(message.at[side], column.at[z], carry_sem, 1, at_z(k))

    def carry_column():
        take(column.at[pl.ds(0, NZ - 1)], carry_sem.at[1, 1])
        forward, backward = start, start
        for k in range(NZ):
            forward = fold(forward, column[k], 0, (s4r, s4i), 8, 12, 13, k < z)
            j = NZ - 1 - k
            backward = fold(backward, column[j], 0, (s4r, s4i), 8, 13, 12, j > z)
        into_f = fold_line(forward, False, lambda k: k < y)
        into_b = fold_line(backward, True, lambda k: k > y)
        enter_f = jnp.where(into_f[2] == edge_first, 1.0, 0.0)
        enter_b = jnp.where(into_b[2] == edge_last, 1.0, 0.0)
        enter_f = (flat_of(into_f[0] * enter_f), flat_of(into_f[1] * enter_f))
        enter_b = (flat_of(into_b[0] * enter_b), flat_of(into_b[1] * enter_b))
        entries_f = chunk_entries(enter_f, fr, fi, fp, False)[0]
        entries_b = chunk_entries(enter_b, br, bi, bp, True)[0]
        return tuple(
            jnp.concatenate([e[part_no] for e in entries], axis=0)
            for entries in (entries_f, entries_b) for part_no in (0, 1)
        )

    def second(j, state):
        fr, fi, br, bi = state
        _, fr, fi = advance(j, (fr, fi), 0)
        k = STEPS - 1 - j
        _, br, bi = advance(k, (br, bi), 1)
        at = pl.ds(pl.multiple_of(j * CHUNKS, CHUNKS), CHUNKS)
        states[at, 0:W] = fr
        states[at, 2 * W : 3 * W] = fi
        at = pl.ds(pl.multiple_of(k * CHUNKS, CHUNKS), CHUNKS)
        states[at, W : 2 * W] = br
        states[at, 3 * W : 4 * W] = bi
        return fr, fi, br, bi

    def scan():
        lax.fori_loop(0, STEPS, second, carry_column())

    def mix_out():
        pre = skip[...] * u
        for n in range(4):
            high, low = halves(states[:, W * n : W * (n + 1)])
            pre = pre + dot_nt(high, maps[0, n]) + dot_nt(high, maps[1, n])
            pre = pre + dot_nt(low, maps[0, n])
        mixed = jax.nn.gelu(pre).astype(BF16)
        back = one_hot(t == lax.rem(r, STEPS) * CHUNKS + r // STEPS, BF16)
        mixes[tp] = dot(back, mixed).astype(BF16)
        for k in (2, 1, 3):
            push(mixes.at[tp], mixes.at[tp], mix_sem, 0, at_x(k))
        push(mixes.at[tp], mixes.at[tp], mix_sem, 1, sibling)

    def of_x(k):
        return lax.rem(x + k, NX) * NC + c

    def share():
        take(shared.at[0], shared_sem.at[1, 0])
        for k, first in ((1, half), (3, 0)):
            ref = shared.at[of_x(k), pl.ds(first, half)]
            push(ref, ref, shared_sem, 1, at_x(NX - k))

    def share_rest():
        take(shared.at[0], shared_sem.at[1, 3])
        for k in (1, 3):
            push(shared.at[of_x(k)], shared.at[of_x(k)], shared_sem, 2, sibling)

    def share_last():
        take(shared.at[0], shared_sem.at[1, 1])
        push(shared.at[of_x(2)], shared.at[of_x(2)], shared_sem, 2, sibling)

    def mix_pass():
        take(mixes.at[pl.ds(0, 3)], mix_sem.at[1, 0])
        for k in (1, 2, 3):
            push(mixes.at[of_x(k)], mixes.at[of_x(k)], mix_sem, 1, sibling)

    def project():
        take(shared.at[pl.ds(0, 4)], shared_sem.at[1, 2])
        take(mixes.at[pl.ds(0, 4)], mix_sem.at[1, 1])
        both = jnp.concatenate([mixes[k] for k in range(TP)], axis=1)
        branch[...] = dot(both, shared[:, 0:CH].reshape(TP * CH, D))

    def normalize():
        scales = gain[...]
        resid[...] = stream[...].astype(F32) + branch[pl.ds(pl.multiple_of(tp * TOK, TOK), TOK)]

        @pl.loop(0, TP)
        def _(k):
            at = pl.ds(pl.multiple_of(k * TOK, TOK), TOK)
            kept = shared[k, CH : CH + TOK].astype(F32) + branch[at]
            scale = lax.rsqrt(jnp.mean(kept * kept, axis=-1, keepdims=True) + 1e-6)
            normed[at] = (kept * scale * scales).astype(BF16)

    def widen():
        gu.all_al()
        rows = normed[...]
        second_part = dot(rows, gua[...].reshape(D, GUA))
        first_part = dot(rows, gub[...].reshape(D, GUB))
        hidden[:, 0:MAIN] = (jax.nn.silu(first_part) * second_part[:, 0:MAIN]).astype(BF16)
        tail_gate = second_part[:, MAIN:FF]
        tail_up = second_part[:, FF:GUA]
        tail = (jax.nn.silu(tail_gate) * tail_up).astype(BF16)
        empty = jnp.zeros((T, FF - MAIN), BF16)
        hidden[:, MAIN:KPAD] = jnp.concatenate([tail, empty, empty, tail], axis=1)

    def product(o):
        zi = gu.zi(o)
        at = pl.ds(zi * NY, NY)
        out = dot_nt(hidden[:, 0:DA], dna[at].reshape(NY * ROWS, DA))
        out = out + dot_nt(hidden[:, DA:MAIN], dnb[at, 0:ROWS].reshape(NY * ROWS, DB))
        rest = dnb[at, ROWS:DROWS].reshape(NY * ROWS // 2, DB)
        sides = [dot_nt(hidden[:, at : at + 128], rest) for at in (MAIN, MAIN + 128)]
        out = out + jnp.concatenate(
            [side[:, k : k + ROWS // 2] for k in range(0, 128, ROWS // 2) for side in sides], axis=1
        )
        out = out.astype(BF16).reshape(NX, NC, TOK, NY * ROWS)
        for k in range(NC):
            ffn_part[zi, k] = out[:, k]
        pltpu.make_async_remote_copy(
            src_ref=ffn_part.at[zi, 1 - c], dst_ref=ffn_pair.at[zi],
            send_sem=fs_send.at[1], recv_sem=pair_sem.at[zi],
            device_id=sibling, device_id_type=MESH).start()

    def combine(o):
        zi = gu.zi(o)
        take(ffn_pair.at[zi], pair_sem.at[zi])
        total = ffn_part[zi, c].astype(F32) + ffn_pair[zi].astype(F32)
        ffn_send[zi] = total.astype(BF16)
        for k in (2, 1, 3):
            pltpu.make_async_remote_copy(
                src_ref=ffn_send.at[zi, lax.rem(x + k, NX)], dst_ref=ffn_recv.at[zi, x],
                send_sem=fs_send.at[0], recv_sem=fs_recv.at[zi],
                device_id=at_x(k), device_id_type=MESH).start()
        ffn_recv[zi, x] = ffn_send[zi, x]

    def finish(o):
        zi = gu.zi(o)
        take(ffn_recv.at[zi, pl.ds(0, NX - 1)], fs_recv.at[zi])
        at = pl.ds(pl.multiple_of(zi * (NY * ROWS), NY * ROWS), NY * ROWS)
        ffn = ffn_recv[zi, 0].astype(F32)
        for k in range(1, NX):
            ffn = ffn + ffn_recv[zi, k].astype(F32)
        result[:, at] = (resid[:, at] + 0.5 * ffn).astype(BF16)

    steps = {
        "maps": output_maps, "line": carry_line, "scan": scan, "out": mix_out, "share": share,
        "share2": share_rest, "last": share_last,
        "pass": mix_pass, "proj": project, "norm": normalize, "widen": widen,
        "product": product, "combine": combine, "finish": finish,
    }
    for step in ORDER:
        name, number = step.split()[0], [int(n) for n in step.split()[1:]]
        if name[0] in "gd" and name[1:] in ("az", "ay", "al", "by", "bz"):
            getattr(gu if name[0] == "g" else dn, name[1:])(*number)
        else:
            steps[name](*number)

    gu.drain()
    dn.drain()
    take(line.at[pl.ds(0, NY - 1)], carry_sem.at[0, 0])
    take(column.at[pl.ds(0, NZ - 1)], carry_sem.at[0, 1])
    take(shared.at[0], shared_sem.at[0, 0])
    take(shared.at[0], shared_sem.at[0, 3])
    take(shared.at[0], shared_sem.at[0, 1])
    take(shared.at[pl.ds(0, 4)], shared_sem.at[0, 2])
    take(mixes.at[pl.ds(0, 3)], mix_sem.at[0, 0])
    take(mixes.at[pl.ds(0, 4)], mix_sem.at[0, 1])
    take(ffn_recv.at[pl.ds(0, NZ * (NX - 1) // NX)], fs_send.at[0])
    take(ffn_pair, fs_send.at[1])


def by_channel(maps):
    return jnp.swapaxes(maps, 2, 3).reshape(2 * CH, S)


def local(
    mix_input, stream, doc_ids, log_dt, decay_rate, frequency, input_real, input_imag,
    output_real, output_imag, skip_gain, log_keep, proj_weight, norm_gain, gate_weight,
    up_weight, down_weight,
):
    vmem = pl.BlockSpec(memory_space=pltpu.VMEM)
    specs = [pl.BlockSpec(memory_space=pl.ANY)] * 17
    dma = pltpu.SemaphoreType.DMA
    scratch = [
        pltpu.VMEM((T, CH), BF16),
        pltpu.VMEM((TOK, D), BF16),
        pltpu.VMEM((1, T), jnp.int32),
        pltpu.VMEM((1, G), F32),
        pltpu.VMEM((G, S), F32),
        pltpu.VMEM((G, S), F32),
        pltpu.VMEM((2 * CH, S), F32),
        pltpu.VMEM((2 * CH, S), F32),
        pltpu.VMEM((2 * CH, S), F32),
        pltpu.VMEM((2 * CH, S), F32),
        pltpu.VMEM((1, CH), F32),
        pltpu.VMEM((G, T), F32),
        pltpu.VMEM((1, D), F32),
        pltpu.VMEM((ROWS, FF), BF16),
        pltpu.VMEM((ROWS, FF), BF16),
        pltpu.VMEM((ROWS, FF), BF16),
        pltpu.VMEM((SP, ROWS, GUA), BF16),
        pltpu.VMEM((SP, ROWS, GUB), BF16),
        pltpu.VMEM((SP, ROWS, DA), BF16),
        pltpu.VMEM((SP, DROWS, DB), BF16),
        pltpu.VMEM((T, 4 * W), F32),
        pltpu.VMEM((T, 2 * W), F32),
        pltpu.VMEM((T, 4 * W), F32),
        pltpu.VMEM((2, 4, CH, W), BF16),
        pltpu.VMEM((NY, 24, 128), F32),
        pltpu.VMEM((2, 16, 128), F32),
        pltpu.VMEM((NZ, 16, 128), F32),
        pltpu.VMEM((TP, CH + TOK, D), BF16),
        pltpu.VMEM((TP, T, CH), BF16),
        pltpu.VMEM((T, D), F32),
        pltpu.VMEM((TOK, D), F32),
        pltpu.VMEM((T, D), BF16),
        pltpu.VMEM((T, KPAD), BF16),
        pltpu.VMEM((NZ, NC, NX, TOK, NY * ROWS), BF16),
        pltpu.VMEM((NZ, NX, TOK, NY * ROWS), BF16),
        pltpu.VMEM((NZ, NX, TOK, NY * ROWS), BF16),
        pltpu.VMEM((NZ, NX, TOK, NY * ROWS), BF16),
        dma((2,)), dma((RECVS,)), dma((2,)), dma((RECVS,)),
        dma((2, 2)), dma((2, 4)), dma((2, 2)), dma((NZ,)), dma((2,)), dma((NZ,)), dma((22,)),
    ]
    return pl.pallas_call(
        kernel,
        out_shape=pltpu.VMEM((TOK, D), BF16),
        in_specs=specs,
        out_specs=vmem,
        scratch_shapes=scratch,
        compiler_params=pltpu.CompilerParams(
            collective_id=0, has_side_effects=True, vmem_limit_bytes=60 << 20
        ),
        name="layer",
    )(
        mix_input, stream, doc_ids.reshape(1, T), log_dt.reshape(1, G), decay_rate, frequency,
        by_channel(input_real), by_channel(input_imag),
        output_real.reshape(2 * CH, S), output_imag.reshape(2 * CH, S),
        skip_gain.reshape(1, CH), log_keep, proj_weight, norm_gain.reshape(1, D),
        gate_weight, up_weight, down_weight.T,
    )


def solution(mesh):
    torus = Mesh(mesh.devices.reshape(NZ, NY, NX, NC), ("z", "y", "x", "c"))
    sp, tp = ("z", "y"), ("x", "c")
    every = ("z", "y", "x", "c")
    in_specs = (
        P(sp, tp), P(every, None), P(sp), P(tp), P(tp, None), P(tp, None),
        P(None, tp, None, None), P(None, tp, None, None),
        P(None, tp, None, None), P(None, tp, None, None),
        P(tp), P(tp, sp), P(tp, None), P(), P(sp, tp), P(sp, tp), P(tp, sp),
    )
    return jax.shard_map(
        local, mesh=torus, in_specs=in_specs, out_specs=P(every, None), check_vma=False
    )
```

```python
import functools

import jax
import jax.numpy as jnp
from jax import lax
from jax.experimental import pallas as pl
from jax.experimental.pallas import tpu as pltpu
from jax.sharding import Mesh
from jax.sharding import PartitionSpec as P

HIGHEST = lax.Precision.HIGHEST
MESH = pl.DeviceIdType.MESH
F32, BF16 = jnp.float32, jnp.bfloat16

NZ, NY, NX, NC = 8, 4, 4, 2
SP, TP = NZ * NY, NX * NC
T, CH, G, S, GW = 256, 128, 8, 64, 16
W = G * S
CHUNKS = 8
STEPS = T // CHUNKS
D = 2048
FF = 704
MAIN = 640
ROWS = D // SP
TOK = T // TP
GUA, GUB = MAIN + 128, MAIN
DA, DB = 512, 128
DROWS = ROWS + ROWS // 2
KPAD = MAIN + 256
NT = (((1,), (1,)), ((), ()))


def dot(a, b, precision=None):
    return jnp.dot(a, b, preferred_element_type=F32, precision=precision)


def dot_nt(a, b, precision=None):
    return lax.dot_general(a, b, NT, preferred_element_type=F32, precision=precision)


def halves(value):
    high = value.astype(BF16)
    return high, (value - high.astype(F32)).astype(BF16)


def iota(shape, dim):
    return lax.broadcasted_iota(jnp.int32, shape, dim)


def one_hot(mask, dtype):
    return jnp.where(mask, 1.0, 0.0).astype(F32).astype(dtype)


def cmul(ar, ai, br, bi):
    return ar * br - ai * bi, ar * bi + ai * br


class Relay:
    def __init__(self, ra, rb, send, recv, z, y, joint):
        self.ra, self.rb, self.send, self.recv = ra, rb, send, recv
        self.z, self.y, self.joint = z, y, joint

    def zi(self, offset):
        return lax.rem(self.z + (offset + NZ), NZ)

    def yi(self, offset):
        return lax.rem(self.y + (offset + NY), NY)

    def start(self, number, ref, axis, to):
        pltpu.make_async_remote_copy(
            src_ref=ref,
            dst_ref=ref,
            send_sem=self.send.at[0 if number < 20 else 1],
            recv_sem=self.recv.at[number],
            device_id={axis: self.zi(to) if axis == "z" else self.yi(to)},
            device_id_type=MESH,
        ).start()

    def wait(self, number, ref):
        pltpu.make_async_copy(ref, ref, self.recv.at[number]).wait()

    def a(self, dz, dy):
        return self.ra.at[self.zi(dz) * NY + self.yi(dy)]

    def send_az(self, d):
        for way in (1, -1):
            ref = self.a(-way * (d - 1), 0)
            if d == 4:
                ref = self.half(ref, way)
            self.start(d - 1, ref, "z", way)

    def send_ay(self, o):
        for way in (1, -1):
            self.start(4 + o % NZ, self.a(o, 0), "y", way)

    def az(self, d):
        self.wait(d - 1, self.ra.at[0] if d == 4 else self.ra.at[pl.ds(0, 2)])
        if d < 4:
            self.send_az(d + 1)
        for o in (4,) if d == 4 else (-d, d):
            self.send_ay(o)

    def ay(self, o):
        self.wait(4 + o % NZ, self.ra.at[pl.ds(0, 2)])
        way = 1 if o % 2 == 0 else -1
        self.start(12 + (0 if self.joint else o % NZ), self.a(o, -way), "y", way)

    def al(self, o):
        self.wait(12 + o % NZ, self.ra.at[0])

    def all_al(self):
        self.wait(12, self.ra.at[pl.ds(0, NZ)])

    def send_by(self, d):
        for way in (1, -1):
            ref = self.rb.at[self.z * NY + self.yi(-way * (d - 1))]
            if d == 2:
                ref = self.half(ref, way)
            self.start(19 + d, ref, "y", way)

    def by(self, d):
        self.wait(19 + d, self.rb.at[pl.ds(0, 2)] if d == 1 else self.rb.at[0])
        if d == 1:
            self.send_by(2)
        self.send_bz(1, d)

    def send_bz(self, d, j):
        for way in (1, -1):
            first = self.zi(-way * (d - 1)) * NY
            for dy in ((0,), (1, -1), (2,))[j]:
                if d == 4 and dy == -way:
                    continue
                ref = self.rb.at[first + self.yi(dy)]
                if d == 4 and j != 1:
                    ref = self.half(ref, way)
                self.start(19 + 3 * d + j, ref, "z", way)

    def bz(self, d, j):
        count = (2 if j == 1 else 1) * (1 if d == 4 else 2)
        self.wait(19 + 3 * d + j, self.rb.at[pl.ds(0, count)])
        if d < 4:
            self.send_bz(d + 1, j)

    def half(self, ref, way):
        rows = ref.shape[0] // 2
        return ref.at[pl.ds(0 if way > 0 else rows, rows)]

    def drain(self):
        for n, ref in enumerate((self.ra, self.rb)):
            part = ref.at[pl.ds(0, SP - 1)]
            pltpu.make_async_copy(part, part, self.send.at[n]).wait()


RECVS = 34
OFFSETS = (0, -1, 1, -2, 2, -3, 3, 4)
ORDER = (
    "gby 1", "dby 1", "gaz 1", "line", "day 0", "gby 2", "daz 1", "gaz 2", "gbz 1 0", "gay 0",
    "share", "gbz 1 2", "gay -1", "share2", "gay -2", "day -1", "maps", "gbz 1 1", "gaz 3",
    "scan", "gbz 2 0", "gay 1", "out", "gay 2", "gbz 2 2", "gbz 2 1", "gay -3", "last", "gaz 4",
    "daz 2", "gbz 3 0", "gbz 3 2", "dby 2", "gay 3", "pass", "gbz 3 1", "gay 4", "day 1", "day 2",
    "daz 3", "dbz 1 1", "proj", "dbz 1 0", "dbz 1 2", "day -2", "norm", "gbz 4 0", "gbz 4 1",
    "gbz 4 2", "widen", "daz 4", "dbz 2 1", "dal 1", "product 1", "dbz 2 0", "dal -1",
    "product -1", "day -3", "day 3", "dbz 2 2", "combine 1", "dal 0", "product 0", "combine -1",
    "dal 2", "product 2", "dal -2", "product -2", "dbz 3 1", "combine 0", "dbz 3 0", "day 4",
    "dbz 3 2", "combine -2", "dal -3", "product -3", "dal 3", "product 3", "combine 2",
    "combine -3", "dbz 4 0", "dbz 4 1", "dbz 4 2", "narrow 4", "dal 4", "product 4", "combine 3", "combine 4",
    "finish 1", "finish -1", "finish 0", "finish -2", "finish 2", "finish -3", "finish 3",
    "finish 4",
)


def row_of(block):
    return jnp.concatenate([block[g : g + 1, :] for g in range(G)], axis=1)


def rows_of(row):
    return jnp.concatenate([row[:, 128 * k : 128 * (k + 1)] for k in range(W // 128)], axis=0)


def flat_of(rows):
    return jnp.concatenate([rows[k : k + 1, :] for k in range(W // 128)], axis=1)


def kernel(
    mix_hbm, stream_hbm, docs_hbm, log_dt_hbm, decay_hbm, freq_hbm, in_real_hbm, in_imag_hbm,
    out_real_hbm, out_imag_hbm, skip_hbm, keep_hbm, proj_hbm, gain_hbm, gate_hbm, up_hbm, down_hbm,
    result,
    mix, stream, docs, log_dt, decay, freq, in_real, in_imag, out_real, out_imag, skip, log_keep,
    gain, gate_w, up_w, down_w,
    gua, gub, dna, dnb, drive, factor, states, maps, line, message, column, shared, mixes,
    branch, resid, normed, hidden, ffn_part, ffn_pair, ffn_send, ffn_recv,
    gu_send, gu_recv, dn_send, dn_recv, carry_sem, shared_sem, mix_sem, pair_sem, fs_send, fs_recv, load_sem,
):
    z, y, x, c = (lax.axis_index(a) for a in ("z", "y", "x", "c"))
    sp, tp = z * NY + y, x * NC + c

    def tp_peer(k):
        other = lax.rem(tp + k, TP)
        return other, {"x": other // NC, "c": lax.rem(other, NC)}

    def at_z(k):
        return {"z": lax.rem(z + k, NZ)}

    def at_y(k):
        return {"y": lax.rem(y + k, NY)}

    def at_x(k):
        return {"x": lax.rem(x + k, NX)}

    sibling = {"c": 1 - c}

    barrier = pltpu.get_barrier_semaphore()

    def greet(device):
        pl.semaphore_signal(barrier, inc=1, device_id=device, device_id_type=MESH)

    for k in (1, 7, 2, 6, 3, 5, 4):
        greet(at_z(k))
    for k in (1, 3, 2):
        greet(at_y(k))
    for k in range(1, TP):
        greet(tp_peer(k)[1])

    def push(source, target, sems, n, device):
        pltpu.make_async_remote_copy(
            src_ref=source, dst_ref=target, send_sem=sems.at[0, n], recv_sem=sems.at[1, n],
            device_id=device, device_id_type=MESH).start()

    def take(ref, sem):
        pltpu.make_async_copy(ref, ref, sem).wait()

    def load(n, *pairs):
        copies = [pltpu.make_async_copy(*pair, load_sem.at[n]) for pair in pairs]
        for copy in copies:
            copy.start()
        return copies

    def loaded(copies):
        for copy in copies:
            copy.wait()

    gate_load = load(0, (gate_hbm, gate_w))
    up_load = load(1, (up_hbm, up_w))
    gate_piece = load(2, (gate_hbm.at[:, pl.ds(0, MAIN)], gub.at[sp]))
    up_piece = load(3, (up_hbm.at[:, pl.ds(0, MAIN)], gua.at[sp, :, pl.ds(0, MAIN)]))
    down_load = load(17, (down_hbm, down_w))
    down_pieces = [
        load(18, (down_hbm.at[:, pl.ds(0, DA)], dna.at[sp])),
        load(19, (down_hbm.at[:, pl.ds(DA, DB)], dnb.at[sp, pl.ds(0, ROWS)])),
    ]
    scan_loads = [
        load(4 + n, pair) for n, pair in enumerate((
            (log_dt_hbm, log_dt), (decay_hbm, decay), (freq_hbm, freq), (mix_hbm, mix),
            (docs_hbm, docs), (keep_hbm, log_keep), (in_real_hbm, in_real), (in_imag_hbm, in_imag),
        ))
    ]
    share_loads = [
        load(12, (proj_hbm, shared.at[tp, pl.ds(0, CH)])),
        load(13, (stream_hbm, shared.at[tp, pl.ds(CH, TOK)])),
    ]
    map_loads = [
        load(n, pair) for n, pair in (
            (14, (out_real_hbm, out_real)), (15, (out_imag_hbm, out_imag)),
            (16, (stream_hbm, stream)), (20, (skip_hbm, skip)), (21, (gain_hbm, gain)),
        )
    ]
    loaded(gate_load)
    loaded(up_load)
    gua[sp, :, MAIN:GUA] = jnp.concatenate([gate_w[:, MAIN:FF], up_w[:, MAIN:FF]], axis=1)
    loaded(down_load)
    rest = down_w[:, MAIN:FF]
    dnb[sp, ROWS:DROWS] = jnp.concatenate([rest[: ROWS // 2], rest[ROWS // 2 :]], axis=1)

    gu = Relay(gua, gub, gu_send, gu_recv, z, y, True)
    dn = Relay(dna, dnb, dn_send, dn_recv, z, y, False)
    loaded(gate_piece)
    loaded(up_piece)
    pl.semaphore_wait(barrier, NZ - 1 + NY - 1 + TP - 1)
    gu.send_by(1)
    gu.send_bz(1, 0)
    gu.send_az(1)
    for copies in down_pieces:
        loaded(copies)
    dn.send_by(1)
    dn.send_ay(0)
    dn.send_az(1)
    dn.send_bz(1, 0)
    for copies in share_loads:
        loaded(copies)
    half = (CH + TOK) // 2
    for n, rows in ((0, (0, half)), (3, (half, 0))):
        for k, first in zip((1, 3), rows):
            ref = shared.at[tp, pl.ds(first, half)]
            push(ref, ref, shared_sem, n, at_x(k))
    push(shared.at[tp], shared.at[tp], shared_sem, 2, sibling)
    for copies in scan_loads:
        loaded(copies)

    group = iota((G, S), 0)
    steps = jnp.zeros((G, S), F32)
    for g in range(G):
        steps = jnp.where(group == g, log_dt[0:1, g : g + 1], steps)
    steps = jnp.exp(steps)
    rate, turn_rate = decay[...], freq[...]
    magnitude = jnp.exp(-steps * rate)
    angle = steps * turn_rate
    a_real, a_imag = magnitude * jnp.cos(angle), magnitude * jnp.sin(angle)
    below = rate * rate + turn_rate * turn_rate
    shifted = a_real - 1.0
    z_real = (-shifted * rate + a_imag * turn_rate) / below
    z_imag = (-a_imag * rate - shifted * turn_rate) / below
    ar, ai, zr, zi = (row_of(v) for v in (a_real, a_imag, z_real, z_imag))

    r, t = iota((T, T), 0), iota((T, T), 1)
    order = t == lax.rem(r, CHUNKS) * STEPS + r // CHUNKS
    order_f = one_hot(order, F32)
    u = dot(order_f.astype(BF16), mix[...])
    ub = u.astype(BF16)

    tile = one_hot(lax.rem(iota((S, W), 1), S) == iota((S, W), 0), BF16)
    own = lax.rem(iota((2 * CH, W), 0), CH) // GW == iota((2 * CH, W), 1) // S
    for n, ref in enumerate((in_real, in_imag)):
        high, low = (
            jnp.where(own, dot(half, tile), 0.0).astype(BF16) for half in halves(ref[...])
        )
        for d in range(2):
            at = slice(CH * d, CH * (d + 1))
            drive[:, W * (2 * n + d) : W * (2 * n + d + 1)] = dot(ub, high[at]) + dot(ub, low[at])

    doc = docs[...].astype(F32) + jnp.zeros((G, T), F32)
    place = iota((G, T), 1)
    before, after = pltpu.roll(doc, 1, 1), pltpu.roll(doc, T - 1, 1)
    keep = jnp.exp(log_keep[...])
    keep_f = jnp.where((place == 0) | (doc == before), keep, 0.0)
    keep_b = jnp.where((place == T - 1) | (doc == after), keep, 0.0)
    both = dot_nt(order_f, jnp.concatenate([keep_f, keep_b], axis=0), HIGHEST)
    spread = one_hot(iota((2 * G, 2 * W), 0) == iota((2 * G, 2 * W), 1) // S, F32)
    factor[...] = dot(both, spread, HIGHEST)

    zero = jnp.zeros((CHUNKS, W), F32)
    ar8, ai8 = zero + ar, zero + ai

    def advance(j, state, direction):
        at = pl.ds(pl.multiple_of(j * CHUNKS, CHUNKS), CHUNKS)
        f = factor[at, W * direction : W * (direction + 1)]
        dr = drive[at, W * direction : W * (direction + 1)]
        di = drive[at, W * (2 + direction) : W * (3 + direction)]
        hr, hi = state
        nr, ni = cmul(f * ar8, f * ai8, hr, hi)
        return f, nr + dr, ni + di

    def first(j, state):
        fr, fi, fp, br, bi, bp = state
        f, fr, fi = advance(j, (fr, fi), 0)
        b, br, bi = advance(STEPS - 1 - j, (br, bi), 1)
        return fr, fi, fp * f, br, bi, bp * b

    fr, fi, fp, br, bi, bp = lax.fori_loop(
        0, STEPS, first, (zero, zero, zero + 1.0, zero, zero, zero + 1.0)
    )
    pr, pi = ar, ai
    for _ in range(5):
        pr, pi = cmul(pr, pi, pr, pi)

    def chunk_entries(enter, hr, hi, passed, backward):
        er, ei = enter
        entries = [None] * CHUNKS
        chunks = range(CHUNKS - 1, -1, -1) if backward else range(CHUNKS)
        for k in chunks:
            entries[k] = (er, ei)
            f = passed[k : k + 1]
            nr, ni = cmul(f * pr, f * pi, er, ei)
            er, ei = nr + hr[k : k + 1], ni + hi[k : k + 1]
        return entries, (er, ei)

    none = (jnp.zeros((1, W), F32), jnp.zeros((1, W), F32))
    end_f = chunk_entries(none, fr, fi, fp, False)[1]
    end_b = chunk_entries(none, br, bi, bp, True)[1]
    passed = fp[0:1]
    for k in range(1, CHUNKS):
        passed = passed * fp[k : k + 1]
    qr, qi = pr, pi
    for _ in range(3):
        qr, qi = cmul(qr, qi, qr, qi)
    edge_first = jnp.broadcast_to(doc[0:1, 0:1], (1, 128))
    edge_last = jnp.broadcast_to(doc[0:1, T - 1 : T], (1, 128))
    passed_rows = rows_of(passed)
    edges = jnp.concatenate(
        [edge_first, edge_last, jnp.zeros((2, 128), F32)], axis=0)
    for n, (er, ei) in enumerate((end_f, end_b)):
        line[y, 8 * n : 8 * n + 4] = rows_of(er)
        line[y, 8 * n + 4 : 8 * n + 8] = rows_of(ei)
    line[y, 16:20] = passed_rows
    line[y, 20:24] = edges

    for k in (2, 1, 3):
        push(line.at[y], line.at[y], carry_sem, 0, at_y(k))
    gu.send_ay(0)

    def output_maps():
        for copies in map_loads:
            loaded(copies)
        spread = tile.astype(F32)
        cr = jnp.where(own, dot(out_real[...], spread, HIGHEST), 0.0)
        ci = jnp.where(own, dot(out_imag[...], spread, HIGHEST), 0.0)
        cr, ci = cmul(zr, zi, cr, ci)
        for n in range(4):
            read = (cr if n < 2 else -ci)[CH * (n % 2) : CH * (n % 2 + 1)]
            maps[0, n], maps[1, n] = halves(read)

    q4r, q4i = rows_of(qr), rows_of(qi)
    s4r, s4i = cmul(q4r, q4i, q4r, q4i)
    s4r, s4i = cmul(s4r, s4i, s4r, s4i)
    four = jnp.zeros((4, 128), F32)
    start = (four, four, jnp.zeros((1, 128), F32) - 1.0)

    def fold(state, m, side, power, passed, near, far, use):
        cr, ci, last = state
        link = jnp.where(m[near : near + 1] == last, 1.0, 0.0) * m[passed : passed + 4]
        nr, ni = cmul(link * power[0], link * power[1], cr, ci)
        cr = jnp.where(use, nr + m[side : side + 4], cr)
        ci = jnp.where(use, ni + m[side + 4 : side + 8], ci)
        return cr, ci, jnp.where(use, m[far : far + 1], last)

    def fold_line(state, backward, use):
        for k in range(NY - 1, -1, -1) if backward else range(NY):
            m = line[k]
            if backward:
                state = fold(state, m, 8, (q4r, q4i), 16, 21, 20, use(k))
            else:
                state = fold(state, m, 0, (q4r, q4i), 16, 20, 21, use(k))
        return state

    def carry_line():
        take(line.at[pl.ds(0, NY - 1)], carry_sem.at[1, 0])
        always = lambda k: k >= 0
        ends = fold_line(start, False, always), fold_line(start, True, always)
        passed = line[0][16:20]
        for k in range(1, NY):
            link = jnp.where(line[k][20:21] == line[k - 1][21:22], 1.0, 0.0)
            passed = passed * (link * line[k][16:20])
        edges = jnp.concatenate(
            [line[0][20:21], line[NY - 1][21:22], jnp.zeros((2, 128), F32)], axis=0)
        for n in range(2):
            message[n, 0:4] = ends[n][0]
            message[n, 4:8] = ends[n][1]
            message[n, 8:12] = passed
            message[n, 12:16] = edges
        column[z] = message[0]
        for k in (4, 3, 5, 2, 6, 1, 7):
            side = jnp.where(lax.rem(z + k, NZ) > z, 0, 1)
            push(message.at[side], column.at[z], carry_sem, 1, at_z(k))

    def carry_column():
        take(column.at[pl.ds(0, NZ - 1)], carry_sem.at[1, 1])
        forward, backward = start, start
        for k in range(NZ):
            forward = fold(forward, column[k], 0, (s4r, s4i), 8, 12, 13, k < z)
            j = NZ - 1 - k
            backward = fold(backward, column[j], 0, (s4r, s4i), 8, 13, 12, j > z)
        into_f = fold_line(forward, False, lambda k: k < y)
        into_b = fold_line(backward, True, lambda k: k > y)
        enter_f = jnp.where(into_f[2] == edge_first, 1.0, 0.0)
        enter_b = jnp.where(into_b[2] == edge_last, 1.0, 0.0)
        enter_f = (flat_of(into_f[0] * enter_f), flat_of(into_f[1] * enter_f))
        enter_b = (flat_of(into_b[0] * enter_b), flat_of(into_b[1] * enter_b))
        entries_f = chunk_entries(enter_f, fr, fi, fp, False)[0]
        entries_b = chunk_entries(enter_b, br, bi, bp, True)[0]
        return tuple(
            jnp.concatenate([e[part_no] for e in entries], axis=0)
            for entries in (entries_f, entries_b) for part_no in (0, 1)
        )

    def second(j, state):
        fr, fi, br, bi = state
        _, fr, fi = advance(j, (fr, fi), 0)
        k = STEPS - 1 - j
        _, br, bi = advance(k, (br, bi), 1)
        at = pl.ds(pl.multiple_of(j * CHUNKS, CHUNKS), CHUNKS)
        states[at, 0:W] = fr
        states[at, 2 * W : 3 * W] = fi
        at = pl.ds(pl.multiple_of(k * CHUNKS, CHUNKS), CHUNKS)
        states[at, W : 2 * W] = br
        states[at, 3 * W : 4 * W] = bi
        return fr, fi, br, bi

    def scan():
        lax.fori_loop(0, STEPS, second, carry_column())

    def mix_out():
        pre = skip[...] * u
        for n in range(4):
            high, low = halves(states[:, W * n : W * (n + 1)])
            pre = pre + dot_nt(high, maps[0, n]) + dot_nt(high, maps[1, n])
            pre = pre + dot_nt(low, maps[0, n])
        mixed = jax.nn.gelu(pre).astype(BF16)
        back = one_hot(t == lax.rem(r, STEPS) * CHUNKS + r // STEPS, BF16)
        mixes[tp] = dot(back, mixed).astype(BF16)
        for k in (2, 1, 3):
            push(mixes.at[tp], mixes.at[tp], mix_sem, 0, at_x(k))
        push(mixes.at[tp], mixes.at[tp], mix_sem, 1, sibling)

    def of_x(k):
        return lax.rem(x + k, NX) * NC + c

    def share():
        take(shared.at[0], shared_sem.at[1, 0])
        for k, first in ((1, half), (3, 0)):
            ref = shared.at[of_x(k), pl.ds(first, half)]
            push(ref, ref, shared_sem, 1, at_x(NX - k))

    def share_rest():
        take(shared.at[0], shared_sem.at[1, 3])
        for k in (1, 3):
            push(shared.at[of_x(k)], shared.at[of_x(k)], shared_sem, 2, sibling)

    def share_last():
        take(shared.at[0], shared_sem.at[1, 1])
        push(shared.at[of_x(2)], shared.at[of_x(2)], shared_sem, 2, sibling)

    def mix_pass():
        take(mixes.at[pl.ds(0, 3)], mix_sem.at[1, 0])
        for k in (1, 2, 3):
            push(mixes.at[of_x(k)], mixes.at[of_x(k)], mix_sem, 1, sibling)

    def project():
        take(shared.at[pl.ds(0, 4)], shared_sem.at[1, 2])
        take(mixes.at[pl.ds(0, 4)], mix_sem.at[1, 1])
        both = jnp.concatenate([mixes[k] for k in range(TP)], axis=1)
        branch[...] = dot(both, shared[:, 0:CH].reshape(TP * CH, D))

    def normalize():
        scales = gain[...]
        resid[...] = stream[...].astype(F32) + branch[pl.ds(pl.multiple_of(tp * TOK, TOK), TOK)]

        @pl.loop(0, TP)
        def _(k):
            at = pl.ds(pl.multiple_of(k * TOK, TOK), TOK)
            kept = shared[k, CH : CH + TOK].astype(F32) + branch[at]
            scale = lax.rsqrt(jnp.mean(kept * kept, axis=-1, keepdims=True) + 1e-6)
            normed[at] = (kept * scale * scales).astype(BF16)

    def widen():
        gu.all_al()
        rows = normed[...]
        second_part = dot(rows, gua[...].reshape(D, GUA))
        first_part = dot(rows, gub[...].reshape(D, GUB))
        hidden[:, 0:MAIN] = (jax.nn.silu(first_part) * second_part[:, 0:MAIN]).astype(BF16)
        tail_gate = second_part[:, MAIN:FF]
        tail_up = second_part[:, FF:GUA]
        tail = (jax.nn.silu(tail_gate) * tail_up).astype(BF16)
        empty = jnp.zeros((T, FF - MAIN), BF16)
        hidden[:, MAIN:KPAD] = jnp.concatenate([tail, empty, empty, tail], axis=1)

    ready = {}

    def narrow(o):
        at = pl.ds(gu.zi(o) * NY, NY)
        main = dot_nt(hidden[:, DA:MAIN], dnb[at, 0:ROWS].reshape(NY * ROWS, DB))
        rest = dnb[at, ROWS:DROWS].reshape(NY * ROWS // 2, DB)
        sides = [dot_nt(hidden[:, k : k + 128], rest) for k in (MAIN, MAIN + 128)]
        ready[o] = main + jnp.concatenate(
            [side[:, k : k + ROWS // 2] for k in range(0, 128, ROWS // 2) for side in sides], axis=1
        )

    def product(o):
        if o not in ready:
            narrow(o)
        zi = gu.zi(o)
        out = dot_nt(hidden[:, 0:DA], dna[pl.ds(zi * NY, NY)].reshape(NY * ROWS, DA)) + ready[o]
        out = out.astype(BF16).reshape(NX, NC, TOK, NY * ROWS)
        for k in range(NC):
            ffn_part[zi, k] = out[:, k]
        pltpu.make_async_remote_copy(
            src_ref=ffn_part.at[zi, 1 - c], dst_ref=ffn_pair.at[zi],
            send_sem=fs_send.at[1], recv_sem=pair_sem.at[zi],
            device_id=sibling, device_id_type=MESH).start()

    def combine(o):
        zi = gu.zi(o)
        take(ffn_pair.at[zi], pair_sem.at[zi])
        total = ffn_part[zi, c].astype(F32) + ffn_pair[zi].astype(F32)
        ffn_send[zi] = total.astype(BF16)
        for k in (2, 1, 3):
            pltpu.make_async_remote_copy(
                src_ref=ffn_send.at[zi, lax.rem(x + k, NX)], dst_ref=ffn_recv.at[zi, x],
                send_sem=fs_send.at[0], recv_sem=fs_recv.at[zi],
                device_id=at_x(k), device_id_type=MESH).start()
        ffn_recv[zi, x] = ffn_send[zi, x]

    def finish(o):
        zi = gu.zi(o)
        take(ffn_recv.at[zi, pl.ds(0, NX - 1)], fs_recv.at[zi])
        at = pl.ds(pl.multiple_of(zi * (NY * ROWS), NY * ROWS), NY * ROWS)
        ffn = ffn_recv[zi, 0].astype(F32)
        for k in range(1, NX):
            ffn = ffn + ffn_recv[zi, k].astype(F32)
        result[:, at] = (resid[:, at] + 0.5 * ffn).astype(BF16)

    steps = {
        "maps": output_maps, "line": carry_line, "scan": scan, "out": mix_out, "share": share,
        "share2": share_rest, "last": share_last,
        "pass": mix_pass, "proj": project, "norm": normalize, "widen": widen,
        "narrow": narrow, "product": product, "combine": combine, "finish": finish,
    }
    for step in ORDER:
        name, number = step.split()[0], [int(n) for n in step.split()[1:]]
        if name[0] in "gd" and name[1:] in ("az", "ay", "al", "by", "bz"):
            getattr(gu if name[0] == "g" else dn, name[1:])(*number)
        else:
            steps[name](*number)

    gu.drain()
    dn.drain()
    take(line.at[pl.ds(0, NY - 1)], carry_sem.at[0, 0])
    take(column.at[pl.ds(0, NZ - 1)], carry_sem.at[0, 1])
    take(shared.at[0], shared_sem.at[0, 0])
    take(shared.at[0], shared_sem.at[0, 3])
    take(shared.at[0], shared_sem.at[0, 1])
    take(shared.at[pl.ds(0, 4)], shared_sem.at[0, 2])
    take(mixes.at[pl.ds(0, 3)], mix_sem.at[0, 0])
    take(mixes.at[pl.ds(0, 4)], mix_sem.at[0, 1])
    take(ffn_recv.at[pl.ds(0, NZ * (NX - 1) // NX)], fs_send.at[0])
    take(ffn_pair, fs_send.at[1])


def by_channel(maps):
    return jnp.swapaxes(maps, 2, 3).reshape(2 * CH, S)


def local(
    mix_input, stream, doc_ids, log_dt, decay_rate, frequency, input_real, input_imag,
    output_real, output_imag, skip_gain, log_keep, proj_weight, norm_gain, gate_weight,
    up_weight, down_weight,
):
    vmem = pl.BlockSpec(memory_space=pltpu.VMEM)
    specs = [pl.BlockSpec(memory_space=pl.ANY)] * 17
    dma = pltpu.SemaphoreType.DMA
    scratch = [
        pltpu.VMEM((T, CH), BF16),
        pltpu.VMEM((TOK, D), BF16),
        pltpu.VMEM((1, T), jnp.int32),
        pltpu.VMEM((1, G), F32),
        pltpu.VMEM((G, S), F32),
        pltpu.VMEM((G, S), F32),
        pltpu.VMEM((2 * CH, S), F32),
        pltpu.VMEM((2 * CH, S), F32),
        pltpu.VMEM((2 * CH, S), F32),
        pltpu.VMEM((2 * CH, S), F32),
        pltpu.VMEM((1, CH), F32),
        pltpu.VMEM((G, T), F32),
        pltpu.VMEM((1, D), F32),
        pltpu.VMEM((ROWS, FF), BF16),
        pltpu.VMEM((ROWS, FF), BF16),
        pltpu.VMEM((ROWS, FF), BF16),
        pltpu.VMEM((SP, ROWS, GUA), BF16),
        pltpu.VMEM((SP, ROWS, GUB), BF16),
        pltpu.VMEM((SP, ROWS, DA), BF16),
        pltpu.VMEM((SP, DROWS, DB), BF16),
        pltpu.VMEM((T, 4 * W), F32),
        pltpu.VMEM((T, 2 * W), F32),
        pltpu.VMEM((T, 4 * W), F32),
        pltpu.VMEM((2, 4, CH, W), BF16),
        pltpu.VMEM((NY, 24, 128), F32),
        pltpu.VMEM((2, 16, 128), F32),
        pltpu.VMEM((NZ, 16, 128), F32),
        pltpu.VMEM((TP, CH + TOK, D), BF16),
        pltpu.VMEM((TP, T, CH), BF16),
        pltpu.VMEM((T, D), F32),
        pltpu.VMEM((TOK, D), F32),
        pltpu.VMEM((T, D), BF16),
        pltpu.VMEM((T, KPAD), BF16),
        pltpu.VMEM((NZ, NC, NX, TOK, NY * ROWS), BF16),
        pltpu.VMEM((NZ, NX, TOK, NY * ROWS), BF16),
        pltpu.VMEM((NZ, NX, TOK, NY * ROWS), BF16),
        pltpu.VMEM((NZ, NX, TOK, NY * ROWS), BF16),
        dma((2,)), dma((RECVS,)), dma((2,)), dma((RECVS,)),
        dma((2, 2)), dma((2, 4)), dma((2, 2)), dma((NZ,)), dma((2,)), dma((NZ,)), dma((22,)),
    ]
    return pl.pallas_call(
        kernel,
        out_shape=pltpu.VMEM((TOK, D), BF16),
        in_specs=specs,
        out_specs=vmem,
        scratch_shapes=scratch,
        compiler_params=pltpu.CompilerParams(
            collective_id=0, has_side_effects=True, vmem_limit_bytes=60 << 20
        ),
        name="layer",
    )(
        mix_input, stream, doc_ids.reshape(1, T), log_dt.reshape(1, G), decay_rate, frequency,
        by_channel(input_real), by_channel(input_imag),
        output_real.reshape(2 * CH, S), output_imag.reshape(2 * CH, S),
        skip_gain.reshape(1, CH), log_keep, proj_weight, norm_gain.reshape(1, D),
        gate_weight, up_weight, down_weight.T,
    )


def solution(mesh):
    torus = Mesh(mesh.devices.reshape(NZ, NY, NX, NC), ("z", "y", "x", "c"))
    sp, tp = ("z", "y"), ("x", "c")
    every = ("z", "y", "x", "c")
    in_specs = (
        P(sp, tp), P(every, None), P(sp), P(tp), P(tp, None), P(tp, None),
        P(None, tp, None, None), P(None, tp, None, None),
        P(None, tp, None, None), P(None, tp, None, None),
        P(tp), P(tp, sp), P(tp, None), P(), P(sp, tp), P(sp, tp), P(tp, sp),
    )
    return jax.shard_map(
        local, mesh=torus, in_specs=in_specs, out_specs=P(every, None), check_vma=False
    )
```
